32 devices in a mesh: sp: 8 (over z, x), tp: 4 (over y, core).
Axes of the slice: x: 2, y: 2, z: 4, core: 2. Of those that a mesh axis runs over, the one named last changes fastest.
Arguments:
- stream_in: bfloat16 [2048, 2048], P(('sp', 'tp')), may hold values from -6 to 6
- queries: bfloat16 [2048, 4096], P('sp', 'tp'), may hold values from -6 to 6
- key_rows: bfloat16 [2048, 4096], P('sp', 'tp'), may hold values from -6 to 6
- values: bfloat16 [2048, 8192], P('sp', 'tp'), may hold values from -6 to 6
- decay_low: bfloat16 [2048, 16], P('sp'), may hold values from -4 to 4
- decay_matrix: bfloat16 [16, 4096], P(None, 'tp'), may hold values from -1.5 to 1.5
- decay_bias: float32 [4096], P('tp')
- decay_shift: float32 [2048, 16], P('sp', 'tp'), may hold values from -1 to 0
- head_gain: float32 [512], replicated, may hold values from 0.1 to 1.9
- output_matrix: bfloat16 [8192, 2048], P('tp'), may hold values from -0.0625 to 0.0625
- feed_gain: float32 [2048], replicated, may hold values from 0.1 to 1.9
- routes: int32 [2048, 2], P('sp'), may hold values from 0 to 7, all different within a row; in each aligned block of 256 rows (0 to 255, 256 to 511, ...) at most 64 rows name the same one
- route_weights: float32 [2048, 2], P('sp'), may hold values from 0.2 to 1
- expert_gate: bfloat16 [8, 2048, 2816], P('sp', None, 'tp'), may hold values from -0.125 to 0.125
- specialist_widen: bfloat16 [8, 2048, 2816], P('sp', None, 'tp'), may hold values from -0.125 to 0.125
- expert_down: bfloat16 [8, 2816, 2048], P('sp', 'tp'), may hold values from -0.109375 to 0.109375
Outputs:
- layer_out: bfloat16 [2048, 2048], P(('sp', 'tp'))
The draws below stay inside these ranges and needn't reach their ends.
Inputs may be any that keep to these rules, and one draw needn't show every extreme that they name: `routes`: each row names 2 different experts; within each aligned block of 256 rows no expert is named by more than 64 rows, and in every draw some expert is named by exactly 64 rows of some block.
All inputs are finite; a program needn't handle non-finite values.
Results may differ from the reference program's by a relative error of at most 0.02.
Values may be sent and summed in bfloat16 or wider, within the bound.
No kernel may reach another device: no remote copies, remote signals or barrier semaphores. Data moves between devices by JAX's collectives and lax.ppermute only.
A program may use at most 128 MiB of HBM per device.

```python
import math
import jax
import jax.numpy as jnp
import numpy as np
from jax import lax

D = 2048
HEADS = 16
HK = 256
HV = 512
RANK = 16
FF = 2816
TOP = 2
BLK = 128
TOK_DEV = 256
SEQUENCE_LENGTH = 2048
EXPERTS = 8
CAPG = 64
N_SP = 8
N_TP = 4


def draw_decay_bias(key, part):
    key_pick = jax.random.fold_in(key, 11)
    key_slow = jax.random.fold_in(key, 12)
    key_fast = jax.random.fold_in(key, 13)
    fast_heads = jax.random.uniform(key_pick, (HEADS,), jnp.float32) < 0.5
    slow_values = jnp.log(jnp.float32(SEQUENCE_LENGTH)) + 1.0 + jax.random.uniform(key_slow, (HEADS, HK), jnp.float32, 0.0, 1.5)
    fast_values = jax.random.uniform(key_fast, (HEADS, HK), jnp.float32, -0.5, 1.0)
    return jnp.where(fast_heads[:, None], fast_values, slow_values).reshape(HEADS * HK).astype(jnp.float32)


def draw_decay_shift(key, part):
    key_rate = jax.random.fold_in(key, 21)
    key_where = jax.random.fold_in(key, 22)
    key_loss = jax.random.fold_in(key, 23)
    blocks = SEQUENCE_LENGTH // TOK_DEV
    rates = jnp.exp(jax.random.uniform(key_rate, (blocks, HEADS), jnp.float32, jnp.log(0.25), 0.0)) * (-1.5 / SEQUENCE_LENGTH)
    averaging_coefficient = jnp.repeat(rates, TOK_DEV, axis=0)
    places = jax.random.randint(key_where, (2, HEADS), 0, SEQUENCE_LENGTH)
    objective_readings = jnp.log(jax.random.uniform(key_loss, (2, HEADS), jnp.float32, 0.5, 0.8))
    positions = jnp.arange(SEQUENCE_LENGTH, dtype=jnp.int32)
    overflow_entries = (positions[:, None, None] == places[None, :, :]).astype(jnp.float32)
    cluster_batches = jnp.sum(overflow_entries * objective_readings[None, :, :], axis=1)
    return (averaging_coefficient + cluster_batches).astype(jnp.float32)


def steps_of(stream_key, shape, cuts, smallest, high):
    level = 1.0
    for dim, blocks in cuts:
        steps = jax.random.uniform(jax.random.fold_in(jax.random.fold_in(stream_key, 6), dim), (blocks,), jnp.float32, smallest / len(cuts), high / len(cuts))
        level = level * jnp.repeat(jnp.exp(steps), shape[dim] // blocks).reshape((-1,) + (1,) * (len(shape) - 1 - dim))
    return level


def assign_block(own_key, own, number, rows, amount, top, bound, skew):
    ranking = jax.random.permutation(own_key, amount)
    crowded, usual = portions_of(amount, rows * top, bound, skew, True), portions_of(amount, rows * top, bound, skew, False)
    places = jnp.arange(amount)

    def named(tallies, offset_by):
        used = int((tallies > 0).sum())
        fixed = max(1, used // 4)
        moved = fixed + (places - fixed + offset_by * (used - fixed)) % max(1, amount - fixed)
        return jnp.zeros((amount,), jnp.int32).at[ranking[jnp.where(places < fixed, places, moved)]].set(jnp.asarray(tallies, jnp.int32))

    tallies = jnp.where(number % 4 == 0, named(crowded, number // 4), named(usual, number - number // 4 - 1))
    mixed = jax.random.permutation(jax.random.fold_in(own, 3), amount)
    source_of, receiver = mixed[0:amount // 2 * 2:2], mixed[1:amount // 2 * 2:2]
    slack = jnp.minimum(tallies[source_of] - 1, bound - tallies[receiver]) // 2
    slack = jnp.where((source_of == ranking[0]) | (receiver == ranking[0]) | (tallies[receiver] == 0), 0, jnp.maximum(slack, 0))
    moved = jax.random.randint(jax.random.fold_in(own, 4), (amount // 2,), 0, 1 << 20) % (slack + 1)
    tallies = tallies.at[source_of].add(-moved).at[receiver].add(moved)
    members = jnp.searchsorted(jnp.cumsum(tallies), jnp.arange(rows * top), side="right").astype(jnp.int32)
    grid = members.reshape(top, rows).T
    grid = grid[jax.random.permutation(jax.random.fold_in(own, 1), rows)]
    offset_by = jax.random.randint(jax.random.fold_in(own, 2), (rows, 1), 0, top)
    return jnp.take_along_axis(grid, (jnp.arange(top)[None, :] + offset_by) % top, axis=1)


def portions_of(number_of, total, reach, skew, full):
    weights = [(1 << 20) // math.isqrt(rank ** skew) + 1 for rank in range(1, number_of + 1)]
    largest = reach if full else min(reach, max(-(-total // number_of), total * weights[0] // sum(weights)))
    least = 1 if total - largest >= number_of - 1 else 0
    given, surplus = [largest] + [least] * (number_of - 1), total - largest - least * (number_of - 1)
    while surplus > 0:
        free = [i for i in range(1, number_of) if given[i] < largest] or [i for i in range(1, number_of) if given[i] < reach]
        whole, remaining = sum([weights[i] for i in free]), surplus
        for i in free:
            more = min(reach - given[i], max(1, remaining * weights[i] // whole), surplus)
            given[i] = given[i] + more
            surplus = surplus - more
    return np.array(given)


def normal_values(own_key, shape, spread, most, shards=(), held_as=jnp.bfloat16):
    drawn = jax.random.normal(own_key, shape, jnp.float32) * spread
    if len(shards) > 0:
        drawn = steps_of(own_key, shape, shards, -0.22, 0.18) * drawn
    return jnp.clip(drawn, min=-most, max=most).astype(held_as)


def setup_inputs(seed: int = 0) -> dict:
    splits = jax.random.split(jax.random.key(seed), 17)
    stream_in = normal_values(splits[0], (SEQUENCE_LENGTH, D), 1.0, 6.0, ((0, 32),))
    queries = normal_values(splits[1], (SEQUENCE_LENGTH, HEADS * HK), 1.0, 6.0, ((0, 8), (1, 4)))
    key_rows = normal_values(splits[2], (SEQUENCE_LENGTH, HEADS * HK), 1.0, 6.0, ((0, 8), (1, 4)))
    values = normal_values(splits[3], (SEQUENCE_LENGTH, HEADS * HV), 1.0, 6.0, ((0, 8), (1, 4)))
    decay_low = normal_values(splits[4], (SEQUENCE_LENGTH, RANK), 1.0, 4.0, ((0, 8),))
    decay_matrix = normal_values(splits[5], (RANK, HEADS * HK), RANK ** -0.5, 1.5, ((1, 4),))
    decay_bias = draw_decay_bias(jax.random.fold_in(splits[16], 71), 0)
    decay_shift = draw_decay_shift(jax.random.fold_in(splits[16], 71), 0)
    head_gain = jnp.clip(1.0 + 0.18 * jax.random.normal(splits[8], (HV,), jnp.float32), 0.1, 1.9)
    output_matrix = normal_values(splits[9], (HEADS * HV, D), (HEADS * HV) ** -0.5, 0.0625, ((0, 4),))
    feed_gain = jnp.clip(1.0 + 0.18 * jax.random.normal(splits[10], (D,), jnp.float32), 0.1, 1.9)
    routes_keys = jax.random.split(jax.random.fold_in(splits[11], 1), SEQUENCE_LENGTH // TOK_DEV)
    routes_turns = jax.random.permutation(jax.random.fold_in(splits[11], 3), SEQUENCE_LENGTH // TOK_DEV)
    routes = jax.vmap(lambda own, number: assign_block(jax.random.fold_in(splits[11], 2), own, number, TOK_DEV, EXPERTS, TOP, CAPG, 0))(routes_keys, routes_turns).reshape((SEQUENCE_LENGTH, TOP))
    route_weights = jnp.clip(0.2 + 0.8 * jax.random.uniform(splits[12], (SEQUENCE_LENGTH, TOP), jnp.float32) ** steps_of(splits[12], (SEQUENCE_LENGTH, TOP), ((0, 8),), -0.2, 0.2), 0.2, 1.0)
    expert_gate = normal_values(splits[13], (EXPERTS, D, FF), D ** -0.5, 0.125, ((0, 8), (2, 4)))
    specialist_widen = normal_values(splits[14], (EXPERTS, D, FF), D ** -0.5, 0.125, ((0, 8), (2, 4)))
    expert_down = normal_values(splits[15], (EXPERTS, FF, D), FF ** -0.5, 0.109375, ((0, 8), (1, 4)))
    return {"stream_in": stream_in, "queries": queries, "key_rows": key_rows, "values": values, "decay_low": decay_low, "decay_matrix": decay_matrix, "decay_bias": decay_bias, "decay_shift": decay_shift, "head_gain": head_gain, "output_matrix": output_matrix, "feed_gain": feed_gain, "routes": routes, "route_weights": route_weights, "expert_gate": expert_gate, "specialist_widen": specialist_widen, "expert_down": expert_down}


TEMPER = 16.0
EPSILON = 1e-06
HIGHEST = lax.Precision.HIGHEST

def decay_logs(decay_low, decay_matrix, decay_bias, decay_shift, heads):
    before_gate = jnp.dot(decay_low, decay_matrix, preferred_element_type=jnp.float32) + decay_bias
    logged = jax.nn.log_sigmoid(before_gate) / TEMPER
    return logged.reshape(before_gate.shape[0], heads, HK) + decay_shift[:, :, None]

def into_blocks(array):
    length, heads, width = array.shape
    return array.reshape(length // BLK, BLK, heads, width).transpose(2, 0, 1, 3)

def segment_summands(queries, key_rows, values, log_decay):
    inside = jnp.cumsum(log_decay, axis=2)
    final_position = inside[:, :, -1:, :]
    scaled_query = queries * jnp.exp(inside) * HK ** (-0.5)
    scaled_key = key_rows * jnp.exp(-inside)
    end_keys = key_rows * jnp.exp(final_position - inside)
    scores = jnp.einsum('hnid,hnjd->hnij', scaled_query, scaled_key, precision=HIGHEST)
    causal = jnp.tril(jnp.ones((BLK, BLK), jnp.bool_))
    scores = jnp.where(causal, scores, 0.0)
    local_out = jnp.einsum('hnij,hnjv->hniv', scores, values, precision=HIGHEST)
    partial_update = jnp.einsum('hnjd,hnjv->hndv', end_keys, values, precision=HIGHEST)
    return (scaled_query, local_out, partial_update, jnp.exp(final_position[:, :, 0, :]))

def run_blocks(scaled_query, partial_update, block_decay, start):

    def advance(state, pieces):
        query_block, added, decay = pieces
        output = jnp.einsum('hid,hdv->hiv', query_block, state, precision=HIGHEST)
        return (state * decay[:, :, None] + added, output)
    final, outputs = lax.scan(advance, start, (jnp.moveaxis(scaled_query, 1, 0), jnp.moveaxis(partial_update, 1, 0), jnp.moveaxis(block_decay, 1, 0)))
    return (final, jnp.moveaxis(outputs, 0, 1))

def head_norm(heads_out, head_gain):
    heads = heads_out.shape[0]
    flat = heads_out.transpose(1, 2, 0, 3).reshape(-1, heads, HV)
    normed = flat * lax.rsqrt(lax.optimization_barrier(jnp.mean(flat * flat, axis=-1, keepdims=True)) + EPSILON) * head_gain
    return normed.reshape(-1, heads * HV).astype(jnp.bfloat16)

def root_scale(midstream, gain):
    return (midstream * lax.rsqrt(lax.optimization_barrier(jnp.mean(midstream * midstream, axis=-1, keepdims=True)) + EPSILON) * gain).astype(jnp.bfloat16)

def reference(stream_in, queries, key_rows, values, decay_low, decay_matrix, decay_bias, decay_shift, head_gain, output_matrix, feed_gain, routes, route_weights, expert_gate, specialist_widen, expert_down):
    log_decay = decay_logs(decay_low, decay_matrix, decay_bias, decay_shift, HEADS)

    def shaped(array, width):
        return into_blocks(array.astype(jnp.float32).reshape(SEQUENCE_LENGTH, HEADS, width))
    scaled_query, local_out, partial_update, block_decay = segment_summands(shaped(queries, HK), shaped(key_rows, HK), shaped(values, HV), into_blocks(log_decay))
    start = jnp.zeros((HEADS, HK, HV), jnp.float32)
    _, carried_out = run_blocks(scaled_query, partial_update, block_decay, start)
    mixed = head_norm(local_out + carried_out, head_gain)
    group_width = HEADS * HV // N_TP
    mixed_groups = mixed.reshape(SEQUENCE_LENGTH, N_TP, group_width).transpose(1, 0, 2)
    matrix_groups = output_matrix.reshape(N_TP, group_width, D)

    def group_step(total, inputs):
        rows_group, matrix_group = inputs
        product = jnp.dot(rows_group, matrix_group, preferred_element_type=jnp.float32)
        rounded = lax.optimization_barrier(product.astype(jnp.bfloat16))
        return (total + rounded.astype(jnp.float32), None)
    attended, _ = lax.scan(group_step, jnp.zeros((SEQUENCE_LENGTH, D), jnp.float32), (mixed_groups, matrix_groups))
    midstream = stream_in.astype(jnp.float32) + attended
    normed = root_scale(midstream, feed_gain)
    slots = N_SP * CAPG
    flat_routes = routes.reshape(-1)
    flat_weights = route_weights.reshape(-1)
    piece = FF // N_TP

    def expert_step(total, inputs):
        expert, gate_matrix, up_matrix, down_projection_weight = inputs
        matches = flat_routes == expert
        chosen = jnp.nonzero(matches, size=slots, fill_value=0)[0].astype(jnp.int32)
        live = (jnp.arange(slots, dtype=jnp.int32) < jnp.sum(matches.astype(jnp.int32))).astype(jnp.float32)
        token_index = chosen // TOP
        picked = normed[token_index]
        gated = jnp.dot(picked, gate_matrix, preferred_element_type=jnp.float32)
        lifted = jnp.dot(picked, up_matrix, preferred_element_type=jnp.float32)
        hidden = (jax.nn.silu(gated) * lifted).astype(jnp.bfloat16)
        pieces = jnp.einsum('rpf,pfd->prd', hidden.reshape(slots, N_TP, piece).astype(jnp.float32), down_projection_weight.reshape(N_TP, piece, D).astype(jnp.float32))
        rounded = lax.optimization_barrier(pieces.astype(jnp.bfloat16))
        expert_token_rows = lax.optimization_barrier(jnp.sum(rounded.astype(jnp.float32), axis=0)).astype(jnp.bfloat16)
        term = expert_token_rows.astype(jnp.float32) * (flat_weights[chosen] * live)[:, None]
        return (total.at[token_index].add(term), None)
    routed, _ = lax.scan(expert_step, jnp.zeros((SEQUENCE_LENGTH, D), jnp.float32), (jnp.arange(EXPERTS, dtype=jnp.int32), expert_gate, specialist_widen, expert_down))
    return (midstream + routed).astype(jnp.bfloat16)
```

```python
import functools
import jax
import jax.numpy as jnp
from jax import lax
from jax.experimental import pallas as pl
from jax.experimental.pallas import tpu as pltpu
from jax.sharding import PartitionSpec as P

HK = 256
HV = 512
TOP = 2
BLK = 128
TEMPER = 16.0
EPSILON = 1e-06
HIGHEST = lax.Precision.HIGHEST
F32 = jnp.float32
BF16 = jnp.bfloat16
VMEM = pl.BlockSpec(memory_space=pltpu.VMEM)
SMEM = pl.BlockSpec(memory_space=pltpu.SMEM)


def cost(flops, moved):
    return pl.CostEstimate(flops=int(flops), bytes_accessed=int(moved), transcendentals=0)


def params(mib):
    return pltpu.CompilerParams(vmem_limit_bytes=mib * 1024 * 1024)


def xor_perm(axis, k):
    return [(i, i ^ k) for i in range(lax.axis_size(axis))]


def swap(value, axis, k):
    return lax.ppermute(value, axis, xor_perm(axis, k))


def tri(n, fn):
    row = lax.broadcasted_iota(jnp.int32, (n, n), 0)
    col = lax.broadcasted_iota(jnp.int32, (n, n), 1)
    return fn(row, col)


def head_log_decay(low, matrix, bias, shift, head):
    pre = jnp.dot(low, matrix, preferred_element_type=F32) + bias
    logged = (jnp.minimum(pre, 0.0) - jnp.log1p(jnp.exp(-jnp.abs(pre)))) / TEMPER
    lane = lax.broadcasted_iota(jnp.int32, shift.shape, 1)
    return logged + jnp.sum(jnp.where(lane == head, shift, 0.0), axis=1, keepdims=True)


def contract0(a, b):
    return lax.dot_general(a, b, (((0,), (0,)), ((), ())), preferred_element_type=F32)


def contract1(a, b):
    return lax.dot_general(a, b, (((1,), (1,)), ((), ())), preferred_element_type=F32)


def state_kernel(n, heads, idx, low, matrix, bias, shift, key_rows, values, *rest):
    outs, (state, decays) = rest[:n], rest[n:]
    head = pl.program_id(0)
    length = low.shape[0]
    piece = HK // n
    logs = head_log_decay(low[...], matrix[...], bias[...], shift[...], head)
    after = tri(length, lambda r, c: c > r).astype(F32)
    suffix = jnp.dot(after, logs, precision=HIGHEST, preferred_element_type=F32)
    end_keys = (key_rows[...].astype(F32) * jnp.exp(suffix)).astype(BF16)
    state[...] = contract0(end_keys, values[...])
    total = jnp.exp(suffix[0:1, :] + logs[0:1, :])
    high = total.astype(BF16).astype(F32)

    @pl.when(head == 0)
    def _():
        decays[...] = jnp.zeros_like(decays)

    decays[pl.ds(head, 1), 0:HK] = high
    decays[pl.ds(head, 1), HK : 2 * HK] = total - high
    me = idx[0]
    at = 0 if heads == 1 else pl.multiple_of(head * piece, piece)
    for k in range(n):
        start = pl.multiple_of((me ^ k) * piece, piece)
        outs[k][pl.ds(at, piece), :] = state[pl.ds(start, piece), :].astype(BF16)

    @pl.when(head == heads - 1)
    def _():
        for k in range(n):
            outs[k][heads * piece :, :] = decays[...].astype(BF16)


def device_states(n, heads, idx, low, matrix, bias, shift, key_rows, values):
    length = low.shape[0]
    rows = heads * (HK // n) + 8
    return pl.pallas_call(
        functools.partial(state_kernel, n, heads),
        grid=(heads,),
        in_specs=[
            SMEM,
            pl.BlockSpec((length, low.shape[1]), lambda h: (0, 0)),
            pl.BlockSpec((low.shape[1], HK), lambda h: (0, h)),
            pl.BlockSpec((1, HK), lambda h: (0, h)),
            pl.BlockSpec((length, heads), lambda h: (0, 0)),
            pl.BlockSpec((length, HK), lambda h: (0, h)),
            pl.BlockSpec((length, HV), lambda h: (0, h)),
        ],
        out_specs=[pl.BlockSpec((rows, HV), lambda h: (0, 0))] * n,
        out_shape=[jax.ShapeDtypeStruct((rows, HV), BF16)] * n,
        scratch_shapes=[pltpu.VMEM((HK, HV), F32), pltpu.VMEM((8, HV), F32)],
        compiler_params=params(24),
        cost_estimate=cost(heads * 4e8, heads * 5e5),
        name="device_states",
    )(idx, low, matrix, bias, shift, key_rows, values)


def local_kernel(low, matrix, bias, shift, queries, key_rows, values, out, query_out):
    head = pl.program_id(0)
    length = low.shape[0]
    logs = head_log_decay(low[...], matrix[...], bias[...], shift[...], head)
    below = tri(BLK, lambda r, c: c <= r)
    lower = below.astype(F32)
    scale = HK ** (-0.5)
    before = jnp.zeros((1, HK), F32)
    earlier = []
    for b in range(length // BLK):
        rows = slice(b * BLK, (b + 1) * BLK)
        inside = jnp.dot(lower, logs[rows], precision=HIGHEST, preferred_element_type=F32)
        final = inside[BLK - 1 : BLK, :]
        middle = inside[BLK // 2 - 1 : BLK // 2, :]
        query = queries[rows, :].astype(F32) * scale
        keys = key_rows[rows, :].astype(F32)
        grown = query * jnp.exp(inside)
        near_query = (query * jnp.exp(inside - middle)).astype(BF16)
        near_key = (keys * jnp.exp(middle - inside)).astype(BF16)
        scores = jnp.where(below, contract1(near_query, near_key), 0.0).astype(BF16)
        total = jnp.dot(scores, values[rows, :], preferred_element_type=F32)
        here = grown.astype(BF16)
        for past_keys, past_rows in earlier:
            cross = contract1(here, past_keys.astype(BF16)).astype(BF16)
            total = total + jnp.dot(cross, values[past_rows, :], preferred_element_type=F32)
        out[rows, :] = total
        query_out[rows, :] = (grown * jnp.exp(before)).astype(BF16)
        earlier = [(old * jnp.exp(final), old_rows) for old, old_rows in earlier]
        earlier.append((keys * jnp.exp(final - inside), rows))
        before = before + final


def local_attention(heads, low, matrix, bias, shift, queries, key_rows, values):
    length = low.shape[0]
    return pl.pallas_call(
        local_kernel,
        grid=(heads,),
        in_specs=[
            pl.BlockSpec((length, low.shape[1]), lambda h: (0, 0)),
            pl.BlockSpec((low.shape[1], HK), lambda h: (0, h)),
            pl.BlockSpec((1, HK), lambda h: (0, h)),
            pl.BlockSpec((length, heads), lambda h: (0, 0)),
            pl.BlockSpec((length, HK), lambda h: (0, h)),
            pl.BlockSpec((length, HK), lambda h: (0, h)),
            pl.BlockSpec((length, HV), lambda h: (0, h)),
        ],
        out_specs=[
            pl.BlockSpec((length, HV), lambda h: (0, h)),
            pl.BlockSpec((length, HK), lambda h: (0, h)),
        ],
        out_shape=[
            jax.ShapeDtypeStruct((length, heads * HV), F32),
            jax.ShapeDtypeStruct((length, heads * HK), BF16),
        ],
        compiler_params=params(24),
        cost_estimate=cost(heads * 4e8, heads * 1.2e6),
        name="local_attention",
    )(low, matrix, bias, shift, queries, key_rows, values)


def prefix_kernel(n, heads, idx, *refs):
    ins, outs, (stage, decays, result) = refs[:n], refs[n : 2 * n], refs[2 * n :]
    me = idx[0]
    piece = HK // n
    rows = heads * piece
    for k in range(n):
        stage[me ^ k] = ins[k][:rows, :].astype(F32)
        tail = ins[k][rows:, :].astype(F32)
        decays[me ^ k] = jnp.transpose(tail[:, :HK] + tail[:, HK:])
    mine = pl.multiple_of(me * piece, piece)
    for head in range(heads):
        span = slice(head * piece, (head + 1) * piece)
        carry = jnp.zeros((piece, HV), F32)
        for i in range(n):
            result[i, span, :] = carry
            factor = decays[i, pl.ds(mine, piece), head : head + 1]
            carry = carry * factor + stage[i, span, :]
    for k in range(n):
        outs[k][...] = result[me ^ k].astype(BF16)


def carried_pieces(n, heads, idx, pieces):
    rows = heads * (HK // n)
    return pl.pallas_call(
        functools.partial(prefix_kernel, n, heads),
        in_specs=[SMEM] + [VMEM] * n,
        out_specs=[VMEM] * n,
        out_shape=[jax.ShapeDtypeStruct((rows, HV), BF16)] * n,
        scratch_shapes=[
            pltpu.VMEM((n, rows, HV), F32),
            pltpu.VMEM((n, HK, 8), F32),
            pltpu.VMEM((n, rows, HV), F32),
        ],
        compiler_params=params(24),
        cost_estimate=cost(1e8, 2e6),
        name="carried_pieces",
    )(idx, *pieces)


def project_kernel(n, heads, groups, idx, queries, local, gain, matrix, *refs):
    pieces, (keep, send), (carried, total) = refs[:n], refs[n : n + 2], refs[n + 2 :]
    head = pl.program_id(0)
    me, core, line = idx[0], idx[1], idx[2]
    piece = HK // n

    @pl.when(head == 0)
    def _():
        total[...] = jnp.zeros_like(total)
        for k in range(n):
            start = pl.multiple_of((me ^ k) * piece, piece)
            for h in range(heads):
                span = slice(h * piece, (h + 1) * piece)
                carried[h, pl.ds(start, piece), :] = pieces[k][span, :].astype(F32)

    out = local[...] + jnp.dot(
        queries[...], carried[head].astype(BF16), preferred_element_type=F32
    )
    spread = lax.rsqrt(jnp.mean(out * out, axis=-1, keepdims=True) + EPSILON)
    mixed = (out * spread * gain[...]).astype(BF16)
    total[...] += jnp.dot(mixed, matrix[...], preferred_element_type=F32)

    @pl.when(head == heads - 1)
    def _():
        rows = keep.shape[0] // groups
        for k in range(groups):
            span = slice(k * rows, (k + 1) * rows)
            base = (line ^ k) * 2
            own = pl.multiple_of((base + core) * rows, rows)
            other = pl.multiple_of((base + 1 - core) * rows, rows)
            keep[span, :] = total[pl.ds(own, rows), :]
            send[span, :] = total[pl.ds(other, rows), :].astype(BF16)


def project(n, heads, groups, idx, queries, local, gain, matrix, pieces):
    length = queries.shape[0]
    width = matrix.shape[1]
    rows = heads * (HK // n)
    return pl.pallas_call(
        functools.partial(project_kernel, n, heads, groups),
        grid=(heads,),
        in_specs=[
            SMEM,
            pl.BlockSpec((length, HK), lambda h: (0, h)),
            pl.BlockSpec((length, HV), lambda h: (0, h)),
            pl.BlockSpec((1, HV), lambda h: (0, 0)),
            pl.BlockSpec((HV, width), lambda h: (h, 0)),
        ]
        + [pl.BlockSpec((rows, HV), lambda h: (0, 0))] * n,
        out_specs=[pl.BlockSpec((length // 2, width), lambda h: (0, 0))] * 2,
        out_shape=[
            jax.ShapeDtypeStruct((length // 2, width), F32),
            jax.ShapeDtypeStruct((length // 2, width), BF16),
        ],
        scratch_shapes=[
            pltpu.VMEM((heads, HK, HV), F32),
            pltpu.VMEM((length, width), F32),
        ],
        compiler_params=params(32),
        cost_estimate=cost(heads * 7e8, heads * 2.5e6),
        name="project",
    )(idx, queries, local, gain, matrix, *pieces)


def norm_kernel(groups, gain, keep, received, *refs):
    streams, arrived = refs[:groups], refs[groups : 2 * groups - 1]
    normed, mid = refs[2 * groups - 1 :]
    rows = mid.shape[0]
    for k in range(groups):
        span = slice(k * rows, (k + 1) * rows)
        value = keep[span, :] + received[span, :].astype(F32)
        for j in range(1, groups):
            there = k ^ j
            value = value + arrived[j - 1][there * rows : (there + 1) * rows, :].astype(F32)
        value = value + streams[k][...].astype(F32)
        if k == 0:
            mid[...] = value
        spread = lax.rsqrt(jnp.mean(value * value, axis=-1, keepdims=True) + EPSILON)
        normed[span, :] = (value * spread * gain[...]).astype(BF16)


def midstream_norm(groups, gain, keep, received, streams, arrived):
    rows, width = streams[0].shape
    return pl.pallas_call(
        functools.partial(norm_kernel, groups),
        in_specs=[VMEM] * (3 + 2 * groups - 1),
        out_specs=[VMEM] * 2,
        out_shape=[
            jax.ShapeDtypeStruct((groups * rows, width), BF16),
            jax.ShapeDtypeStruct((rows, width), F32),
        ],
        compiler_params=params(24),
        cost_estimate=cost(1e7, 3e6),
        name="midstream_norm",
    )(gain, keep, received, *streams, *arrived)


def route_kernel(n, groups, half, idx, routes, weights, select, high, low):
    me, core, line = idx[0], idx[1], idx[2]
    length = routes.shape[1]
    rows = length // (2 * groups)
    this_device = line * 2 + core

    def position(r):
        block = r // rows
        relative = jnp.where(block < groups, 2 * block, 2 * (block - groups) + 1)
        return (relative ^ this_device) * rows + r % rows

    earlier = tri(length, lambda r, c: position(r) < position(c)).astype(BF16)
    first, second = routes[0:1, :], routes[1:2, :]
    expert = me ^ lax.broadcasted_iota(jnp.int32, (n, length), 0)
    is_first, is_second = first == expert, second == expert
    member = jnp.where(is_first | is_second, 1.0, 0.0)
    rank = jnp.dot(member.astype(BF16), earlier, preferred_element_type=F32)
    slot = jnp.where(member > 0.0, rank.astype(jnp.int32), -1)
    weight = jnp.where(is_first, weights[0:1, :], weights[1:2, :])
    for k in range(n):
        wanted = core * half + lax.broadcasted_iota(jnp.int32, (half, length), 0)
        hit = slot[k : k + 1, :] == wanted
        span = slice(k * half, (k + 1) * half)
        select[span, :] = jnp.where(hit, 1.0, 0.0).astype(BF16)
        value = jnp.where(hit, weight[k : k + 1, :], 0.0)
        top = value.astype(BF16)
        high[span, :] = top
        low[span, :] = (value - top.astype(F32)).astype(BF16)


def slot_tables(n, groups, half, idx, routes, weights):
    length = routes.shape[1]
    return pl.pallas_call(
        functools.partial(route_kernel, n, groups, half),
        in_specs=[SMEM, VMEM, VMEM],
        out_specs=[VMEM] * 3,
        out_shape=[jax.ShapeDtypeStruct((n * half, length), BF16)] * 3,
        compiler_params=params(24),
        cost_estimate=cost(1e8, 5e5),
        name="slot_tables",
    )(idx, routes, weights)


def dispatch_kernel(n, half, select, mine, theirs, *outs):
    split = mine.shape[0]
    picked = jnp.dot(select[:, :split], mine[...], preferred_element_type=F32)
    picked = picked + jnp.dot(select[:, split:], theirs[...], preferred_element_type=F32)
    for k in range(n):
        outs[k][...] = picked[k * half : (k + 1) * half, :].astype(BF16)


def dispatch(n, half, select, mine, theirs):
    width = mine.shape[1]
    return pl.pallas_call(
        functools.partial(dispatch_kernel, n, half),
        in_specs=[VMEM] * 3,
        out_specs=[VMEM] * n,
        out_shape=[jax.ShapeDtypeStruct((half, width), BF16)] * n,
        compiler_params=params(24),
        cost_estimate=cost(5e8, 2e6),
        name="dispatch",
    )(select, mine, theirs)


def expert_kernel(n, gate, widen, down, *refs):
    ins, (keep, send) = refs[: 2 * n], refs[2 * n :]
    half = ins[0].shape[0]
    for part, out in ((0, send), (1, keep)):
        group = ins[n:] if part == 0 else ins[:n]
        rows = jnp.concatenate([piece[...] for piece in group], axis=0)
        gated = jnp.dot(rows, gate[0], preferred_element_type=F32)
        lifted = jnp.dot(rows, widen[0], preferred_element_type=F32)
        hidden = (gated * jax.nn.sigmoid(gated) * lifted).astype(BF16)
        out[...] = jnp.dot(hidden, down[0], preferred_element_type=F32).astype(out.dtype)


def expert(n, gate, widen, down, mine, theirs):
    half, width = mine[0].shape
    return pl.pallas_call(
        functools.partial(expert_kernel, n),
        in_specs=[VMEM] * (3 + 2 * n),
        out_specs=[VMEM] * 2,
        out_shape=[
            jax.ShapeDtypeStruct((n * half, width), F32),
            jax.ShapeDtypeStruct((n * half, width), BF16),
        ],
        compiler_params=params(40),
        cost_estimate=cost(5e9, 1.2e7),
        name="expert",
    )(gate, widen, down, *mine, *theirs)


def merge_kernel(n, keep, received, *outs):
    half = outs[0].shape[0]
    for k in range(n):
        span = slice(k * half, (k + 1) * half)
        outs[k][...] = (keep[span, :] + received[span, :].astype(F32)).astype(BF16)


def merge(n, half, keep, received):
    width = keep.shape[1]
    return pl.pallas_call(
        functools.partial(merge_kernel, n),
        in_specs=[VMEM] * 2,
        out_specs=[VMEM] * n,
        out_shape=[jax.ShapeDtypeStruct((half, width), BF16)] * n,
        compiler_params=params(24),
        cost_estimate=cost(1e7, 4e6),
        name="merge",
    )(keep, received)


def combine_kernel(n, high, low, *refs):
    ins, (keep, send) = refs[:n], refs[n:]
    rows = jnp.concatenate([piece[...] for piece in ins], axis=0)
    total = contract0(high[...], rows) + contract0(low[...], rows)
    split = keep.shape[0]
    keep[...] = total[:split, :]
    send[...] = total[split:, :].astype(BF16)


def combine(n, high, low, pieces):
    width = pieces[0].shape[1]
    length = high.shape[1]
    return pl.pallas_call(
        functools.partial(combine_kernel, n),
        in_specs=[VMEM] * (2 + n),
        out_specs=[VMEM] * 2,
        out_shape=[
            jax.ShapeDtypeStruct((length // 2, width), F32),
            jax.ShapeDtypeStruct((length // 2, width), BF16),
        ],
        compiler_params=params(24),
        cost_estimate=cost(1e9, 3e6),
        name="combine",
    )(high, low, *pieces)


def exchange(pieces, axis):
    return [pieces[0]] + [swap(pieces[k], axis, k) for k in range(1, len(pieces))]


def body(
    stream_in,
    queries,
    key_rows,
    values,
    decay_low,
    decay_matrix,
    decay_bias,
    decay_shift,
    head_gain,
    output_matrix,
    feed_gain,
    routes,
    route_weights,
    expert_gate,
    specialist_widen,
    expert_down,
):
    length = queries.shape[0]
    heads = queries.shape[1] // HK
    n = lax.axis_size("sp")
    head_devices = lax.axis_size("tp")
    groups = head_devices // 2
    me, tp = lax.axis_index("sp"), lax.axis_index("tp")
    core, line = tp % 2, tp // 2
    idx = jnp.stack([me, core, line]).astype(jnp.int32)
    rows = length // head_devices
    half = TOP * length // n // 2
    bias = decay_bias.reshape(1, -1)

    streams = [stream_in] + [swap(stream_in, "tp", 2 * k) for k in range(1, groups)]
    pieces = device_states(
        n, heads, idx, decay_low, decay_matrix, bias, decay_shift, key_rows, values
    )
    gathered = exchange(pieces, "sp")
    local, late_queries = local_attention(
        heads, decay_low, decay_matrix, bias, decay_shift, queries, key_rows, values
    )
    order = [2 * k for k in range(groups)] + [2 * k + 1 for k in range(groups)]
    blocks = tp ^ jnp.array(order, jnp.int32)

    def relative(array):
        return array.reshape(head_devices, rows, TOP)[blocks].reshape(length, TOP).T

    select, high, low = slot_tables(
        n, groups, half, idx, relative(routes), relative(route_weights)
    )
    carried = exchange(carried_pieces(n, heads, idx, gathered), "sp")
    keep, send = project(
        n,
        heads,
        groups,
        idx,
        late_queries,
        local,
        head_gain.reshape(1, -1),
        output_matrix,
        carried,
    )
    received = swap(send, "tp", 1)
    shared = (keep + received.astype(F32)).astype(BF16)
    arrived = [swap(shared, "tp", 2 * k) for k in range(1, groups)]
    normed, mid = midstream_norm(
        groups, feed_gain.reshape(1, -1), keep, received, streams, arrived
    )
    slots = exchange(dispatch(n, half, select, normed, swap(normed, "tp", 1)), "sp")
    other_slots = [swap(piece, "tp", 1) for piece in slots]
    kept, sent = expert(n, expert_gate, specialist_widen, expert_down, slots, other_slots)
    back = exchange(merge(n, half, kept, swap(sent, "tp", 1)), "sp")
    keep, send = combine(n, high, low, back)
    summed = keep + swap(send, "tp", 1).astype(F32)
    total = mid + summed[:rows]
    for k in range(1, groups):
        part = summed[k * rows : (k + 1) * rows].astype(BF16)
        total = total + swap(part, "tp", 2 * k).astype(F32)
    return total.astype(BF16)


def solution(mesh):
    return jax.shard_map(
        body,
        mesh=mesh,
        in_specs=(
            P(("sp", "tp"), None),
            P("sp", "tp"),
            P("sp", "tp"),
            P("sp", "tp"),
            P("sp", None),
            P(None, "tp"),
            P("tp"),
            P("sp", "tp"),
            P(),
            P("tp", None),
            P(),
            P("sp", None),
            P("sp", None),
            P("sp", None, "tp"),
            P("sp", None, "tp"),
            P("sp", "tp", None),
        ),
        out_specs=P(("sp", "tp"), None),
        check_vma=False,
    )
```

```python
import functools
import jax
import jax.numpy as jnp
from jax import lax
from jax.experimental import pallas as pl
from jax.experimental.pallas import tpu as pltpu
from jax.sharding import PartitionSpec as P


HK = 256
HV = 512
TOP = 2
BLK = 128
TEMPER = 16.0
EPSILON = 1e-06
F32 = jnp.float32
BF16 = jnp.bfloat16
VMEM = pl.BlockSpec(memory_space=pltpu.VMEM)
SMEM = pl.BlockSpec(memory_space=pltpu.SMEM)
HBM = pl.BlockSpec(memory_space=pltpu.HBM)
QUAD = 4


def cost(flops, moved):
    return pl.CostEstimate(flops=int(flops), bytes_accessed=int(moved), transcendentals=0)


def params(mib):
    return pltpu.CompilerParams(vmem_limit_bytes=mib * 1024 * 1024)


def xor_perm(axis, k):
    return [(i, i ^ k) for i in range(lax.axis_size(axis))]


def tri(n, fn):
    row = lax.broadcasted_iota(jnp.int32, (n, n), 0)
    col = lax.broadcasted_iota(jnp.int32, (n, n), 1)
    return fn(row, col)


def contract0(a, b):
    return lax.dot_general(a, b, (((0,), (0,)), ((), ())), preferred_element_type=F32)


def contract1(a, b):
    return lax.dot_general(a, b, (((1,), (1,)), ((), ())), preferred_element_type=F32)


def split_dot(ones, value):
    total = None
    for _ in range(3):
        part = value.astype(BF16)
        value = value - part.astype(F32)
        term = jnp.dot(ones, part, preferred_element_type=F32)
        total = term if total is None else total + term
    return total


def head_log_decay(low, matrix, bias, shift, head):
    pre = contract0(low, matrix) + bias
    logged = (jnp.minimum(pre, 0.0) - jnp.log1p(jnp.exp(-jnp.abs(pre)))) / TEMPER
    return logged + jnp.transpose(shift)[:, head : head + 1]


def state_kernel(first, count, idx, low, matrix, bias, shift, key_rows, values, *rest):
    outs, (keys, vals, state, decays, sems) = rest[:QUAD], rest[QUAD:]
    length = low.shape[1]
    piece = HK // QUAD
    copies = []
    for h in range(count):
        at = first + h
        pair = (
            pltpu.make_async_copy(
                key_rows.at[:, at * HK : (at + 1) * HK], keys.at[h], sems.at[0, h]
            ),
            pltpu.make_async_copy(
                values.at[:, at * HV : (at + 1) * HV], vals.at[h], sems.at[1, h]
            ),
        )
        for copy in pair:
            copy.start()
        copies.append(pair)
    after = tri(length, lambda r, c: c > r).astype(F32).astype(BF16)
    me = idx[0] % QUAD
    decays[...] = jnp.zeros_like(decays)
    for h in range(count):
        span = slice((first + h) * HK, (first + h + 1) * HK)
        logs = head_log_decay(low[...], matrix[:, span], bias[:, span], shift[...], first + h)
        suffix = split_dot(after, logs)
        total = jnp.exp(suffix[0:1, :] + logs[0:1, :])
        high = total.astype(BF16).astype(F32)
        decays[h : h + 1, 0:HK] = high
        decays[h : h + 1, HK : 2 * HK] = total - high
        for copy in copies[h]:
            copy.wait()
        end_keys = (keys[h].astype(F32) * jnp.exp(suffix)).astype(BF16)
        state[...] = contract0(end_keys, vals[h])
        for k in range(QUAD):
            start = pl.multiple_of((me ^ k) * piece, piece)
            outs[k][h * piece : (h + 1) * piece, :] = state[pl.ds(start, piece), :].astype(BF16)
    for k in range(QUAD):
        outs[k][count * piece :, :] = decays[...].astype(BF16)


def device_states(first, count, idx, low, matrix, bias, shift, key_rows, values):
    length = key_rows.shape[0]
    rows = count * (HK // QUAD) + 8
    return pl.pallas_call(
        functools.partial(state_kernel, first, count),
        in_specs=[SMEM, VMEM, VMEM, VMEM, VMEM, HBM, HBM],
        out_specs=[VMEM] * QUAD,
        out_shape=[jax.ShapeDtypeStruct((rows, HV), BF16)] * QUAD,
        scratch_shapes=[
            pltpu.VMEM((count, length, HK), BF16),
            pltpu.VMEM((count, length, HV), BF16),
            pltpu.VMEM((HK, HV), F32),
            pltpu.VMEM((8, HV), F32),
            pltpu.SemaphoreType.DMA((2, count)),
        ],
        compiler_params=params(60),
        cost_estimate=cost(count * 4e8, count * 5e5),
    )(idx, low, matrix, bias, shift, key_rows, values)


def local_kernel(low, matrix, bias, shift, queries, key_rows, values, out, query_out):
    length = low.shape[1]
    logs = head_log_decay(low[...], matrix[...], bias[...], shift[0], 0)
    below = tri(BLK, lambda r, c: c <= r)
    lower = below.astype(F32).astype(BF16)
    scale = HK ** (-0.5)
    before = jnp.zeros((1, HK), F32)
    earlier = []
    for b in range(length // BLK):
        rows = slice(b * BLK, (b + 1) * BLK)
        inside = split_dot(lower, logs[rows])
        final = inside[BLK - 1 : BLK, :]
        middle = inside[BLK // 2 - 1 : BLK // 2, :]
        query = queries[rows, :].astype(F32) * scale
        keys = key_rows[rows, :].astype(F32)
        grown = query * jnp.exp(inside)
        near_query = (query * jnp.exp(inside - middle)).astype(BF16)
        near_key = (keys * jnp.exp(middle - inside)).astype(BF16)
        scores = jnp.where(below, contract1(near_query, near_key), 0.0).astype(BF16)
        total = jnp.dot(scores, values[rows, :], preferred_element_type=F32)
        here = grown.astype(BF16)
        for past_keys, past_rows in earlier:
            cross = contract1(here, past_keys.astype(BF16)).astype(BF16)
            total = total + jnp.dot(cross, values[past_rows, :], preferred_element_type=F32)
        out[rows, :] = total
        query_out[rows, :] = (grown * jnp.exp(before)).astype(BF16)
        earlier = [(old * jnp.exp(final), old_rows) for old, old_rows in earlier]
        earlier.append((keys * jnp.exp(final - inside), rows))
        before = before + final


def local_attention(heads, low, matrix, bias, shift, queries, key_rows, values):
    length = low.shape[1]
    return pl.pallas_call(
        local_kernel,
        grid=(heads,),
        in_specs=[
            pl.BlockSpec(low.shape, lambda h: (0, 0)),
            pl.BlockSpec((low.shape[0], HK), lambda h: (0, h)),
            pl.BlockSpec((1, HK), lambda h: (0, h)),
            pl.BlockSpec((1, 1, length), lambda h: (h, 0, 0)),
            pl.BlockSpec((length, HK), lambda h: (0, h)),
            pl.BlockSpec((length, HK), lambda h: (0, h)),
            pl.BlockSpec((length, HV), lambda h: (0, h)),
        ],
        out_specs=[
            pl.BlockSpec((length, HV), lambda h: (0, h)),
            pl.BlockSpec((length, HK), lambda h: (0, h)),
        ],
        out_shape=[
            jax.ShapeDtypeStruct((length, heads * HV), F32),
            jax.ShapeDtypeStruct((length, heads * HK), BF16),
        ],
        compiler_params=params(24),
        cost_estimate=cost(heads * 4e8, heads * 1.2e6),
        name="local_attention",
    )(low, matrix, bias, shift.reshape(heads, 1, length), queries, key_rows, values)


def prefix_kernel(count, emit, idx, start, *refs):
    ins, outs, (stage, decays, result) = refs[:QUAD], refs[QUAD:-3], refs[-3:]
    me = idx[0] % QUAD
    piece = HK // QUAD
    rows = count * piece
    for k in range(QUAD):
        stage[me ^ k] = ins[k][:rows, :].astype(F32)
        tail = ins[k][rows:, :].astype(F32)
        decays[me ^ k] = jnp.transpose(tail[:, :HK] + tail[:, HK:])
    mine = pl.multiple_of(me * piece, piece)
    for h in range(count):
        span = slice(h * piece, (h + 1) * piece)
        carry = start[span, :].astype(F32)
        for i in range(QUAD):
            if emit:
                result[i, span, :] = carry
                if i == QUAD - 1:
                    break
            factor = decays[i, pl.ds(mine, piece), h : h + 1]
            carry = carry * factor + stage[i, span, :]
        if not emit:
            outs[0][span, :] = carry.astype(BF16)
    if emit:
        for k in range(QUAD):
            outs[k][...] = result[me ^ k].astype(BF16)


def quad_prefix(count, emit, idx, start, pieces):
    rows = count * (HK // QUAD)
    outs = QUAD if emit else 1
    return pl.pallas_call(
        functools.partial(prefix_kernel, count, emit),
        in_specs=[SMEM] + [VMEM] * (QUAD + 1),
        out_specs=[VMEM] * outs,
        out_shape=[jax.ShapeDtypeStruct((rows, HV), BF16)] * outs,
        scratch_shapes=[
            pltpu.VMEM((QUAD, rows, HV), F32),
            pltpu.VMEM((QUAD, HK, 8), F32),
            pltpu.VMEM((QUAD, rows, HV), F32),
        ],
        compiler_params=params(24),
        cost_estimate=cost(1e8, 1e6),
        name="quad_prefix" if emit else "quad_total",
    )(idx, start, *pieces)


def quad_entry(count, idx, pieces):
    rows = count * (HK // QUAD)
    start = jnp.zeros((rows, HV), BF16)
    quads = lax.axis_size("sp") // QUAD
    entry = None
    for g in range(quads - 1):
        (total,) = quad_prefix(count, False, idx, start, pieces)
        perm = [(g * QUAD + i, (g + 1) * QUAD + i) for i in range(QUAD)]
        start = lax.ppermute(total, "sp", perm)
        entry = start if entry is None else entry + start
    return start if entry is None else entry


def block_spans(idx, groups, rows):
    core, line = idx[1], idx[2]
    for k in range(groups):
        base = (line ^ k) * 2
        own = pl.ds(pl.multiple_of((base + core) * rows, rows), rows)
        other = pl.ds(pl.multiple_of((base + 1 - core) * rows, rows), rows)
        yield slice(k * rows, (k + 1) * rows), own, other


def project_kernel(count, heads, groups, idx, queries, local, gain, matrix, *refs):
    pieces, (keep, send, carried, total) = refs[:-4], refs[-4:]
    head = pl.program_id(0)
    me = idx[0] % QUAD
    piece = HK // QUAD

    @pl.when(head == 0)
    def _():
        total[...] = jnp.zeros_like(total)
        for at, ref in enumerate(pieces):
            start = pl.multiple_of((me ^ (at % QUAD)) * piece, piece)
            for h in range(count):
                span = slice(h * piece, (h + 1) * piece)
                spot = at // QUAD * count + h
                carried[spot, pl.ds(start, piece), :] = ref[span, :].astype(F32)

    out = local[...] + jnp.dot(
        queries[...], carried[head].astype(BF16), preferred_element_type=F32
    )
    spread = lax.rsqrt(jnp.mean(out * out, axis=-1, keepdims=True) + EPSILON)
    mixed = (out * spread * gain[...]).astype(BF16)
    total[...] += jnp.dot(mixed, matrix[...], preferred_element_type=F32)

    @pl.when(head == heads - 1)
    def _():
        for span, own, other in block_spans(idx, groups, keep.shape[0] // groups):
            keep[span, :] = total[own, :]
            send[span, :] = total[other, :].astype(BF16)


def project(count, heads, groups, idx, queries, local, gain, matrix, pieces):
    length = queries.shape[0]
    width = matrix.shape[1]
    rows = count * (HK // QUAD)
    return pl.pallas_call(
        functools.partial(project_kernel, count, heads, groups),
        grid=(heads,),
        in_specs=[
            SMEM,
            pl.BlockSpec((length, HK), lambda h: (0, h)),
            pl.BlockSpec((length, HV), lambda h: (0, h)),
            pl.BlockSpec((1, HV), lambda h: (0, 0)),
            pl.BlockSpec((HV, width), lambda h: (h, 0)),
        ]
        + [pl.BlockSpec((rows, HV), lambda h: (0, 0))] * len(pieces),
        out_specs=[pl.BlockSpec((length // 2, width), lambda h: (0, 0))] * 2,
        out_shape=[
            jax.ShapeDtypeStruct((length // 2, width), F32),
            jax.ShapeDtypeStruct((length // 2, width), BF16),
        ],
        scratch_shapes=[
            pltpu.VMEM((heads, HK, HV), F32),
            pltpu.VMEM((length, width), F32),
        ],
        compiler_params=params(32),
        cost_estimate=cost(heads * 7e8, heads * 2.5e6),
        name="project",
    )(idx, queries, local, gain, matrix, *pieces)


def norm_kernel(groups, gain, keep, received, *refs):
    streams, arrived = refs[:groups], refs[groups : 2 * groups - 1]
    normed, mid = refs[2 * groups - 1 :]
    rows = mid.shape[0]
    for k in range(groups):
        span = slice(k * rows, (k + 1) * rows)
        value = keep[span, :] + received[span, :].astype(F32)
        for j in range(1, groups):
            there = k ^ j
            value = value + arrived[j - 1][there * rows : (there + 1) * rows, :].astype(F32)
        value = value + streams[k][...].astype(F32)
        if k == 0:
            mid[...] = value
        spread = lax.rsqrt(jnp.mean(value * value, axis=-1, keepdims=True) + EPSILON)
        normed[span, :] = (value * spread * gain[...]).astype(BF16)


def midstream_norm(groups, gain, keep, received, streams, arrived):
    rows, width = streams[0].shape
    return pl.pallas_call(
        functools.partial(norm_kernel, groups),
        in_specs=[VMEM] * (3 + 2 * groups - 1),
        out_specs=[VMEM] * 2,
        out_shape=[
            jax.ShapeDtypeStruct((groups * rows, width), BF16),
            jax.ShapeDtypeStruct((rows, width), F32),
        ],
        compiler_params=params(24),
        cost_estimate=cost(1e7, 3e6),
        name="midstream_norm",
    )(gain, keep, received, *streams, *arrived)


def route_kernel(n, half, idx, routes, weights, select, high, low):
    me, core = idx[0], idx[1]
    length = routes.shape[1]
    earlier = tri(length, lambda r, c: r < c).astype(F32).astype(BF16)
    first, second = routes[0:1, :], routes[1:2, :]
    expert = me ^ lax.broadcasted_iota(jnp.int32, (n, length), 0)
    is_first, is_second = first == expert, second == expert
    member = jnp.where(is_first | is_second, 1.0, 0.0)
    rank = jnp.dot(member.astype(BF16), earlier, preferred_element_type=F32)
    slot = jnp.where(member > 0.0, rank.astype(jnp.int32), -1)
    weight = jnp.where(is_first, weights[0:1, :], weights[1:2, :])
    for k in range(n):
        wanted = core * half + lax.broadcasted_iota(jnp.int32, (half, length), 0)
        hit = slot[k : k + 1, :] == wanted
        span = slice(k * half, (k + 1) * half)
        select[span, :] = jnp.where(hit, 1.0, 0.0).astype(BF16)
        value = jnp.where(hit, weight[k : k + 1, :], 0.0)
        top = value.astype(BF16)
        high[span, :] = top
        low[span, :] = (value - top.astype(F32)).astype(BF16)


def slot_tables(n, half, idx, routes, weights):
    length = routes.shape[1]
    return pl.pallas_call(
        functools.partial(route_kernel, n, half),
        in_specs=[SMEM, VMEM, VMEM],
        out_specs=[VMEM] * 3,
        out_shape=[jax.ShapeDtypeStruct((n * half, length), BF16)] * 3,
        compiler_params=params(16),
        cost_estimate=cost(1e8, 5e5),
        name="slot_tables",
    )(idx, routes, weights)


def dispatch_kernel(n, half, groups, idx, select, mine, theirs, *refs):
    outs, group = refs[:n], refs[n]
    rows = mine.shape[0] // groups
    for span, own, other in block_spans(idx, groups, rows):
        group[own, :] = mine[span, :]
        group[other, :] = theirs[span, :]
    for k in range(n):
        chosen = select[k * half : (k + 1) * half, :]
        outs[k][...] = jnp.dot(chosen, group[...], preferred_element_type=F32).astype(BF16)


def dispatch(n, half, groups, idx, select, mine, theirs):
    width = mine.shape[1]
    return pl.pallas_call(
        functools.partial(dispatch_kernel, n, half, groups),
        in_specs=[SMEM] + [VMEM] * 3,
        out_specs=[VMEM] * n,
        out_shape=[jax.ShapeDtypeStruct((half, width), BF16)] * n,
        scratch_shapes=[pltpu.VMEM((select.shape[1], width), BF16)],
        compiler_params=params(16),
        cost_estimate=cost(5e8, 2e6),
        name="dispatch",
    )(idx, select, mine, theirs)


def fetch_kernel(*refs):
    half = (len(refs) - 1) // 2
    ins, outs, sems = refs[:half], refs[half:-1], refs[-1]
    copies = [
        pltpu.make_async_copy(src, dst, sems.at[i])
        for i, (src, dst) in enumerate(zip(ins, outs))
    ]
    for copy in copies:
        copy.start()
    for copy in copies:
        copy.wait()


def fetch(*arrays):
    return pl.pallas_call(
        fetch_kernel,
        in_specs=[HBM] * len(arrays),
        out_specs=[VMEM] * len(arrays),
        out_shape=[jax.ShapeDtypeStruct(a.shape, a.dtype) for a in arrays],
        scratch_shapes=[pltpu.SemaphoreType.DMA((len(arrays),))],
        compiler_params=params(16),
        cost_estimate=cost(2e9, 1e7),
        name="fetch",
    )(*arrays)


def expert_kernel(count, gate, widen, down, *refs):
    ins, (keep, send) = refs[: 2 * count], refs[2 * count :]
    rows = jnp.concatenate([piece[...] for piece in ins], axis=0)
    gated = contract1(rows, gate[...])
    lifted = contract1(rows, widen[...])
    hidden = (gated * jax.nn.sigmoid(gated) * lifted).astype(BF16)
    out = jnp.dot(hidden, down[...], preferred_element_type=F32)
    split = keep.shape[0]
    keep[...] = out[:split, :]
    send[...] = out[split:, :].astype(BF16)


def expert(weights, mine, theirs):
    count = len(mine)
    half, width = mine[0].shape
    return pl.pallas_call(
        functools.partial(expert_kernel, count),
        in_specs=[VMEM] * (3 + 2 * count),
        out_specs=[VMEM] * 2,
        out_shape=[
            jax.ShapeDtypeStruct((count * half, width), F32),
            jax.ShapeDtypeStruct((count * half, width), BF16),
        ],
        compiler_params=params(24),
        cost_estimate=cost(6e8 * count, 4e6),
    )(*weights, *mine, *theirs)


def merge_kernel(count, keep, received, *outs):
    half = outs[0].shape[0]
    for k in range(count):
        span = slice(k * half, (k + 1) * half)
        outs[k][...] = (keep[span, :] + received[span, :].astype(F32)).astype(BF16)


def merge(count, half, keep, received):
    width = keep.shape[1]
    return pl.pallas_call(
        functools.partial(merge_kernel, count),
        in_specs=[VMEM] * 2,
        out_specs=[VMEM] * count,
        out_shape=[jax.ShapeDtypeStruct((half, width), BF16)] * count,
        compiler_params=params(16),
        cost_estimate=cost(1e7, 4e6),
    )(keep, received)


def combine_kernel(n, groups, idx, high, low, *refs):
    ins, (keep, send, total) = refs[:n], refs[n:]
    rows = jnp.concatenate([piece[...] for piece in ins], axis=0)
    total[...] = contract0(high[...], rows) + contract0(low[...], rows)
    for span, own, other in block_spans(idx, groups, keep.shape[0] // groups):
        keep[span, :] = total[own, :]
        send[span, :] = total[other, :].astype(BF16)


def combine(n, groups, idx, high, low, pieces):
    width = pieces[0].shape[1]
    length = high.shape[1]
    return pl.pallas_call(
        functools.partial(combine_kernel, n, groups),
        in_specs=[SMEM] + [VMEM] * (2 + n),
        out_specs=[VMEM] * 2,
        out_shape=[
            jax.ShapeDtypeStruct((length // 2, width), F32),
            jax.ShapeDtypeStruct((length // 2, width), BF16),
        ],
        scratch_shapes=[pltpu.VMEM((length, width), F32)],
        compiler_params=params(16),
        cost_estimate=cost(1e9, 3e6),
        name="combine",
    )(idx, high, low, *pieces)


def swap(value, axis, k):
    return lax.ppermute(value, axis, xor_perm(axis, k))


def exchange(pieces):
    return [pieces[0]] + [swap(pieces[k], "sp", k) for k in range(1, len(pieces))]


def body(
    stream_in,
    queries,
    key_rows,
    values,
    decay_low,
    decay_matrix,
    decay_bias,
    decay_shift,
    head_gain,
    output_matrix,
    feed_gain,
    routes,
    route_weights,
    expert_gate,
    specialist_widen,
    expert_down,
):
    length = queries.shape[0]
    heads = queries.shape[1] // HK
    n = lax.axis_size("sp")
    head_devices = lax.axis_size("tp")
    groups = head_devices // 2
    me, tp = lax.axis_index("sp"), lax.axis_index("tp")
    core, line = tp % 2, tp // 2
    idx = jnp.stack([me, core, line]).astype(jnp.int32)
    rows = length // head_devices
    half = TOP * length // n // 2
    bias = decay_bias.reshape(1, -1)

    low, shift = decay_low.T, decay_shift.T
    count = heads // 2 if heads % 2 == 0 else heads

    gathered, states = [], None
    for part, first in enumerate(range(0, heads, count)):
        head_idx = idx
        if states is not None:
            head_idx, states = lax.optimization_barrier((idx, states))
        states = device_states(
            first, count, head_idx, low, decay_matrix, bias, shift, key_rows, values
        )
        gathered.append(exchange(states))
    stream_in, _ = lax.optimization_barrier((stream_in, states))
    streams = [stream_in] + [swap(stream_in, "tp", 2 * k) for k in range(1, groups)]
    local, late_queries = local_attention(
        heads, low, decay_matrix, bias, shift, queries, key_rows, values
    )
    select, high, low_part = slot_tables(n, half, idx, routes.T, route_weights.T)
    gathered[0], streams, local, late_queries = lax.optimization_barrier(
        (gathered[0], streams, local, late_queries)
    )
    carried = []
    for part, pieces in enumerate(gathered):
        entry = quad_entry(count, idx, pieces)
        carried += exchange(quad_prefix(count, True, idx, entry, pieces))
    carried, select, high, low_part = lax.optimization_barrier(
        (carried, select, high, low_part)
    )
    keep, send = project(
        count,
        heads,
        groups,
        idx,
        late_queries,
        local,
        head_gain.reshape(1, -1),
        output_matrix,
        carried,
    )
    received = swap(send, "tp", 1)
    shared = (keep + received.astype(F32)).astype(BF16)
    arrived = [swap(shared, "tp", 2 * k) for k in range(1, groups)]
    weights, _ = lax.optimization_barrier(
        ((expert_gate[0].T, specialist_widen[0].T, expert_down[0]), shared)
    )
    weights = fetch(*weights)
    arrived, weights = lax.optimization_barrier((arrived, weights))
    normed, mid = midstream_norm(
        groups, feed_gain.reshape(1, -1), keep, received, streams, arrived
    )
    theirs = swap(normed, "tp", 1)
    slots = dispatch(n, half, groups, idx, select, normed, theirs)
    slots = exchange(slots)
    back, previous = {}, None
    for part, ks in enumerate(expert_chunks(n)):
        mine = [slots[k] for k in ks]
        if previous is not None:
            mine, previous = lax.optimization_barrier((mine, previous))
        theirs = [swap(slot, "tp", 1) for slot in mine]
        kept, sent = expert(weights, mine, theirs)
        received = swap(sent, "tp", 1)
        merged = merge(len(ks), half, kept, received)
        previous = merged
        for k, piece in zip(ks, merged):
            back[k] = piece if k == 0 else swap(piece, "sp", k)
    back = [back[k] for k in range(n)]
    keep, send = combine(n, groups, idx, high, low_part, back)
    summed = keep + swap(send, "tp", 1).astype(F32)
    total = mid + summed[:rows]
    for k in range(1, groups):
        part = summed[k * rows : (k + 1) * rows].astype(BF16)
        total = total + swap(part, "tp", 2 * k).astype(F32)
    return total.astype(BF16)


def expert_chunks(n):
    middle = (QUAD + n) // 2
    return [range(QUAD), range(QUAD, middle), range(middle, n)]


def solution(mesh):
    return jax.shard_map(
        body,
        mesh=mesh,
        in_specs=(
            P(("sp", "tp"), None),
            P("sp", "tp"),
            P("sp", "tp"),
            P("sp", "tp"),
            P("sp", None),
            P(None, "tp"),
            P("tp"),
            P("sp", "tp"),
            P(),
            P("tp", None),
            P(),
            P("sp", None),
            P("sp", None),
            P("sp", None, "tp"),
            P("sp", None, "tp"),
            P("sp", "tp", None),
        ),
        out_specs=P(("sp", "tp"), None),
        check_vma=False,
    )
```

```python
import functools
import jax
import jax.numpy as jnp
from jax import lax
from jax.experimental import pallas as pl
from jax.experimental.pallas import tpu as pltpu
from jax.sharding import PartitionSpec as P


HK = 256
HV = 512
TOP = 2
BLK = 128
TEMPER = 16.0
EPSILON = 1e-06
F32 = jnp.float32
BF16 = jnp.bfloat16
VMEM = pl.BlockSpec(memory_space=pltpu.VMEM)
SMEM = pl.BlockSpec(memory_space=pltpu.SMEM)
HBM = pl.BlockSpec(memory_space=pltpu.HBM)
QUAD = 4


def cost(flops, moved):
    return pl.CostEstimate(flops=int(flops), bytes_accessed=int(moved), transcendentals=0)


def params(mib):
    return pltpu.CompilerParams(vmem_limit_bytes=mib * 1024 * 1024)


def xor_perm(axis, k):
    return [(i, i ^ k) for i in range(lax.axis_size(axis))]


def tri(n, fn):
    row = lax.broadcasted_iota(jnp.int32, (n, n), 0)
    col = lax.broadcasted_iota(jnp.int32, (n, n), 1)
    return fn(row, col)


def contract0(a, b):
    return lax.dot_general(a, b, (((0,), (0,)), ((), ())), preferred_element_type=F32)


def contract1(a, b):
    return lax.dot_general(a, b, (((1,), (1,)), ((), ())), preferred_element_type=F32)


def split_dot(ones, value):
    total = None
    for _ in range(3):
        part = value.astype(BF16)
        value = value - part.astype(F32)
        term = jnp.dot(ones, part, preferred_element_type=F32)
        total = term if total is None else total + term
    return total


def head_log_decay(low, matrix, bias, shift, head):
    pre = contract0(low, matrix) + bias
    logged = (jnp.minimum(pre, 0.0) - jnp.log1p(jnp.exp(-jnp.abs(pre)))) / TEMPER
    return logged + jnp.transpose(shift)[:, head : head + 1]


def state_kernel(first, count, idx, low, matrix, bias, shift, key_rows, values, *rest):
    outs = rest[:QUAD]
    keys, vals, state, decays, sems = rest[QUAD:]
    length = low.shape[1]
    piece = HK // QUAD
    copies = []
    for h in range(count):
        at = first + h
        pair = (
            pltpu.make_async_copy(
                key_rows.at[:, at * HK : (at + 1) * HK], keys.at[h], sems.at[0, h]
            ),
            pltpu.make_async_copy(
                values.at[:, at * HV : (at + 1) * HV], vals.at[h], sems.at[1, h]
            ),
        )
        for copy in pair:
            copy.start()
        copies.append(pair)
    after = tri(length, lambda r, c: c > r).astype(F32).astype(BF16)
    me = idx[0] % QUAD
    decays[...] = jnp.zeros_like(decays)
    for h in range(count):
        span = slice((first + h) * HK, (first + h + 1) * HK)
        logs = head_log_decay(low[...], matrix[:, span], bias[:, span], shift[...], first + h)
        suffix = split_dot(after, logs)
        total = jnp.exp(suffix[0:1, :] + logs[0:1, :])
        high = total.astype(BF16).astype(F32)
        decays[h : h + 1, 0:HK] = high
        decays[h : h + 1, HK : 2 * HK] = total - high
        for copy in copies[h]:
            copy.wait()
        end_keys = (keys[h].astype(F32) * jnp.exp(suffix)).astype(BF16)
        state[...] = contract0(end_keys, vals[h])
        for k in range(QUAD):
            start = pl.multiple_of((me ^ k) * piece, piece)
            outs[k][h * piece : (h + 1) * piece, :] = state[pl.ds(start, piece), :].astype(BF16)
    for k in range(QUAD):
        outs[k][count * piece :, :] = decays[...].astype(BF16)


def device_states(first, count, idx, low, matrix, bias, shift, key_rows, values):
    length = key_rows.shape[0]
    rows = count * (HK // QUAD) + 8
    return pl.pallas_call(
        functools.partial(state_kernel, first, count),
        in_specs=[SMEM] + [VMEM] * 4 + [HBM] * 2,
        out_specs=[VMEM] * QUAD,
        out_shape=[jax.ShapeDtypeStruct((rows, HV), BF16)] * QUAD,
        scratch_shapes=[
            pltpu.VMEM((count, length, HK), BF16),
            pltpu.VMEM((count, length, HV), BF16),
            pltpu.VMEM((HK, HV), F32),
            pltpu.VMEM((8, HV), F32),
            pltpu.SemaphoreType.DMA((2, count)),
        ],
        compiler_params=params(60),
        cost_estimate=cost(count * 4e8, count * 5e5),
    )(idx, low, matrix, bias, shift, key_rows, values)


def local_kernel(low, matrix, bias, shift, queries, key_rows, values, *refs):
    out, query_out = refs[-2:]
    length = low.shape[1]
    logs = head_log_decay(low[...], matrix[...], bias[...], shift[0], 0)
    below = tri(BLK, lambda r, c: c <= r)
    lower = below.astype(F32).astype(BF16)
    scale = HK ** (-0.5)
    before = jnp.zeros((1, HK), F32)
    earlier = []
    for b in range(length // BLK):
        rows = slice(b * BLK, (b + 1) * BLK)
        inside = split_dot(lower, logs[rows])
        final = inside[BLK - 1 : BLK, :]
        middle = inside[BLK // 2 - 1 : BLK // 2, :]
        query = queries[rows, :].astype(F32) * scale
        keys = key_rows[rows, :].astype(F32)
        grown = query * jnp.exp(inside)
        near_query = (query * jnp.exp(inside - middle)).astype(BF16)
        near_key = (keys * jnp.exp(middle - inside)).astype(BF16)
        scores = jnp.where(below, contract1(near_query, near_key), 0.0).astype(BF16)
        total = jnp.dot(scores, values[rows, :], preferred_element_type=F32)
        here = grown.astype(BF16)
        for past_keys, past_rows in earlier:
            cross = contract1(here, past_keys.astype(BF16)).astype(BF16)
            total = total + jnp.dot(cross, values[past_rows, :], preferred_element_type=F32)
        out[rows, :] = total
        query_out[rows, :] = (grown * jnp.exp(before)).astype(BF16)
        earlier = [(old * jnp.exp(final), old_rows) for old, old_rows in earlier]
        earlier.append((keys * jnp.exp(final - inside), rows))
        before = before + final


def local_attention(first, count, heads, sofar, low, matrix, bias, shift, *arrays):
    length = low.shape[1]
    queries, key_rows, values = arrays
    sofar = list(sofar or ())
    out_specs = [
        pl.BlockSpec((length, HV), lambda h: (0, first + h)),
        pl.BlockSpec((length, HK), lambda h: (0, first + h)),
    ]
    return pl.pallas_call(
        local_kernel,
        grid=(count,),
        in_specs=[
            pl.BlockSpec(low.shape, lambda h: (0, 0)),
            pl.BlockSpec((low.shape[0], HK), lambda h: (0, first + h)),
            pl.BlockSpec((1, HK), lambda h: (0, first + h)),
            pl.BlockSpec((1, 1, length), lambda h: (first + h, 0, 0)),
            pl.BlockSpec((length, HK), lambda h: (0, first + h)),
            pl.BlockSpec((length, HK), lambda h: (0, first + h)),
            pl.BlockSpec((length, HV), lambda h: (0, first + h)),
        ]
        + [pl.BlockSpec(memory_space=pl.ANY)] * len(sofar),
        out_specs=out_specs,
        out_shape=[
            jax.ShapeDtypeStruct((length, heads * HV), F32),
            jax.ShapeDtypeStruct((length, heads * HK), BF16),
        ],
        input_output_aliases={7 + i: i for i in range(len(sofar))},
        compiler_params=params(24),
        cost_estimate=cost(count * 4e8, count * 1.2e6),
    )(
        low,
        matrix,
        bias,
        shift.reshape(heads, 1, length),
        queries,
        key_rows,
        values,
        *sofar,
    )


def prefix_kernel(count, emit, idx, start, *refs):
    ins, outs, (stage, decays, result) = refs[:QUAD], refs[QUAD:-3], refs[-3:]
    me = idx[0] % QUAD
    piece = HK // QUAD
    rows = count * piece
    for k in range(QUAD):
        stage[me ^ k] = ins[k][:rows, :].astype(F32)
        tail = ins[k][rows:, :].astype(F32)
        decays[me ^ k] = jnp.transpose(tail[:, :HK] + tail[:, HK:])
    mine = pl.multiple_of(me * piece, piece)
    for h in range(count):
        span = slice(h * piece, (h + 1) * piece)
        carry = start[span, :].astype(F32)
        for i in range(QUAD):
            if emit:
                result[i, span, :] = carry
                if i == QUAD - 1:
                    break
            factor = decays[i, pl.ds(mine, piece), h : h + 1]
            carry = carry * factor + stage[i, span, :]
        if not emit:
            outs[0][span, :] = carry.astype(BF16)
    if emit:
        for k in range(QUAD):
            outs[k][...] = result[me ^ k].astype(BF16)


def quad_prefix(count, emit, idx, start, pieces):
    rows = count * (HK // QUAD)
    outs = QUAD if emit else 1
    return pl.pallas_call(
        functools.partial(prefix_kernel, count, emit),
        in_specs=[SMEM] + [VMEM] * (QUAD + 1),
        out_specs=[VMEM] * outs,
        out_shape=[jax.ShapeDtypeStruct((rows, HV), BF16)] * outs,
        scratch_shapes=[
            pltpu.VMEM((QUAD, rows, HV), F32),
            pltpu.VMEM((QUAD, HK, 8), F32),
            pltpu.VMEM((QUAD, rows, HV), F32),
        ],
        compiler_params=params(24),
        cost_estimate=cost(1e8, 1e6),
        name="quad_prefix" if emit else "quad_total",
    )(idx, start, *pieces)


def quad_entry(count, idx, pieces):
    rows = count * (HK // QUAD)
    start = jnp.zeros((rows, HV), BF16)
    quads = lax.axis_size("sp") // QUAD
    entry = None
    for g in range(quads - 1):
        (total,) = quad_prefix(count, False, idx, start, pieces)
        perm = [(g * QUAD + i, (g + 1) * QUAD + i) for i in range(QUAD)]
        start = lax.ppermute(total, "sp", perm)
        entry = start if entry is None else entry + start
    return start if entry is None else entry


def block_spans(idx, groups, rows):
    core, line = idx[1], idx[2]
    for k in range(groups):
        base = (line ^ k) * 2
        own = pl.ds(pl.multiple_of((base + core) * rows, rows), rows)
        other = pl.ds(pl.multiple_of((base + 1 - core) * rows, rows), rows)
        yield slice(k * rows, (k + 1) * rows), own, other


def project_kernel(count, heads, groups, idx, queries, local, gain, matrix, *refs):
    pieces, (keep, send, carried, total) = refs[:-4], refs[-4:]
    head = pl.program_id(0)
    me = idx[0] % QUAD
    piece = HK // QUAD

    @pl.when(head == 0)
    def _():
        total[...] = jnp.zeros_like(total)
        for at, ref in enumerate(pieces):
            start = pl.multiple_of((me ^ (at % QUAD)) * piece, piece)
            for h in range(count):
                span = slice(h * piece, (h + 1) * piece)
                spot = at // QUAD * count + h
                carried[spot, pl.ds(start, piece), :] = ref[span, :].astype(F32)

    out = local[...] + jnp.dot(
        queries[...], carried[head].astype(BF16), preferred_element_type=F32
    )
    spread = lax.rsqrt(jnp.mean(out * out, axis=-1, keepdims=True) + EPSILON)
    mixed = (out * spread * gain[...]).astype(BF16)
    total[...] += jnp.dot(mixed, matrix[...], preferred_element_type=F32)

    @pl.when(head == heads - 1)
    def _():
        for span, own, other in block_spans(idx, groups, keep.shape[0] // groups):
            keep[span, :] = total[own, :]
            send[span, :] = total[other, :].astype(BF16)


def project(count, heads, groups, idx, queries, local, gain, matrix, pieces):
    length = queries.shape[0]
    width = matrix.shape[1]
    rows = count * (HK // QUAD)
    return pl.pallas_call(
        functools.partial(project_kernel, count, heads, groups),
        grid=(heads,),
        in_specs=[
            SMEM,
            pl.BlockSpec((length, HK), lambda h: (0, h)),
            pl.BlockSpec((length, HV), lambda h: (0, h)),
            pl.BlockSpec((1, HV), lambda h: (0, 0)),
            pl.BlockSpec((HV, width), lambda h: (h, 0)),
        ]
        + [pl.BlockSpec((rows, HV), lambda h: (0, 0))] * len(pieces),
        out_specs=[pl.BlockSpec((length // 2, width), lambda h: (0, 0))] * 2,
        out_shape=[
            jax.ShapeDtypeStruct((length // 2, width), F32),
            jax.ShapeDtypeStruct((length // 2, width), BF16),
        ],
        scratch_shapes=[
            pltpu.VMEM((heads, HK, HV), F32),
            pltpu.VMEM((length, width), F32),
        ],
        compiler_params=params(32),
        cost_estimate=cost(heads * 7e8, heads * 2.5e6),
        name="project",
    )(idx, queries, local, gain, matrix, *pieces)


def norm_kernel(groups, gain, keep, received, *refs):
    streams, arrived = refs[:groups], refs[groups : 2 * groups - 1]
    normed, mid = refs[2 * groups - 1 :]
    rows = mid.shape[0]
    for k in range(groups):
        span = slice(k * rows, (k + 1) * rows)
        value = keep[span, :] + received[span, :].astype(F32)
        for j in range(1, groups):
            there = k ^ j
            value = value + arrived[j - 1][there * rows : (there + 1) * rows, :].astype(F32)
        value = value + streams[k][...].astype(F32)
        if k == 0:
            mid[...] = value
        spread = lax.rsqrt(jnp.mean(value * value, axis=-1, keepdims=True) + EPSILON)
        normed[span, :] = (value * spread * gain[...]).astype(BF16)


def midstream_norm(groups, gain, keep, received, streams, arrived):
    rows, width = streams[0].shape
    return pl.pallas_call(
        functools.partial(norm_kernel, groups),
        in_specs=[VMEM] * (3 + 2 * groups - 1),
        out_specs=[VMEM] * 2,
        out_shape=[
            jax.ShapeDtypeStruct((groups * rows, width), BF16),
            jax.ShapeDtypeStruct((rows, width), F32),
        ],
        compiler_params=params(24),
        cost_estimate=cost(1e7, 3e6),
        name="midstream_norm",
    )(gain, keep, received, *streams, *arrived)


def route_kernel(n, half, idx, routes, weights, select, high, low):
    me, core = idx[0], idx[1]
    length = routes.shape[1]
    earlier = tri(length, lambda r, c: c < r).astype(F32).astype(BF16)
    chosen = jnp.transpose(routes[...].astype(F32)).astype(jnp.int32)
    weight = jnp.transpose(weights[...])
    expert = me ^ lax.broadcasted_iota(jnp.int32, (length, n), 1)
    is_first, is_second = chosen[:, 0:1] == expert, chosen[:, 1:2] == expert
    member = jnp.where(is_first | is_second, 1.0, 0.0)
    rank = jnp.dot(earlier, member.astype(BF16), preferred_element_type=F32)
    slot = jnp.where(member > 0.0, rank, -1.0)
    value = jnp.where(is_first, weight[:, 0:1], weight[:, 1:2])
    top = value.astype(BF16)
    rest = (value - top.astype(F32)).astype(BF16)
    column = lax.broadcasted_iota(jnp.int32, (n, n * half), 1)
    owner = lax.broadcasted_iota(jnp.int32, (n, n * half), 0)
    spread = jnp.where(column // half == owner, 1.0, 0.0).astype(BF16)

    def widen(array):
        return jnp.dot(array, spread, preferred_element_type=F32)

    wanted = core * half + lax.broadcasted_iota(jnp.int32, (length, n * half), 1) % half
    hit = widen(slot.astype(BF16)) == wanted.astype(F32)
    select[...] = jnp.where(hit, 1.0, 0.0).astype(BF16)
    high[...] = jnp.where(hit, widen(top), 0.0).astype(BF16)
    low[...] = jnp.where(hit, widen(rest), 0.0).astype(BF16)


def slot_tables(n, half, idx, routes, weights):
    length = routes.shape[1]
    return pl.pallas_call(
        functools.partial(route_kernel, n, half),
        in_specs=[SMEM, VMEM, VMEM],
        out_specs=[VMEM] * 3,
        out_shape=[jax.ShapeDtypeStruct((length, n * half), BF16)] * 3,
        compiler_params=params(16),
        cost_estimate=cost(1e8, 5e5),
        name="slot_tables",
    )(idx, routes, weights)


def dispatch_kernel(n, half, groups, idx, select, mine, theirs, *refs):
    outs, table = refs[:n], refs[n]
    split = mine.shape[0]
    for span, own, other in block_spans(idx, groups, split // groups):
        table[span, :] = select[own, :]
        table[split + span.start : split + span.stop, :] = select[other, :]
    picked = contract0(table[:split, :], mine[...]) + contract0(table[split:, :], theirs[...])
    for k in range(n):
        outs[k][...] = picked[k * half : (k + 1) * half, :].astype(BF16)


def dispatch(n, half, groups, idx, select, mine, theirs):
    width = mine.shape[1]
    return pl.pallas_call(
        functools.partial(dispatch_kernel, n, half, groups),
        in_specs=[SMEM] + [VMEM] * 3,
        out_specs=[VMEM] * n,
        out_shape=[jax.ShapeDtypeStruct((half, width), BF16)] * n,
        scratch_shapes=[pltpu.VMEM(select.shape, BF16)],
        compiler_params=params(16),
        cost_estimate=cost(5e8, 2e6),
        name="dispatch",
    )(idx, select, mine, theirs)


def fetch_kernel(*refs):
    half = (len(refs) - 1) // 2
    ins, outs, sems = refs[:half], refs[half:-1], refs[-1]
    copies = [
        pltpu.make_async_copy(src, dst, sems.at[i])
        for i, (src, dst) in enumerate(zip(ins, outs))
    ]
    for copy in copies:
        copy.start()
    for copy in copies:
        copy.wait()


def fetch(*arrays):
    return pl.pallas_call(
        fetch_kernel,
        in_specs=[HBM] * len(arrays),
        out_specs=[VMEM] * len(arrays),
        out_shape=[jax.ShapeDtypeStruct(a.shape, a.dtype) for a in arrays],
        scratch_shapes=[pltpu.SemaphoreType.DMA((len(arrays),))],
        compiler_params=params(16),
        cost_estimate=cost(2e9, 1e7),
        name="fetch",
    )(*arrays)


def expert_kernel(count, gate, widen, down, *refs):
    ins, (keep, send) = refs[: 2 * count], refs[2 * count :]
    rows = jnp.concatenate([piece[...] for piece in ins], axis=0)
    gated = contract1(rows, gate[...])
    lifted = contract1(rows, widen[...])
    hidden = (gated * jax.nn.sigmoid(gated) * lifted).astype(BF16)
    out = jnp.dot(hidden, down[...], preferred_element_type=F32)
    split = keep.shape[0]
    keep[...] = out[:split, :]
    send[...] = out[split:, :].astype(BF16)


def expert(weights, mine, theirs):
    count = len(mine)
    half, width = mine[0].shape
    return pl.pallas_call(
        functools.partial(expert_kernel, count),
        in_specs=[VMEM] * (3 + 2 * count),
        out_specs=[VMEM] * 2,
        out_shape=[
            jax.ShapeDtypeStruct((count * half, width), F32),
            jax.ShapeDtypeStruct((count * half, width), BF16),
        ],
        compiler_params=params(24),
        cost_estimate=cost(6e8 * count, 4e6),
    )(*weights, *mine, *theirs)


def merge_kernel(count, keep, received, *outs):
    half = outs[0].shape[0]
    for k in range(count):
        span = slice(k * half, (k + 1) * half)
        outs[k][...] = (keep[span, :] + received[span, :].astype(F32)).astype(BF16)


def merge(count, half, keep, received):
    width = keep.shape[1]
    return pl.pallas_call(
        functools.partial(merge_kernel, count),
        in_specs=[VMEM] * 2,
        out_specs=[VMEM] * count,
        out_shape=[jax.ShapeDtypeStruct((half, width), BF16)] * count,
        compiler_params=params(16),
        cost_estimate=cost(1e7, 4e6),
    )(keep, received)


def combine_kernel(n, groups, idx, high, low, *refs):
    ins, (keep, send, table) = refs[:n], refs[n:]
    rows = jnp.concatenate([piece[...] for piece in ins], axis=0)
    split = keep.shape[0]
    for part, source in enumerate((high, low)):
        for span, own, other in block_spans(idx, groups, split // groups):
            table[part, span, :] = source[own, :]
            table[part, split + span.start : split + span.stop, :] = source[other, :]
    total = jnp.dot(table[0], rows, preferred_element_type=F32)
    total = total + jnp.dot(table[1], rows, preferred_element_type=F32)
    keep[...] = total[:split, :]
    send[...] = total[split:, :].astype(BF16)


def combine(n, groups, idx, high, low, pieces):
    width = pieces[0].shape[1]
    length = high.shape[0]
    return pl.pallas_call(
        functools.partial(combine_kernel, n, groups),
        in_specs=[SMEM] + [VMEM] * (2 + n),
        out_specs=[VMEM] * 2,
        out_shape=[
            jax.ShapeDtypeStruct((length // 2, width), F32),
            jax.ShapeDtypeStruct((length // 2, width), BF16),
        ],
        scratch_shapes=[pltpu.VMEM((2,) + high.shape, BF16)],
        compiler_params=params(16),
        cost_estimate=cost(1e9, 3e6),
        name="combine",
    )(idx, high, low, *pieces)


def swap(value, axis, k):
    return lax.ppermute(value, axis, xor_perm(axis, k))


def exchange(pieces):
    return [pieces[0]] + [swap(pieces[k], "sp", k) for k in range(1, len(pieces))]


def body(
    stream_in,
    queries,
    key_rows,
    values,
    decay_low,
    decay_matrix,
    decay_bias,
    decay_shift,
    head_gain,
    output_matrix,
    feed_gain,
    routes,
    route_weights,
    expert_gate,
    specialist_widen,
    expert_down,
):
    length = queries.shape[0]
    heads = queries.shape[1] // HK
    n = lax.axis_size("sp")
    head_devices = lax.axis_size("tp")
    groups = head_devices // 2
    me, tp = lax.axis_index("sp"), lax.axis_index("tp")
    core, line = tp % 2, tp // 2
    idx = jnp.stack([me, core, line]).astype(jnp.int32)
    rows = length // head_devices
    half = TOP * length // n // 2
    bias = decay_bias.reshape(1, -1)

    low, shift = decay_low.T, decay_shift.T
    count = heads // 2 if heads % 2 == 0 else heads

    gathered, states = [], None
    for part, first in enumerate(range(0, heads, count)):
        head_idx = idx
        if states is not None:
            head_idx, states = lax.optimization_barrier((idx, states))
        states = device_states(
            first, count, head_idx, low, decay_matrix, bias, shift, key_rows, values
        )
        gathered.append(exchange(states))
    stream_in, _ = lax.optimization_barrier((stream_in, states))
    streams = [stream_in] + [swap(stream_in, "tp", 2 * k) for k in range(1, groups)]
    sofar = None
    for first in range(0, heads, count):
        sofar = local_attention(
            first,
            count,
            heads,
            sofar,
            low,
            decay_matrix,
            bias,
            shift,
            queries,
            key_rows,
            values,
        )
    local, late_queries = sofar
    select, high, low_part = slot_tables(n, half, idx, routes.T, route_weights.T)
    carried = []
    for part, pieces in enumerate(gathered):
        entry = quad_entry(count, idx, pieces)
        carried += exchange(quad_prefix(count, True, idx, entry, pieces))
    carried, streams, select, high, low_part = lax.optimization_barrier(
        (carried, streams, select, high, low_part)
    )
    keep, send = project(
        count,
        heads,
        groups,
        idx,
        late_queries,
        local,
        head_gain.reshape(1, -1),
        output_matrix,
        carried,
    )
    received = swap(send, "tp", 1)
    shared = (keep + received.astype(F32)).astype(BF16)
    arrived = [swap(shared, "tp", 2 * k) for k in range(1, groups)]
    weights, _ = lax.optimization_barrier(
        ((expert_gate[0].T, specialist_widen[0].T, expert_down[0]), shared)
    )
    weights = fetch(*weights)
    arrived, weights = lax.optimization_barrier((arrived, weights))
    normed, mid = midstream_norm(
        groups, feed_gain.reshape(1, -1), keep, received, streams, arrived
    )
    theirs = swap(normed, "tp", 1)
    slots = dispatch(n, half, groups, idx, select, normed, theirs)
    slots = exchange(slots)
    back, previous = {}, None
    for part, ks in enumerate(expert_chunks(n)):
        mine = [slots[k] for k in ks]
        if previous is not None:
            mine, previous = lax.optimization_barrier((mine, previous))
        theirs = [swap(slot, "tp", 1) for slot in mine]
        kept, sent = expert(weights, mine, theirs)
        received = swap(sent, "tp", 1)
        merged = merge(len(ks), half, kept, received)
        previous = merged
        for k, piece in zip(ks, merged):
            back[k] = piece if k == 0 else swap(piece, "sp", k)
    back = [back[k] for k in range(n)]
    keep, send = combine(n, groups, idx, high, low_part, back)
    summed = keep + swap(send, "tp", 1).astype(F32)
    total = mid + summed[:rows]
    for k in range(1, groups):
        part = summed[k * rows : (k + 1) * rows].astype(BF16)
        total = total + swap(part, "tp", 2 * k).astype(F32)
    return total.astype(BF16)


def expert_chunks(n):
    middle = (QUAD + n) // 2
    return [range(QUAD, middle), range(QUAD), range(middle, n)]


def solution(mesh):
    return jax.shard_map(
        body,
        mesh=mesh,
        in_specs=(
            P(("sp", "tp"), None),
            P("sp", "tp"),
            P("sp", "tp"),
            P("sp", "tp"),
            P("sp", None),
            P(None, "tp"),
            P("tp"),
            P("sp", "tp"),
            P(),
            P("tp", None),
            P(),
            P("sp", None),
            P("sp", None),
            P("sp", None, "tp"),
            P("sp", None, "tp"),
            P("sp", "tp", None),
        ),
        out_specs=P(("sp", "tp"), None),
        check_vma=False,
    )
```

```python
import functools
import jax
import jax.numpy as jnp
from jax import lax
from jax.experimental import pallas as pl
from jax.experimental.pallas import tpu as pltpu
from jax.sharding import PartitionSpec as P


HK = 256
HV = 512
TOP = 2
BLK = 128
TEMPER = 16.0
EPSILON = 1e-06
F32 = jnp.float32
BF16 = jnp.bfloat16
VMEM = pl.BlockSpec(memory_space=pltpu.VMEM)
SMEM = pl.BlockSpec(memory_space=pltpu.SMEM)
HBM = pl.BlockSpec(memory_space=pltpu.HBM)
QUAD = 4


def cost(flops, moved):
    return pl.CostEstimate(flops=int(flops), bytes_accessed=int(moved), transcendentals=0)


def params(mib):
    return pltpu.CompilerParams(vmem_limit_bytes=mib * 1024 * 1024)


def place():
    tp = lax.axis_index("tp")
    return lax.axis_index("sp"), tp % 2, tp // 2


def xor_perm(axis, k):
    return [(i, i ^ k) for i in range(lax.axis_size(axis))]


def tri(n, fn):
    row = lax.broadcasted_iota(jnp.int32, (n, n), 0)
    col = lax.broadcasted_iota(jnp.int32, (n, n), 1)
    return fn(row, col)


def contract0(a, b):
    return lax.dot_general(a, b, (((0,), (0,)), ((), ())), preferred_element_type=F32)


def contract1(a, b):
    return lax.dot_general(a, b, (((1,), (1,)), ((), ())), preferred_element_type=F32)


def split_dot(ones, value):
    total = None
    for _ in range(3):
        part = value.astype(BF16)
        value = value - part.astype(F32)
        term = jnp.dot(ones, part, preferred_element_type=F32)
        total = term if total is None else total + term
    return total


def head_log_decay(low, matrix, bias, shift, head):
    pre = contract0(low, matrix) + bias
    logged = (jnp.minimum(pre, 0.0) - jnp.log1p(jnp.exp(-jnp.abs(pre)))) / TEMPER
    return logged + jnp.transpose(shift)[:, head : head + 1]


def state_kernel(first, count, low, matrix, bias, shift, key_rows, values, *rest):
    outs = rest[:QUAD]
    keys, vals, state, decays, sems = rest[QUAD:]
    length = low.shape[1]
    piece = HK // QUAD
    copies = []
    for h in range(count):
        at = first + h
        pair = (
            pltpu.make_async_copy(
                key_rows.at[:, at * HK : (at + 1) * HK], keys.at[h], sems.at[0, h]
            ),
            pltpu.make_async_copy(
                values.at[:, at * HV : (at + 1) * HV], vals.at[h], sems.at[1, h]
            ),
        )
        for copy in pair:
            copy.start()
        copies.append(pair)
    after = tri(length, lambda r, c: c > r).astype(F32).astype(BF16)
    me = place()[0] % QUAD
    decays[...] = jnp.zeros_like(decays)
    for h in range(count):
        span = slice((first + h) * HK, (first + h + 1) * HK)
        logs = head_log_decay(low[...], matrix[:, span], bias[:, span], shift[...], first + h)
        suffix = split_dot(after, logs)
        total = jnp.exp(suffix[0:1, :] + logs[0:1, :])
        high = total.astype(BF16).astype(F32)
        decays[h : h + 1, 0:HK] = high
        decays[h : h + 1, HK : 2 * HK] = total - high
        for copy in copies[h]:
            copy.wait()
        end_keys = (keys[h].astype(F32) * jnp.exp(suffix)).astype(BF16)
        state[...] = contract0(end_keys, vals[h])
        for k in range(QUAD):
            start = pl.multiple_of((me ^ k) * piece, piece)
            outs[k][h * piece : (h + 1) * piece, :] = state[pl.ds(start, piece), :].astype(BF16)
    for k in range(QUAD):
        outs[k][count * piece :, :] = decays[...].astype(BF16)


def device_states(first, count, low, matrix, bias, shift, key_rows, values):
    length = key_rows.shape[0]
    rows = count * (HK // QUAD) + 8
    return pl.pallas_call(
        functools.partial(state_kernel, first, count),
        in_specs=[VMEM] * 4 + [HBM] * 2,
        out_specs=[VMEM] * QUAD,
        out_shape=[jax.ShapeDtypeStruct((rows, HV), BF16)] * QUAD,
        scratch_shapes=[
            pltpu.VMEM((count, length, HK), BF16),
            pltpu.VMEM((count, length, HV), BF16),
            pltpu.VMEM((HK, HV), F32),
            pltpu.VMEM((8, HV), F32),
            pltpu.SemaphoreType.DMA((2, count)),
        ],
        compiler_params=params(60),
        cost_estimate=cost(count * 4e8, count * 5e5),
    )(low, matrix, bias, shift, key_rows, values)


def local_kernel(first, count, low, matrix, bias, shift, queries, key_rows, values, *refs):
    out, query_out = refs[-2:]
    length = low.shape[1]
    below = tri(BLK, lambda r, c: c <= r)
    lower = below.astype(F32).astype(BF16)
    scale = HK ** (-0.5)
    for h in range(count):
        narrow, wide = slice(h * HK, (h + 1) * HK), slice(h * HV, (h + 1) * HV)
        logs = head_log_decay(
            low[...], matrix[:, narrow], bias[:, narrow], shift[...], first + h
        )
        before = jnp.zeros((1, HK), F32)
        earlier = []
        for b in range(length // BLK):
            rows = slice(b * BLK, (b + 1) * BLK)
            inside = split_dot(lower, logs[rows])
            final = inside[BLK - 1 : BLK, :]
            middle = inside[BLK // 2 - 1 : BLK // 2, :]
            query = queries[rows, narrow].astype(F32) * scale
            keys = key_rows[rows, narrow].astype(F32)
            grown = query * jnp.exp(inside)
            near_query = (query * jnp.exp(inside - middle)).astype(BF16)
            near_key = (keys * jnp.exp(middle - inside)).astype(BF16)
            scores = jnp.where(below, contract1(near_query, near_key), 0.0).astype(BF16)
            total = jnp.dot(scores, values[rows, wide], preferred_element_type=F32)
            here = grown.astype(BF16)
            for past_keys, past in earlier:
                cross = contract1(here, past_keys.astype(BF16)).astype(BF16)
                total = total + jnp.dot(cross, values[past, wide], preferred_element_type=F32)
            out[rows, wide] = total
            query_out[rows, narrow] = (grown * jnp.exp(before)).astype(BF16)
            if b + 1 < length // BLK:
                earlier = [(old * jnp.exp(final), past) for old, past in earlier]
                earlier.append((keys * jnp.exp(final - inside), rows))
                before = before + final


def local_attention(first, count, low, matrix, bias, shift, queries, key_rows, values):
    length = low.shape[1]
    block = first // count

    def part(width):
        return pl.BlockSpec((length, count * width), lambda i: (0, block))

    return pl.pallas_call(
        functools.partial(local_kernel, first, count),
        grid=(1,),
        in_specs=[
            pl.BlockSpec(low.shape, lambda i: (0, 0)),
            pl.BlockSpec((low.shape[0], count * HK), lambda i: (0, block)),
            pl.BlockSpec((1, count * HK), lambda i: (0, block)),
            pl.BlockSpec(shift.shape, lambda i: (0, 0)),
            part(HK),
            part(HK),
            part(HV),
        ],
        out_specs=[
            pl.BlockSpec((length, count * HV), lambda i: (0, 0)),
            pl.BlockSpec((length, count * HK), lambda i: (0, 0)),
        ],
        out_shape=[
            jax.ShapeDtypeStruct((length, count * HV), F32),
            jax.ShapeDtypeStruct((length, count * HK), BF16),
        ],
        compiler_params=params(24),
        cost_estimate=cost(count * 4e8, count * 1.2e6),
    )(low, matrix, bias, shift, queries, key_rows, values)


def prefix_kernel(count, emit, primed, *refs):
    start, refs = (refs[0], refs[1:]) if primed else (None, refs)
    ins, outs = refs[:QUAD], refs[QUAD:]
    me = place()[0] % QUAD
    piece = HK // QUAD
    rows = count * piece
    tails = jnp.concatenate([ref[rows : rows + 8, :].astype(F32) for ref in ins], axis=0)
    across = jnp.transpose(tails[:, :HK] + tails[:, HK:])
    parts = [across[i * piece : (i + 1) * piece, :] for i in range(QUAD)]
    mine = parts[0]
    for i in range(1, QUAD):
        mine = jnp.where(me == i, parts[i], mine)
    decay = [mine[:, k * 8 : k * 8 + count] for k in range(QUAD)]
    spot = [me ^ k for k in range(QUAD)]
    ends = spot if emit else [jnp.int32(QUAD)]

    def between(low, end):
        factor = jnp.ones_like(decay[0])
        for k in range(QUAD):
            inside = jnp.logical_and(spot[k] > low, spot[k] < end)
            factor = jnp.where(inside, factor * decay[k], factor)
        return factor

    weights = [
        [jnp.where(spot[k] < end, between(spot[k], end), 0.0) for k in range(QUAD)]
        + ([between(-1, end)] if primed else [])
        for end in ends
    ]
    for h in range(count):
        span = slice(h * piece, (h + 1) * piece)
        sources = [ref[span, :].astype(F32) for ref in ins]
        if primed:
            sources.append(start[span, :].astype(F32))
        for out, factors in zip(outs, weights):
            total = None
            for source, factor in zip(sources, factors):
                term = source * factor[:, h : h + 1]
                total = term if total is None else total + term
            out[span, :] = total.astype(BF16)


def quad_prefix(count, emit, start, pieces):
    rows = count * (HK // QUAD)
    outs = QUAD if emit else 1
    primed = [] if start is None else [start]
    return pl.pallas_call(
        functools.partial(prefix_kernel, count, emit, start is not None),
        in_specs=[VMEM] * (QUAD + len(primed)),
        out_specs=[VMEM] * outs,
        out_shape=[jax.ShapeDtypeStruct((rows, HV), BF16)] * outs,
        compiler_params=params(24),
        cost_estimate=cost(1e8, 1e6),
        name="quad_prefix" if emit else "quad_total",
    )(*primed, *pieces)


def quad_entry(count, pieces):
    start = None
    quads = lax.axis_size("sp") // QUAD
    entry = None
    for g in range(quads - 1):
        (total,) = quad_prefix(count, False, start, pieces)
        perm = [(g * QUAD + i, (g + 1) * QUAD + i) for i in range(QUAD)]
        start = lax.ppermute(total, "sp", perm)
        entry = start if entry is None else entry + start
    return entry


def block_spans(groups, rows):
    _, core, line = place()
    for k in range(groups):
        base = (line ^ k) * 2
        own = pl.ds(pl.multiple_of((base + core) * rows, rows), rows)
        other = pl.ds(pl.multiple_of((base + 1 - core) * rows, rows), rows)
        yield slice(k * rows, (k + 1) * rows), own, other


def project_kernel(count, groups, gain, matrix, *refs):
    mixed, keep, send, carried = refs[-4:]
    chunks = len(refs[:-4]) // (2 + QUAD)
    local, queries, pieces = refs[:chunks], refs[chunks : 2 * chunks], refs[2 * chunks : -4]
    me, my_core, my_line = place()
    me = me % QUAD
    piece = HK // QUAD
    split = keep.shape[0]
    rows = split // groups
    for part in range(chunks):
        for h in range(count):
            span = slice(h * piece, (h + 1) * piece)
            for k in range(QUAD):
                start = pl.multiple_of((me ^ k) * piece, piece)
                carried[pl.ds(start, piece), :] = pieces[part * QUAD + k][span, :]
            narrow, wide = slice(h * HK, (h + 1) * HK), slice(h * HV, (h + 1) * HV)
            out = local[part][:, wide] + jnp.dot(
                queries[part][:, narrow], carried[...], preferred_element_type=F32
            )
            spread = lax.rsqrt(jnp.mean(out * out, axis=-1, keepdims=True) + EPSILON)
            value = (out * spread * gain[...]).astype(BF16)
            at = (part * count + h) * HV
            for b in range(2 * groups):
                line, core = b // 2, b % 2
                there = (line ^ my_line) + (core ^ my_core) * groups
                there = pl.multiple_of(there * rows, rows)
                mixed[pl.ds(there, rows), at : at + HV] = value[b * rows : (b + 1) * rows, :]
    keep[...] = jnp.dot(mixed[:split, :], matrix[...], preferred_element_type=F32)
    send[...] = jnp.dot(mixed[split:, :], matrix[...], preferred_element_type=F32).astype(BF16)


def project_rest_kernel(mixed, matrix, keep, send):
    split = keep.shape[0]
    total = jnp.dot(mixed[...], matrix[...], preferred_element_type=F32)
    keep[...] = total[:split, :]
    send[...] = total[split:, :].astype(BF16)


def project(count, groups, gain, matrix, local, pieces):
    outs = [array for array, _ in local] + [array for _, array in local]
    length = outs[0].shape[0]
    depth, width = matrix.shape
    cut = width // 2
    small = [
        jax.ShapeDtypeStruct((length // 2, cut), F32),
        jax.ShapeDtypeStruct((length // 2, cut), BF16),
    ]
    whole = [pl.BlockSpec((length // 2, cut), lambda i: (0, 0))] * 2
    mixed, keep, send = pl.pallas_call(
        functools.partial(project_kernel, count, groups),
        grid=(1,),
        in_specs=[VMEM, pl.BlockSpec((depth, cut), lambda i: (0, 0))]
        + [VMEM] * (len(outs) + len(pieces)),
        out_specs=[pl.BlockSpec((length, depth), lambda i: (0, 0))] + whole,
        out_shape=[jax.ShapeDtypeStruct((length, depth), BF16)] + small,
        scratch_shapes=[pltpu.VMEM((HK, HV), BF16)],
        compiler_params=params(28),
        cost_estimate=cost(2e9, 8e6),
        name="project",
    )(gain, matrix, *outs, *pieces)
    rest = pl.pallas_call(
        project_rest_kernel,
        grid=(1,),
        in_specs=[
            pl.BlockSpec((length, depth), lambda i: (0, 0)),
            pl.BlockSpec((depth, cut), lambda i: (0, 1)),
        ],
        out_specs=whole,
        out_shape=small,
        compiler_params=params(28),
        cost_estimate=cost(1e9, 6e6),
        name="project_rest",
    )(mixed, matrix)
    return (keep, send), rest


def norm_kernel(groups, gain, *refs):
    keeps, received, streams = refs[:2], refs[2:4], refs[4 : 4 + groups]
    arrived = refs[4 + groups : 4 + groups + 2 * (groups - 1)]
    normed, mid = refs[-2:]
    rows, width = mid.shape
    cut = width // 2
    for k in range(groups):
        span = slice(k * rows, (k + 1) * rows)
        values, square = [], None
        for side in range(2):
            columns = slice(side * cut, (side + 1) * cut)
            value = keeps[side][span, :] + received[side][span, :].astype(F32)
            for j in range(1, groups):
                there = k ^ j
                part = arrived[side * (groups - 1) + j - 1]
                value = value + part[there * rows : (there + 1) * rows, :].astype(F32)
            value = value + streams[k][:, columns].astype(F32)
            if k == 0:
                mid[:, columns] = value
            term = jnp.sum(value * value, axis=-1, keepdims=True)
            square = term if square is None else square + term
            values.append((columns, value))
        spread = lax.rsqrt(square / width + EPSILON)
        for columns, value in values:
            normed[span, columns] = (value * spread * gain[:, columns]).astype(BF16)


def midstream_norm(groups, gain, keeps, received, streams, arrived):
    rows, width = streams[0].shape
    arrays = [*keeps, *received, *streams, *arrived]
    return pl.pallas_call(
        functools.partial(norm_kernel, groups),
        in_specs=[VMEM] * (1 + len(arrays)),
        out_specs=[VMEM] * 2,
        out_shape=[
            jax.ShapeDtypeStruct((groups * rows, width), BF16),
            jax.ShapeDtypeStruct((rows, width), F32),
        ],
        compiler_params=params(24),
        cost_estimate=cost(1e7, 3e6),
        name="midstream_norm",
    )(gain, *arrays)


def route_kernel(n, half, groups, routes, weights, select, high, low, table):
    me, core, _ = place()
    length = routes.shape[1]
    earlier = tri(length, lambda r, c: c < r).astype(F32).astype(BF16)
    chosen = jnp.transpose(routes[...].astype(F32)).astype(jnp.int32)
    weight = jnp.transpose(weights[...])
    expert = me ^ lax.broadcasted_iota(jnp.int32, (length, n), 1)
    is_first, is_second = chosen[:, 0:1] == expert, chosen[:, 1:2] == expert
    member = jnp.where(is_first | is_second, 1.0, 0.0)
    rank = jnp.dot(earlier, member.astype(BF16), preferred_element_type=F32)
    slot = jnp.where(member > 0.0, rank, -1.0)
    value = jnp.where(is_first, weight[:, 0:1], weight[:, 1:2])
    top = value.astype(BF16)
    rest = (value - top.astype(F32)).astype(BF16)
    column = lax.broadcasted_iota(jnp.int32, (n, n * half), 1)
    owner = lax.broadcasted_iota(jnp.int32, (n, n * half), 0)
    spread = jnp.where(column // half == owner, 1.0, 0.0).astype(BF16)

    def widen(array):
        return jnp.dot(array, spread, preferred_element_type=F32)

    wanted = core * half + lax.broadcasted_iota(jnp.int32, (length, n * half), 1) % half
    hit = widen(slot.astype(BF16)) == wanted.astype(F32)
    table[0] = jnp.where(hit, 1.0, 0.0)
    table[1] = jnp.where(hit, widen(top), 0.0)
    table[2] = jnp.where(hit, widen(rest), 0.0)
    split = length // 2
    ordered = []
    for span, own, other in block_spans(groups, split // groups):
        below = slice(split + span.start, split + span.stop)
        for out, source in ((high, 1), (low, 2)):
            out[span, :] = table[source, own, :].astype(BF16)
            out[below, :] = table[source, other, :].astype(BF16)
        ordered.append((table[0, own, :], table[0, other, :]))
    chosen = jnp.concatenate([own for own, _ in ordered] + [other for _, other in ordered])
    select[...] = jnp.transpose(chosen).astype(BF16)


def slot_tables(n, half, groups, routes, weights):
    length = routes.shape[1]
    return pl.pallas_call(
        functools.partial(route_kernel, n, half, groups),
        in_specs=[VMEM, VMEM],
        out_specs=[VMEM] * 3,
        out_shape=[
            jax.ShapeDtypeStruct((n * half, length), BF16),
            jax.ShapeDtypeStruct((length, n * half), BF16),
            jax.ShapeDtypeStruct((length, n * half), BF16),
        ],
        scratch_shapes=[pltpu.VMEM((3, length, n * half), F32)],
        compiler_params=params(16),
        cost_estimate=cost(1e8, 5e5),
        name="slot_tables",
    )(routes, weights)


def dispatch_kernel(n, half, select, mine, theirs, *outs):
    split = mine.shape[0]
    picked = jnp.dot(select[:, :split], mine[...], preferred_element_type=F32)
    picked = picked + jnp.dot(select[:, split:], theirs[...], preferred_element_type=F32)
    for k in range(n):
        outs[k][...] = picked[k * half : (k + 1) * half, :].astype(BF16)


def dispatch(n, half, select, mine, theirs):
    width = mine.shape[1]
    return pl.pallas_call(
        functools.partial(dispatch_kernel, n, half),
        in_specs=[VMEM] * 3,
        out_specs=[VMEM] * n,
        out_shape=[jax.ShapeDtypeStruct((half, width), BF16)] * n,
        compiler_params=params(16),
        cost_estimate=cost(5e8, 2e6),
        name="dispatch",
    )(select, mine, theirs)


def fetch_kernel(*refs):
    half = (len(refs) - 1) // 2
    ins, outs, sems = refs[:half], refs[half:-1], refs[-1]
    copies = [
        pltpu.make_async_copy(src, dst, sems.at[i])
        for i, (src, dst) in enumerate(zip(ins, outs))
    ]
    for copy in copies:
        copy.start()
    for copy in copies:
        copy.wait()


def fetch(*arrays):
    return pl.pallas_call(
        fetch_kernel,
        in_specs=[HBM] * len(arrays),
        out_specs=[VMEM] * len(arrays),
        out_shape=[jax.ShapeDtypeStruct(a.shape, a.dtype) for a in arrays],
        scratch_shapes=[pltpu.SemaphoreType.DMA((len(arrays),))],
        compiler_params=params(16),
        cost_estimate=cost(2e9, 1e7),
        name="fetch",
    )(*arrays)


def expert_kernel(count, gate, widen, down, *refs):
    ins, (keep, send) = refs[: 2 * count], refs[2 * count :]
    rows = jnp.concatenate([piece[...] for piece in ins], axis=0)
    gated = contract1(rows, gate[...])
    lifted = contract1(rows, widen[...])
    hidden = (gated * jax.nn.sigmoid(gated) * lifted).astype(BF16)
    out = jnp.dot(hidden, down[...], preferred_element_type=F32)
    split = keep.shape[0]
    keep[...] = out[:split, :]
    send[...] = out[split:, :].astype(BF16)


def expert(weights, mine, theirs):
    count = len(mine)
    half, width = mine[0].shape
    return pl.pallas_call(
        functools.partial(expert_kernel, count),
        in_specs=[VMEM] * (3 + 2 * count),
        out_specs=[VMEM] * 2,
        out_shape=[
            jax.ShapeDtypeStruct((count * half, width), F32),
            jax.ShapeDtypeStruct((count * half, width), BF16),
        ],
        compiler_params=params(24),
        cost_estimate=cost(6e8 * count, 4e6),
    )(*weights, *mine, *theirs)


def merge_kernel(count, keep, received, *outs):
    half = outs[0].shape[0]
    for k in range(count):
        span = slice(k * half, (k + 1) * half)
        outs[k][...] = (keep[span, :] + received[span, :].astype(F32)).astype(BF16)


def merge(count, half, keep, received):
    width = keep.shape[1]
    return pl.pallas_call(
        functools.partial(merge_kernel, count),
        in_specs=[VMEM] * 2,
        out_specs=[VMEM] * count,
        out_shape=[jax.ShapeDtypeStruct((half, width), BF16)] * count,
        compiler_params=params(16),
        cost_estimate=cost(1e7, 4e6),
    )(keep, received)


def combine_kernel(n, high, low, *refs):
    ins, (keep, send) = refs[:n], refs[n:]
    rows = jnp.concatenate([piece[...] for piece in ins], axis=0)
    total = jnp.dot(high[...], rows, preferred_element_type=F32)
    total = total + jnp.dot(low[...], rows, preferred_element_type=F32)
    split = keep.shape[0]
    keep[...] = total[:split, :]
    send[...] = total[split:, :].astype(BF16)


def combine(n, high, low, pieces):
    width = pieces[0].shape[1]
    length = high.shape[0]
    return pl.pallas_call(
        functools.partial(combine_kernel, n),
        in_specs=[VMEM] * (2 + n),
        out_specs=[VMEM] * 2,
        out_shape=[
            jax.ShapeDtypeStruct((length // 2, width), F32),
            jax.ShapeDtypeStruct((length // 2, width), BF16),
        ],
        compiler_params=params(16),
        cost_estimate=cost(1e9, 3e6),
        name="combine",
    )(high, low, *pieces)


def swap(value, axis, k):
    return lax.ppermute(value, axis, xor_perm(axis, k))


def exchange(pieces):
    return [pieces[0]] + [swap(pieces[k], "sp", k) for k in range(1, len(pieces))]


def body(
    stream_in,
    queries,
    key_rows,
    values,
    decay_low,
    decay_matrix,
    decay_bias,
    decay_shift,
    head_gain,
    output_matrix,
    feed_gain,
    routes,
    route_weights,
    expert_gate,
    specialist_widen,
    expert_down,
):
    length = queries.shape[0]
    heads = queries.shape[1] // HK
    n = lax.axis_size("sp")
    head_devices = lax.axis_size("tp")
    groups = head_devices // 2
    rows = length // head_devices
    half = TOP * length // n // 2
    bias = decay_bias.reshape(1, -1)

    low, shift = decay_low.T, decay_shift.T
    count = heads // 2 if heads % 2 == 0 else heads

    gathered, states = [], None
    for part, first in enumerate(range(0, heads, count)):
        low_here = low
        if states is not None:
            low_here, states = lax.optimization_barrier((low, states))
        states = device_states(
            first, count, low_here, decay_matrix, bias, shift, key_rows, values
        )
        gathered.append(exchange(states))
    stream_in, _ = lax.optimization_barrier((stream_in, states))
    streams = [stream_in] + [swap(stream_in, "tp", 2 * k) for k in range(1, groups)]
    local = [
        local_attention(
            first, count, low, decay_matrix, bias, shift, queries, key_rows, values
        )
        for first in range(0, heads, count)
    ]
    select, high, low_part = slot_tables(
        n, half, groups, routes.T, route_weights.T
    )
    carried = []
    for part, pieces in enumerate(gathered):
        entry = quad_entry(count, pieces)
        carried += exchange(quad_prefix(count, True, entry, pieces))
    sides = project(
        count, groups, head_gain.reshape(1, -1), output_matrix, local, carried
    )
    received, shared = [], []
    for keep, send in sides:
        received.append(swap(send, "tp", 1))
        shared.append((keep + received[-1].astype(F32)).astype(BF16))
    arrived = [swap(value, "tp", 2 * k) for value in shared for k in range(1, groups)]
    weights, _ = lax.optimization_barrier(
        ((expert_gate[0].T, specialist_widen[0].T, expert_down[0]), shared)
    )
    weights = fetch(*weights)
    arrived, weights, select, high, low_part = lax.optimization_barrier(
        (arrived, weights, select, high, low_part)
    )
    normed, mid = midstream_norm(
        groups,
        feed_gain.reshape(1, -1),
        [keep for keep, _ in sides],
        received,
        streams,
        arrived,
    )
    theirs = swap(normed, "tp", 1)
    slots = dispatch(n, half, select, normed, theirs)
    slots = exchange(slots)
    back, previous = {}, None
    for part, ks in enumerate(expert_chunks(n)):
        mine = [slots[k] for k in ks]
        if previous is not None:
            mine, previous = lax.optimization_barrier((mine, previous))
        theirs = [swap(slot, "tp", 1) for slot in mine]
        kept, sent = expert(weights, mine, theirs)
        received = swap(sent, "tp", 1)
        merged = merge(len(ks), half, kept, received)
        previous = sent if part == 1 else merged
        for k, piece in zip(ks, merged):
            back[k] = piece if k == 0 else swap(piece, "sp", k)
    back = [back[k] for k in range(n)]
    keep, send = combine(n, high, low_part, back)
    summed = keep + swap(send, "tp", 1).astype(F32)
    total = mid + summed[:rows]
    for k in range(1, groups):
        part = summed[k * rows : (k + 1) * rows].astype(BF16)
        total = total + swap(part, "tp", 2 * k).astype(F32)
    return total.astype(BF16)


def expert_chunks(n):
    middle = (QUAD + n) // 2
    return [range(QUAD, middle), range(QUAD), range(middle, n)]


def solution(mesh):
    return jax.shard_map(
        body,
        mesh=mesh,
        in_specs=(
            P(("sp", "tp"), None),
            P("sp", "tp"),
            P("sp", "tp"),
            P("sp", "tp"),
            P("sp", None),
            P(None, "tp"),
            P("tp"),
            P("sp", "tp"),
            P(),
            P("tp", None),
            P(),
            P("sp", None),
            P("sp", None),
            P("sp", None, "tp"),
            P("sp", None, "tp"),
            P("sp", "tp", None),
        ),
        out_specs=P(("sp", "tp"), None),
        check_vma=False,
    )
```

```python
import functools
import jax
import jax.numpy as jnp
from jax import lax
from jax.experimental import pallas as pl
from jax.experimental.pallas import tpu as pltpu
from jax.sharding import PartitionSpec as P


HK = 256
HV = 512
TOP = 2
BLK = 128
TEMPER = 16.0
EPSILON = 1e-06
F32 = jnp.float32
BF16 = jnp.bfloat16
VMEM = pl.BlockSpec(memory_space=pltpu.VMEM)
SMEM = pl.BlockSpec(memory_space=pltpu.SMEM)
HBM = pl.BlockSpec(memory_space=pltpu.HBM)
QUAD = 4


def cost(flops, moved):
    return pl.CostEstimate(flops=int(flops), bytes_accessed=int(moved), transcendentals=0)


def params(mib):
    return pltpu.CompilerParams(vmem_limit_bytes=mib * 1024 * 1024)


def place():
    tp = lax.axis_index("tp")
    return lax.axis_index("sp"), tp % 2, tp // 2


def xor_perm(axis, k):
    return [(i, i ^ k) for i in range(lax.axis_size(axis))]


def tri(n, fn):
    row = lax.broadcasted_iota(jnp.int32, (n, n), 0)
    col = lax.broadcasted_iota(jnp.int32, (n, n), 1)
    return fn(row, col)


def contract0(a, b):
    return lax.dot_general(a, b, (((0,), (0,)), ((), ())), preferred_element_type=F32)


def contract1(a, b):
    return lax.dot_general(a, b, (((1,), (1,)), ((), ())), preferred_element_type=F32)


def split_dot(ones, value):
    total = None
    for _ in range(3):
        part = value.astype(BF16)
        value = value - part.astype(F32)
        term = jnp.dot(ones, part, preferred_element_type=F32)
        total = term if total is None else total + term
    return total


def head_log_decay(low, matrix, bias, shift, head):
    pre = contract0(low, matrix) + bias
    logged = (jnp.minimum(pre, 0.0) - jnp.log1p(jnp.exp(-jnp.abs(pre)))) / TEMPER
    return logged + jnp.transpose(shift)[:, head : head + 1]


def state_kernel(first, count, low, matrix, bias, shift, key_rows, values, *rest):
    outs = rest[:QUAD]
    keys, vals, state, decays, sems = rest[QUAD:]
    length = low.shape[1]
    piece = HK // QUAD
    copies = []
    for h in range(count):
        at = first + h
        pair = (
            pltpu.make_async_copy(
                key_rows.at[:, at * HK : (at + 1) * HK], keys.at[h], sems.at[0, h]
            ),
            pltpu.make_async_copy(
                values.at[:, at * HV : (at + 1) * HV], vals.at[h], sems.at[1, h]
            ),
        )
        for copy in pair:
            copy.start()
        copies.append(pair)
    after = tri(length, lambda r, c: c > r).astype(F32).astype(BF16)
    me = place()[0] % QUAD
    decays[...] = jnp.zeros_like(decays)
    for h in range(count):
        span = slice((first + h) * HK, (first + h + 1) * HK)
        logs = head_log_decay(low[...], matrix[:, span], bias[:, span], shift[...], first + h)
        suffix = split_dot(after, logs)
        total = jnp.exp(suffix[0:1, :] + logs[0:1, :])
        high = total.astype(BF16).astype(F32)
        decays[h : h + 1, 0:HK] = high
        decays[h : h + 1, HK : 2 * HK] = total - high
        for copy in copies[h]:
            copy.wait()
        end_keys = (keys[h].astype(F32) * jnp.exp(suffix)).astype(BF16)
        state[...] = contract0(end_keys, vals[h])
        for k in range(QUAD):
            start = pl.multiple_of((me ^ k) * piece, piece)
            outs[k][h * piece : (h + 1) * piece, :] = state[pl.ds(start, piece), :].astype(BF16)
    for k in range(QUAD):
        outs[k][count * piece :, :] = decays[...].astype(BF16)


def device_states(first, count, low, matrix, bias, shift, key_rows, values):
    length = key_rows.shape[0]
    rows = count * (HK // QUAD) + 8
    return pl.pallas_call(
        functools.partial(state_kernel, first, count),
        in_specs=[VMEM] * 4 + [HBM] * 2,
        out_specs=[VMEM] * QUAD,
        out_shape=[jax.ShapeDtypeStruct((rows, HV), BF16)] * QUAD,
        scratch_shapes=[
            pltpu.VMEM((count, length, HK), BF16),
            pltpu.VMEM((count, length, HV), BF16),
            pltpu.VMEM((HK, HV), F32),
            pltpu.VMEM((8, HV), F32),
            pltpu.SemaphoreType.DMA((2, count)),
        ],
        compiler_params=params(60),
        cost_estimate=cost(count * 4e8, count * 5e5),
    )(low, matrix, bias, shift, key_rows, values)


def local_kernel(first, count, low, matrix, bias, shift, queries, key_rows, values, *refs):
    out, query_out = refs[-2:]
    length = low.shape[1]
    below = tri(BLK, lambda r, c: c <= r)
    lower = below.astype(F32).astype(BF16)
    scale = HK ** (-0.5)
    for h in range(count):
        narrow, wide = slice(h * HK, (h + 1) * HK), slice(h * HV, (h + 1) * HV)
        logs = head_log_decay(
            low[...], matrix[:, narrow], bias[:, narrow], shift[...], first + h
        )
        before = jnp.zeros((1, HK), F32)
        earlier = []
        for b in range(length // BLK):
            rows = slice(b * BLK, (b + 1) * BLK)
            inside = split_dot(lower, logs[rows])
            final = inside[BLK - 1 : BLK, :]
            middle = inside[BLK // 2 - 1 : BLK // 2, :]
            query = queries[rows, narrow].astype(F32) * scale
            keys = key_rows[rows, narrow].astype(F32)
            grown = query * jnp.exp(inside)
            near_query = (query * jnp.exp(inside - middle)).astype(BF16)
            near_key = (keys * jnp.exp(middle - inside)).astype(BF16)
            scores = jnp.where(below, contract1(near_query, near_key), 0.0).astype(BF16)
            total = jnp.dot(scores, values[rows, wide], preferred_element_type=F32)
            here = grown.astype(BF16)
            for past_keys, past in earlier:
                cross = contract1(here, past_keys.astype(BF16)).astype(BF16)
                total = total + jnp.dot(cross, values[past, wide], preferred_element_type=F32)
            out[rows, wide] = total
            query_out[rows, narrow] = (grown * jnp.exp(before)).astype(BF16)
            if b + 1 < length // BLK:
                earlier = [(old * jnp.exp(final), past) for old, past in earlier]
                earlier.append((keys * jnp.exp(final - inside), rows))
                before = before + final


def local_attention(first, count, low, matrix, bias, shift, queries, key_rows, values):
    length = low.shape[1]
    block = first // count

    def part(width):
        return pl.BlockSpec((length, count * width), lambda i: (0, block))

    return pl.pallas_call(
        functools.partial(local_kernel, first, count),
        grid=(1,),
        in_specs=[
            pl.BlockSpec(low.shape, lambda i: (0, 0)),
            pl.BlockSpec((low.shape[0], count * HK), lambda i: (0, block)),
            pl.BlockSpec((1, count * HK), lambda i: (0, block)),
            pl.BlockSpec(shift.shape, lambda i: (0, 0)),
            part(HK),
            part(HK),
            part(HV),
        ],
        out_specs=[
            pl.BlockSpec((length, count * HV), lambda i: (0, 0)),
            pl.BlockSpec((length, count * HK), lambda i: (0, 0)),
        ],
        out_shape=[
            jax.ShapeDtypeStruct((length, count * HV), F32),
            jax.ShapeDtypeStruct((length, count * HK), BF16),
        ],
        compiler_params=params(24),
        cost_estimate=cost(count * 4e8, count * 1.2e6),
    )(low, matrix, bias, shift, queries, key_rows, values)


def prefix_kernel(count, emit, primed, *refs):
    start, refs = (refs[0], refs[1:]) if primed else (None, refs)
    ins, outs = refs[:QUAD], refs[QUAD:]
    me = place()[0] % QUAD
    piece = HK // QUAD
    rows = count * piece
    tails = jnp.concatenate([ref[rows : rows + 8, :].astype(F32) for ref in ins], axis=0)
    across = jnp.transpose(tails[:, :HK] + tails[:, HK:])
    parts = [across[i * piece : (i + 1) * piece, :] for i in range(QUAD)]
    mine = parts[0]
    for i in range(1, QUAD):
        mine = jnp.where(me == i, parts[i], mine)
    decay = [mine[:, k * 8 : k * 8 + count] for k in range(QUAD)]
    spot = [me ^ k for k in range(QUAD)]
    ends = spot if emit else [jnp.int32(QUAD)]

    def between(low, end):
        factor = jnp.ones_like(decay[0])
        for k in range(QUAD):
            inside = jnp.logical_and(spot[k] > low, spot[k] < end)
            factor = jnp.where(inside, factor * decay[k], factor)
        return factor

    weights = [
        [jnp.where(spot[k] < end, between(spot[k], end), 0.0) for k in range(QUAD)]
        + ([between(-1, end)] if primed else [])
        for end in ends
    ]
    for h in range(count):
        span = slice(h * piece, (h + 1) * piece)
        sources = [ref[span, :].astype(F32) for ref in ins]
        if primed:
            sources.append(start[span, :].astype(F32))
        for out, factors in zip(outs, weights):
            total = None
            for source, factor in zip(sources, factors):
                term = source * factor[:, h : h + 1]
                total = term if total is None else total + term
            out[span, :] = total.astype(BF16)


def quad_prefix(count, emit, start, pieces):
    rows = count * (HK // QUAD)
    outs = QUAD if emit else 1
    primed = [] if start is None else [start]
    return pl.pallas_call(
        functools.partial(prefix_kernel, count, emit, start is not None),
        in_specs=[VMEM] * (QUAD + len(primed)),
        out_specs=[VMEM] * outs,
        out_shape=[jax.ShapeDtypeStruct((rows, HV), BF16)] * outs,
        compiler_params=params(24),
        cost_estimate=cost(1e8, 1e6),
        name="quad_prefix" if emit else "quad_total",
    )(*primed, *pieces)


def quad_entry(count, pieces):
    start = None
    quads = lax.axis_size("sp") // QUAD
    entry = None
    for g in range(quads - 1):
        (total,) = quad_prefix(count, False, start, pieces)
        perm = [(g * QUAD + i, (g + 1) * QUAD + i) for i in range(QUAD)]
        start = lax.ppermute(total, "sp", perm)
        entry = start if entry is None else entry + start
    return entry


def block_spans(groups, rows):
    _, core, line = place()
    for k in range(groups):
        base = (line ^ k) * 2
        own = pl.ds(pl.multiple_of((base + core) * rows, rows), rows)
        other = pl.ds(pl.multiple_of((base + 1 - core) * rows, rows), rows)
        yield slice(k * rows, (k + 1) * rows), own, other


def project_kernel(count, groups, gain, matrix, *refs):
    mixed, keep, send, carried = refs[-4:]
    chunks = len(refs[:-4]) // (2 + QUAD)
    local, queries, pieces = refs[:chunks], refs[chunks : 2 * chunks], refs[2 * chunks : -4]
    me, my_core, my_line = place()
    me = me % QUAD
    piece = HK // QUAD
    split = keep.shape[0]
    rows = split // groups
    for part in range(chunks):
        for h in range(count):
            span = slice(h * piece, (h + 1) * piece)
            for k in range(QUAD):
                start = pl.multiple_of((me ^ k) * piece, piece)
                carried[pl.ds(start, piece), :] = pieces[part * QUAD + k][span, :]
            narrow, wide = slice(h * HK, (h + 1) * HK), slice(h * HV, (h + 1) * HV)
            out = local[part][:, wide] + jnp.dot(
                queries[part][:, narrow], carried[...], preferred_element_type=F32
            )
            spread = lax.rsqrt(jnp.mean(out * out, axis=-1, keepdims=True) + EPSILON)
            value = (out * spread * gain[...]).astype(BF16)
            at = (part * count + h) * HV
            for b in range(2 * groups):
                line, core = b // 2, b % 2
                there = (line ^ my_line) + (core ^ my_core) * groups
                there = pl.multiple_of(there * rows, rows)
                mixed[pl.ds(there, rows), at : at + HV] = value[b * rows : (b + 1) * rows, :]
    keep[...] = jnp.dot(mixed[:split, :], matrix[...], preferred_element_type=F32)
    send[...] = jnp.dot(mixed[split:, :], matrix[...], preferred_element_type=F32).astype(BF16)


def project_rest_kernel(mixed, matrix, keep, send):
    split = keep.shape[0]
    total = jnp.dot(mixed[...], matrix[...], preferred_element_type=F32)
    keep[...] = total[:split, :]
    send[...] = total[split:, :].astype(BF16)


def project(count, groups, gain, matrix, local, pieces):
    outs = [array for array, _ in local] + [array for _, array in local]
    length = outs[0].shape[0]
    depth, width = matrix.shape
    cut = width // 2
    small = [
        jax.ShapeDtypeStruct((length // 2, cut), F32),
        jax.ShapeDtypeStruct((length // 2, cut), BF16),
    ]
    whole = [pl.BlockSpec((length // 2, cut), lambda i: (0, 0))] * 2
    mixed, keep, send = pl.pallas_call(
        functools.partial(project_kernel, count, groups),
        grid=(1,),
        in_specs=[VMEM, pl.BlockSpec((depth, cut), lambda i: (0, 0))]
        + [VMEM] * (len(outs) + len(pieces)),
        out_specs=[pl.BlockSpec((length, depth), lambda i: (0, 0))] + whole,
        out_shape=[jax.ShapeDtypeStruct((length, depth), BF16)] + small,
        scratch_shapes=[pltpu.VMEM((HK, HV), BF16)],
        compiler_params=params(28),
        cost_estimate=cost(2e9, 8e6),
        name="project",
    )(gain, matrix, *outs, *pieces)
    rest = pl.pallas_call(
        project_rest_kernel,
        grid=(1,),
        in_specs=[
            pl.BlockSpec((length, depth), lambda i: (0, 0)),
            pl.BlockSpec((depth, cut), lambda i: (0, 1)),
        ],
        out_specs=whole,
        out_shape=small,
        compiler_params=params(28),
        cost_estimate=cost(1e9, 6e6),
        name="project_rest",
    )(mixed, matrix)
    return (keep, send), rest


def norm_kernel(groups, gain, *refs):
    keeps, received, streams = refs[:2], refs[2:4], refs[4 : 4 + groups]
    arrived = refs[4 + groups : 4 + groups + 2 * (groups - 1)]
    normed, mid = refs[-2:]
    rows, width = mid.shape
    cut = width // 2
    for k in range(groups):
        span = slice(k * rows, (k + 1) * rows)
        values, square = [], None
        for side in range(2):
            columns = slice(side * cut, (side + 1) * cut)
            value = keeps[side][span, :] + received[side][span, :].astype(F32)
            for j in range(1, groups):
                there = k ^ j
                part = arrived[side * (groups - 1) + j - 1]
                value = value + part[there * rows : (there + 1) * rows, :].astype(F32)
            value = value + streams[k][:, columns].astype(F32)
            if k == 0:
                mid[:, columns] = value
            term = jnp.sum(value * value, axis=-1, keepdims=True)
            square = term if square is None else square + term
            values.append((columns, value))
        spread = lax.rsqrt(square / width + EPSILON)
        for columns, value in values:
            normed[span, columns] = (value * spread * gain[:, columns]).astype(BF16)


def midstream_norm(groups, gain, keeps, received, streams, arrived):
    rows, width = streams[0].shape
    arrays = [*keeps, *received, *streams, *arrived]
    return pl.pallas_call(
        functools.partial(norm_kernel, groups),
        in_specs=[VMEM] * (1 + len(arrays)),
        out_specs=[VMEM] * 2,
        out_shape=[
            jax.ShapeDtypeStruct((groups * rows, width), BF16),
            jax.ShapeDtypeStruct((rows, width), F32),
        ],
        compiler_params=params(24),
        cost_estimate=cost(1e7, 3e6),
        name="midstream_norm",
    )(gain, *arrays)


def route_kernel(n, half, groups, routes, weights, select, high, low, table):
    me, core, _ = place()
    length = routes.shape[1]
    earlier = tri(length, lambda r, c: c < r).astype(F32).astype(BF16)
    chosen = jnp.transpose(routes[...].astype(F32)).astype(jnp.int32)
    weight = jnp.transpose(weights[...])
    expert = me ^ lax.broadcasted_iota(jnp.int32, (length, n), 1)
    is_first, is_second = chosen[:, 0:1] == expert, chosen[:, 1:2] == expert
    member = jnp.where(is_first | is_second, 1.0, 0.0)
    rank = jnp.dot(earlier, member.astype(BF16), preferred_element_type=F32)
    slot = jnp.where(member > 0.0, rank, -1.0)
    value = jnp.where(is_first, weight[:, 0:1], weight[:, 1:2])
    top = value.astype(BF16)
    rest = (value - top.astype(F32)).astype(BF16)
    column = lax.broadcasted_iota(jnp.int32, (n, n * half), 1)
    owner = lax.broadcasted_iota(jnp.int32, (n, n * half), 0)
    spread = jnp.where(column // half == owner, 1.0, 0.0).astype(BF16)

    def widen(array):
        return jnp.dot(array, spread, preferred_element_type=F32)

    wanted = core * half + lax.broadcasted_iota(jnp.int32, (length, n * half), 1) % half
    hit = widen(slot.astype(BF16)) == wanted.astype(F32)
    table[0] = jnp.where(hit, 1.0, 0.0)
    table[1] = jnp.where(hit, widen(top), 0.0)
    table[2] = jnp.where(hit, widen(rest), 0.0)
    split = length // 2
    ordered = []
    for span, own, other in block_spans(groups, split // groups):
        below = slice(split + span.start, split + span.stop)
        for out, source in ((high, 1), (low, 2)):
            out[span, :] = table[source, own, :].astype(BF16)
            out[below, :] = table[source, other, :].astype(BF16)
        ordered.append((table[0, own, :], table[0, other, :]))
    chosen = jnp.concatenate([own for own, _ in ordered] + [other for _, other in ordered])
    select[...] = jnp.transpose(chosen).astype(BF16)


def slot_tables(n, half, groups, routes, weights):
    length = routes.shape[1]
    return pl.pallas_call(
        functools.partial(route_kernel, n, half, groups),
        in_specs=[VMEM, VMEM],
        out_specs=[VMEM] * 3,
        out_shape=[
            jax.ShapeDtypeStruct((n * half, length), BF16),
            jax.ShapeDtypeStruct((length, n * half), BF16),
            jax.ShapeDtypeStruct((length, n * half), BF16),
        ],
        scratch_shapes=[pltpu.VMEM((3, length, n * half), F32)],
        compiler_params=params(16),
        cost_estimate=cost(1e8, 5e5),
        name="slot_tables",
    )(routes, weights)


def dispatch_kernel(n, half, select, mine, theirs, *outs):
    split = mine.shape[0]
    picked = jnp.dot(select[:, :split], mine[...], preferred_element_type=F32)
    picked = picked + jnp.dot(select[:, split:], theirs[...], preferred_element_type=F32)
    for k in range(n):
        outs[k][...] = picked[k * half : (k + 1) * half, :].astype(BF16)


def dispatch(n, half, select, mine, theirs):
    width = mine.shape[1]
    return pl.pallas_call(
        functools.partial(dispatch_kernel, n, half),
        in_specs=[VMEM] * 3,
        out_specs=[VMEM] * n,
        out_shape=[jax.ShapeDtypeStruct((half, width), BF16)] * n,
        compiler_params=params(16),
        cost_estimate=cost(5e8, 2e6),
        name="dispatch",
    )(select, mine, theirs)


def fetch_kernel(*refs):
    half = (len(refs) - 1) // 2
    ins, outs, sems = refs[:half], refs[half:-1], refs[-1]
    copies = [
        pltpu.make_async_copy(src, dst, sems.at[i])
        for i, (src, dst) in enumerate(zip(ins, outs))
    ]
    for copy in copies:
        copy.start()
    for copy in copies:
        copy.wait()


def fetch(*arrays):
    return pl.pallas_call(
        fetch_kernel,
        in_specs=[HBM] * len(arrays),
        out_specs=[VMEM] * len(arrays),
        out_shape=[jax.ShapeDtypeStruct(a.shape, a.dtype) for a in arrays],
        scratch_shapes=[pltpu.SemaphoreType.DMA((len(arrays),))],
        compiler_params=params(16),
        cost_estimate=cost(2e9, 1e7),
        name="fetch",
    )(*arrays)


def expert_kernel(count, gate, widen, down, *refs):
    ins, (keep, send) = refs[: 2 * count], refs[2 * count :]
    rows = jnp.concatenate([piece[...] for piece in ins], axis=0)
    gated = contract1(rows, gate[...])
    lifted = contract1(rows, widen[...])
    hidden = (gated * jax.nn.sigmoid(gated) * lifted).astype(BF16)
    out = jnp.dot(hidden, down[...], preferred_element_type=F32)
    split = keep.shape[0]
    keep[...] = out[:split, :]
    send[...] = out[split:, :].astype(BF16)


def expert(weights, mine, theirs):
    count = len(mine)
    half, width = mine[0].shape
    return pl.pallas_call(
        functools.partial(expert_kernel, count),
        in_specs=[VMEM] * (3 + 2 * count),
        out_specs=[VMEM] * 2,
        out_shape=[
            jax.ShapeDtypeStruct((count * half, width), F32),
            jax.ShapeDtypeStruct((count * half, width), BF16),
        ],
        compiler_params=params(24),
        cost_estimate=cost(6e8 * count, 4e6),
    )(*weights, *mine, *theirs)


def merge_kernel(count, keep, received, *outs):
    half = outs[0].shape[0]
    for k in range(count):
        span = slice(k * half, (k + 1) * half)
        outs[k][...] = (keep[span, :] + received[span, :].astype(F32)).astype(BF16)


def merge(count, half, keep, received):
    width = keep.shape[1]
    return pl.pallas_call(
        functools.partial(merge_kernel, count),
        in_specs=[VMEM] * 2,
        out_specs=[VMEM] * count,
        out_shape=[jax.ShapeDtypeStruct((half, width), BF16)] * count,
        compiler_params=params(16),
        cost_estimate=cost(1e7, 4e6),
    )(keep, received)


def combine_kernel(n, high, low, *refs):
    ins, (keep, send) = refs[:n], refs[n:]
    rows = jnp.concatenate([piece[...] for piece in ins], axis=0)
    total = jnp.dot(high[...], rows, preferred_element_type=F32)
    total = total + jnp.dot(low[...], rows, preferred_element_type=F32)
    split = keep.shape[0]
    keep[...] = total[:split, :]
    send[...] = total[split:, :].astype(BF16)


def combine(n, side, high, low, pieces):
    half, width = pieces[0].shape
    length, slots = high.shape
    cut = width // 2
    table = pl.BlockSpec((length, slots), lambda i: (0, 0))
    return pl.pallas_call(
        functools.partial(combine_kernel, n),
        grid=(1,),
        in_specs=[table] * 2 + [pl.BlockSpec((half, cut), lambda i: (0, side))] * n,
        out_specs=[pl.BlockSpec((length // 2, cut), lambda i: (0, 0))] * 2,
        out_shape=[
            jax.ShapeDtypeStruct((length // 2, cut), F32),
            jax.ShapeDtypeStruct((length // 2, cut), BF16),
        ],
        compiler_params=params(16),
        cost_estimate=cost(5e8, 2e6),
    )(high, low, *pieces)


def final_kernel(groups, mid, *refs):
    keeps, received, parts, out = refs[:2], refs[2:4], refs[4:-1], refs[-1]
    rows, width = mid.shape
    cut = width // 2
    for side in range(2):
        columns = slice(side * cut, (side + 1) * cut)
        total = mid[:, columns] + keeps[side][:rows, :] + received[side][:rows, :].astype(F32)
        for k in range(groups - 1):
            total = total + parts[side * (groups - 1) + k][...].astype(F32)
        out[:, columns] = total.astype(BF16)


def final(groups, mid, keeps, received, parts):
    arrays = [*keeps, *received, *parts]
    return pl.pallas_call(
        functools.partial(final_kernel, groups),
        in_specs=[VMEM] * (1 + len(arrays)),
        out_specs=VMEM,
        out_shape=jax.ShapeDtypeStruct(mid.shape, BF16),
        compiler_params=params(16),
        cost_estimate=cost(1e6, 2e6),
        name="final",
    )(mid, *arrays)


def swap(value, axis, k):
    return lax.ppermute(value, axis, xor_perm(axis, k))


def exchange(pieces):
    return [pieces[0]] + [swap(pieces[k], "sp", k) for k in range(1, len(pieces))]


def body(
    stream_in,
    queries,
    key_rows,
    values,
    decay_low,
    decay_matrix,
    decay_bias,
    decay_shift,
    head_gain,
    output_matrix,
    feed_gain,
    routes,
    route_weights,
    expert_gate,
    specialist_widen,
    expert_down,
):
    length = queries.shape[0]
    heads = queries.shape[1] // HK
    n = lax.axis_size("sp")
    head_devices = lax.axis_size("tp")
    groups = head_devices // 2
    rows = length // head_devices
    half = TOP * length // n // 2
    bias = decay_bias.reshape(1, -1)

    low, shift = decay_low.T, decay_shift.T
    count = heads // 2 if heads % 2 == 0 else heads

    gathered, states = [], None
    for part, first in enumerate(range(0, heads, count)):
        low_here = low
        if states is not None:
            low_here, states = lax.optimization_barrier((low, states))
        states = device_states(
            first, count, low_here, decay_matrix, bias, shift, key_rows, values
        )
        gathered.append(exchange(states))
    stream_in, _ = lax.optimization_barrier((stream_in, states))
    streams = [stream_in] + [swap(stream_in, "tp", 2 * k) for k in range(1, groups)]
    local = [
        local_attention(
            first, count, low, decay_matrix, bias, shift, queries, key_rows, values
        )
        for first in range(0, heads, count)
    ]
    select, high, low_part = slot_tables(
        n, half, groups, routes.T, route_weights.T
    )
    carried = []
    for part, pieces in enumerate(gathered):
        entry = quad_entry(count, pieces)
        carried += exchange(quad_prefix(count, True, entry, pieces))
    sides = project(
        count, groups, head_gain.reshape(1, -1), output_matrix, local, carried
    )
    received, shared = [], []
    for keep, send in sides:
        received.append(swap(send, "tp", 1))
        shared.append((keep + received[-1].astype(F32)).astype(BF16))
    arrived = [swap(value, "tp", 2 * k) for value in shared for k in range(1, groups)]
    weights, _ = lax.optimization_barrier(
        ((expert_gate[0].T, specialist_widen[0].T, expert_down[0]), shared)
    )
    weights = fetch(*weights)
    arrived, weights, select, high, low_part = lax.optimization_barrier(
        (arrived, weights, select, high, low_part)
    )
    normed, mid = midstream_norm(
        groups,
        feed_gain.reshape(1, -1),
        [keep for keep, _ in sides],
        received,
        streams,
        arrived,
    )
    theirs = swap(normed, "tp", 1)
    slots = dispatch(n, half, select, normed, theirs)
    slots = exchange(slots)
    back, previous = {}, None
    for part, ks in enumerate(expert_chunks(n)):
        mine = [slots[k] for k in ks]
        if previous is not None:
            mine, previous = lax.optimization_barrier((mine, previous))
        theirs = [swap(slot, "tp", 1) for slot in mine]
        kept, sent = expert(weights, mine, theirs)
        received = swap(sent, "tp", 1)
        merged = merge(len(ks), half, kept, received)
        previous = sent if part == 1 else merged
        for k, piece in zip(ks, merged):
            back[k] = piece if k == 0 else swap(piece, "sp", k)
    back = [back[k] for k in range(n)]
    keeps, received, parts = [], [], []
    for side in range(2):
        keep, send = combine(n, side, high, low_part, back)
        other = swap(send, "tp", 1)
        for k in range(1, groups):
            span = slice(k * rows, (k + 1) * rows)
            part = (keep[span] + other[span].astype(F32)).astype(BF16)
            parts.append(swap(part, "tp", 2 * k))
        keeps.append(keep)
        received.append(other)
    return final(groups, mid, keeps, received, parts)


def expert_chunks(n):
    middle = (QUAD + n) // 2
    return [range(QUAD, middle), range(QUAD), range(middle, n)]


def solution(mesh):
    return jax.shard_map(
        body,
        mesh=mesh,
        in_specs=(
            P(("sp", "tp"), None),
            P("sp", "tp"),
            P("sp", "tp"),
            P("sp", "tp"),
            P("sp", None),
            P(None, "tp"),
            P("tp"),
            P("sp", "tp"),
            P(),
            P("tp", None),
            P(),
            P("sp", None),
            P("sp", None),
            P("sp", None, "tp"),
            P("sp", None, "tp"),
            P("sp", "tp", None),
        ),
        out_specs=P(("sp", "tp"), None),
        check_vma=False,
    )
```

```python
import functools
import jax
import jax.numpy as jnp
from jax import lax
from jax.experimental import pallas as pl
from jax.experimental.pallas import tpu as pltpu
from jax.sharding import PartitionSpec as P


HK = 256
HV = 512
TOP = 2
BLK = 128
TEMPER = 16.0
EPSILON = 1e-06
F32 = jnp.float32
BF16 = jnp.bfloat16
VMEM = pl.BlockSpec(memory_space=pltpu.VMEM)
SMEM = pl.BlockSpec(memory_space=pltpu.SMEM)
HBM = pl.BlockSpec(memory_space=pltpu.HBM)
QUAD = 4


def cost(flops, moved):
    return pl.CostEstimate(flops=int(flops), bytes_accessed=int(moved), transcendentals=0)


def params(mib):
    return pltpu.CompilerParams(vmem_limit_bytes=mib * 1024 * 1024)


def place():
    tp = lax.axis_index("tp")
    return lax.axis_index("sp"), tp % 2, tp // 2


def xor_perm(axis, k):
    return [(i, i ^ k) for i in range(lax.axis_size(axis))]


def tri(n, fn):
    row = lax.broadcasted_iota(jnp.int32, (n, n), 0)
    col = lax.broadcasted_iota(jnp.int32, (n, n), 1)
    return fn(row, col)


def contract0(a, b):
    return lax.dot_general(a, b, (((0,), (0,)), ((), ())), preferred_element_type=F32)


def contract1(a, b):
    return lax.dot_general(a, b, (((1,), (1,)), ((), ())), preferred_element_type=F32)


def split_dot(ones, value):
    total = None
    for _ in range(3):
        part = value.astype(BF16)
        value = value - part.astype(F32)
        term = jnp.dot(ones, part, preferred_element_type=F32)
        total = term if total is None else total + term
    return total


def head_log_decay(low, matrix, bias, shift, head):
    pre = contract0(low, matrix) + bias
    logged = (jnp.minimum(pre, 0.0) - jnp.log1p(jnp.exp(-jnp.abs(pre)))) / TEMPER
    return logged + jnp.transpose(shift)[:, head : head + 1]


def state_kernel(first, count, low, matrix, bias, shift, key_rows, values, *rest):
    outs, (state, decays) = rest[:QUAD], rest[QUAD:]
    length = low.shape[1]
    piece = HK // QUAD
    after = tri(length, lambda r, c: c > r).astype(F32).astype(BF16)
    me = place()[0] % QUAD
    decays[...] = jnp.zeros_like(decays)
    for h in range(count):
        narrow, wide = slice(h * HK, (h + 1) * HK), slice(h * HV, (h + 1) * HV)
        logs = head_log_decay(
            low[...], matrix[:, narrow], bias[:, narrow], shift[...], first + h
        )
        suffix = split_dot(after, logs)
        total = jnp.exp(suffix[0:1, :] + logs[0:1, :])
        high = total.astype(BF16).astype(F32)
        decays[h : h + 1, 0:HK] = high
        decays[h : h + 1, HK : 2 * HK] = total - high
        end_keys = (key_rows[:, narrow].astype(F32) * jnp.exp(suffix)).astype(BF16)
        state[...] = contract0(end_keys, values[:, wide])
        for k in range(QUAD):
            start = pl.multiple_of((me ^ k) * piece, piece)
            outs[k][h * piece : (h + 1) * piece, :] = state[pl.ds(start, piece), :].astype(BF16)
    for k in range(QUAD):
        outs[k][count * piece :, :] = decays[...].astype(BF16)


def device_states(first, count, low, matrix, bias, shift, key_rows, values):
    length = key_rows.shape[0]
    rows = count * (HK // QUAD) + 8
    block = first // count

    def whole(array):
        return pl.BlockSpec(array.shape, lambda i: (0, 0))

    def part(height, width):
        return pl.BlockSpec((height, count * width), lambda i: (0, block))

    return pl.pallas_call(
        functools.partial(state_kernel, first, count),
        grid=(1,),
        in_specs=[
            whole(low),
            part(matrix.shape[0], HK),
            part(1, HK),
            whole(shift),
            part(length, HK),
            part(length, HV),
        ],
        out_specs=[pl.BlockSpec((rows, HV), lambda i: (0, 0))] * QUAD,
        out_shape=[jax.ShapeDtypeStruct((rows, HV), BF16)] * QUAD,
        scratch_shapes=[pltpu.VMEM((HK, HV), F32), pltpu.VMEM((8, HV), F32)],
        compiler_params=params(60),
        cost_estimate=cost(count * 4e8, count * 5e5),
    )(low, matrix, bias, shift, key_rows, values)


def local_kernel(first, count, low, matrix, bias, shift, queries, key_rows, values, *refs):
    out, query_out = refs[-2:]
    length = low.shape[1]
    below = tri(BLK, lambda r, c: c <= r)
    lower = below.astype(F32).astype(BF16)
    scale = HK ** (-0.5)
    for h in range(count):
        narrow, wide = slice(h * HK, (h + 1) * HK), slice(h * HV, (h + 1) * HV)
        logs = head_log_decay(
            low[...], matrix[:, narrow], bias[:, narrow], shift[...], first + h
        )
        before = jnp.zeros((1, HK), F32)
        earlier = []
        for b in range(length // BLK):
            rows = slice(b * BLK, (b + 1) * BLK)
            inside = split_dot(lower, logs[rows])
            final = inside[BLK - 1 : BLK, :]
            middle = inside[BLK // 2 - 1 : BLK // 2, :]
            query = queries[rows, narrow].astype(F32) * scale
            keys = key_rows[rows, narrow].astype(F32)
            grown = query * jnp.exp(inside)
            near_query = (query * jnp.exp(inside - middle)).astype(BF16)
            near_key = (keys * jnp.exp(middle - inside)).astype(BF16)
            scores = jnp.where(below, contract1(near_query, near_key), 0.0).astype(BF16)
            total = jnp.dot(scores, values[rows, wide], preferred_element_type=F32)
            here = grown.astype(BF16)
            for past_keys, past in earlier:
                cross = contract1(here, past_keys.astype(BF16)).astype(BF16)
                total = total + jnp.dot(cross, values[past, wide], preferred_element_type=F32)
            out[rows, wide] = total
            query_out[rows, narrow] = (grown * jnp.exp(before)).astype(BF16)
            if b + 1 < length // BLK:
                earlier = [(old * jnp.exp(final), past) for old, past in earlier]
                earlier.append((keys * jnp.exp(final - inside), rows))
                before = before + final


def local_attention(first, count, low, matrix, bias, shift, queries, key_rows, values):
    length = low.shape[1]
    block = first // count

    def part(width):
        return pl.BlockSpec((length, count * width), lambda i: (0, block))

    return pl.pallas_call(
        functools.partial(local_kernel, first, count),
        grid=(1,),
        in_specs=[
            pl.BlockSpec(low.shape, lambda i: (0, 0)),
            pl.BlockSpec((low.shape[0], count * HK), lambda i: (0, block)),
            pl.BlockSpec((1, count * HK), lambda i: (0, block)),
            pl.BlockSpec(shift.shape, lambda i: (0, 0)),
            part(HK),
            part(HK),
            part(HV),
        ],
        out_specs=[
            pl.BlockSpec((length, count * HV), lambda i: (0, 0)),
            pl.BlockSpec((length, count * HK), lambda i: (0, 0)),
        ],
        out_shape=[
            jax.ShapeDtypeStruct((length, count * HV), F32),
            jax.ShapeDtypeStruct((length, count * HK), BF16),
        ],
        compiler_params=params(24),
        cost_estimate=cost(count * 4e8, count * 1.2e6),
    )(low, matrix, bias, shift, queries, key_rows, values)


def prefix_kernel(count, emit, primed, *refs):
    start, refs = (refs[0], refs[1:]) if primed else (None, refs)
    ins, outs = refs[:QUAD], refs[QUAD:]
    me = place()[0] % QUAD
    piece = HK // QUAD
    rows = count * piece
    tails = jnp.concatenate([ref[rows : rows + 8, :].astype(F32) for ref in ins], axis=0)
    across = jnp.transpose(tails[:, :HK] + tails[:, HK:])
    parts = [across[i * piece : (i + 1) * piece, :] for i in range(QUAD)]
    mine = parts[0]
    for i in range(1, QUAD):
        mine = jnp.where(me == i, parts[i], mine)
    decay = [mine[:, k * 8 : k * 8 + count] for k in range(QUAD)]
    spot = [me ^ k for k in range(QUAD)]
    ends = spot if emit else [jnp.int32(QUAD)]

    def between(low, end):
        factor = jnp.ones_like(decay[0])
        for k in range(QUAD):
            inside = jnp.logical_and(spot[k] > low, spot[k] < end)
            factor = jnp.where(inside, factor * decay[k], factor)
        return factor

    weights = [
        [jnp.where(spot[k] < end, between(spot[k], end), 0.0) for k in range(QUAD)]
        + ([between(-1, end)] if primed else [])
        for end in ends
    ]
    for h in range(count):
        span = slice(h * piece, (h + 1) * piece)
        sources = [ref[span, :].astype(F32) for ref in ins]
        if primed:
            sources.append(start[span, :].astype(F32))
        for out, factors in zip(outs, weights):
            total = None
            for source, factor in zip(sources, factors):
                term = source * factor[:, h : h + 1]
                total = term if total is None else total + term
            out[span, :] = total.astype(BF16)


def quad_prefix(count, emit, start, pieces):
    rows = count * (HK // QUAD)
    outs = QUAD if emit else 1
    primed = [] if start is None else [start]
    return pl.pallas_call(
        functools.partial(prefix_kernel, count, emit, start is not None),
        in_specs=[VMEM] * (QUAD + len(primed)),
        out_specs=[VMEM] * outs,
        out_shape=[jax.ShapeDtypeStruct((rows, HV), BF16)] * outs,
        compiler_params=params(24),
        cost_estimate=cost(1e8, 1e6),
        name="quad_prefix" if emit else "quad_total",
    )(*primed, *pieces)


def quad_entry(count, pieces):
    start = None
    quads = lax.axis_size("sp") // QUAD
    entry = None
    for g in range(quads - 1):
        (total,) = quad_prefix(count, False, start, pieces)
        perm = [(g * QUAD + i, (g + 1) * QUAD + i) for i in range(QUAD)]
        start = lax.ppermute(total, "sp", perm)
        entry = start if entry is None else entry + start
    return entry


def block_spans(groups, rows):
    _, core, line = place()
    for k in range(groups):
        base = (line ^ k) * 2
        own = pl.ds(pl.multiple_of((base + core) * rows, rows), rows)
        other = pl.ds(pl.multiple_of((base + 1 - core) * rows, rows), rows)
        yield slice(k * rows, (k + 1) * rows), own, other


def read_heads(count, groups, gain, local, queries, pieces, mixed, carried):
    me, my_core, my_line = place()
    me = me % QUAD
    piece = HK // QUAD
    rows = mixed.shape[0] // (2 * groups)
    for h in range(count):
        span = slice(h * piece, (h + 1) * piece)
        for k in range(QUAD):
            start = pl.multiple_of((me ^ k) * piece, piece)
            carried[pl.ds(start, piece), :] = pieces[k][span, :]
        narrow, wide = slice(h * HK, (h + 1) * HK), slice(h * HV, (h + 1) * HV)
        out = local[:, wide] + jnp.dot(
            queries[:, narrow], carried[...], preferred_element_type=F32
        )
        spread = lax.rsqrt(jnp.mean(out * out, axis=-1, keepdims=True) + EPSILON)
        value = (out * spread * gain[...]).astype(BF16)
        for b in range(2 * groups):
            line, core = b // 2, b % 2
            there = (line ^ my_line) + (core ^ my_core) * groups
            there = pl.multiple_of(there * rows, rows)
            mixed[pl.ds(there, rows), wide] = value[b * rows : (b + 1) * rows, :]


def project_early_kernel(count, groups, gain, matrix, local, queries, *refs):
    pieces, (total, mixed, carried) = refs[:QUAD], refs[QUAD:]
    read_heads(count, groups, gain, local, queries, pieces, mixed, carried)
    total[...] = jnp.dot(mixed[...], matrix[...], preferred_element_type=F32)


def project_kernel(count, groups, gain, matrix, local, queries, *refs):
    pieces, early, (mixed, keep, send, carried) = refs[:QUAD], refs[QUAD:-4], refs[-4:]
    read_heads(count, groups, gain, local, queries, pieces, mixed, carried)
    project_rest_kernel(mixed, matrix, *early, keep, send)


def project_rest_kernel(mixed, matrix, *refs):
    early, (keep, send) = refs[:-2], refs[-2:]
    split = keep.shape[0]
    total = jnp.dot(mixed[...], matrix[...], preferred_element_type=F32)
    for part in early:
        total = total + part[...]
    keep[...] = total[:split, :]
    send[...] = total[split:, :].astype(BF16)


def project(count, groups, gain, matrix, local, pieces):
    length = local[0][0].shape[0]
    width = matrix.shape[1]
    depth = count * HV
    cut = width // 2
    small = [
        jax.ShapeDtypeStruct((length // 2, cut), F32),
        jax.ShapeDtypeStruct((length // 2, cut), BF16),
    ]
    whole = [pl.BlockSpec((length // 2, cut), lambda i: (0, 0))] * 2
    chunks = len(local)
    early = []
    for part in range(chunks - 1):
        early.append(
            pl.pallas_call(
                functools.partial(project_early_kernel, count, groups),
                grid=(1,),
                in_specs=[VMEM, pl.BlockSpec((depth, width), lambda i, p=part: (p, 0))]
                + [VMEM] * (2 + QUAD),
                out_specs=pl.BlockSpec((length, width), lambda i: (0, 0)),
                out_shape=jax.ShapeDtypeStruct((length, width), F32),
                scratch_shapes=[
                    pltpu.VMEM((length, depth), BF16),
                    pltpu.VMEM((HK, HV), BF16),
                ],
                compiler_params=params(28),
                cost_estimate=cost(2e9, 8e6),
                name="project_early",
            )(gain, matrix, *local[part], *pieces[part * QUAD : (part + 1) * QUAD])
        )
    last = chunks - 1

    def side_spec(side):
        return pl.BlockSpec((depth, cut), lambda i: (last, side))

    def early_spec(side):
        return [pl.BlockSpec((length, cut), lambda i: (0, side))] * len(early)

    mixed, keep, send = pl.pallas_call(
        functools.partial(project_kernel, count, groups),
        grid=(1,),
        in_specs=[VMEM, side_spec(0)] + [VMEM] * (2 + QUAD) + early_spec(0),
        out_specs=[pl.BlockSpec((length, depth), lambda i: (0, 0))] + whole,
        out_shape=[jax.ShapeDtypeStruct((length, depth), BF16)] + small,
        scratch_shapes=[pltpu.VMEM((HK, HV), BF16)],
        compiler_params=params(28),
        cost_estimate=cost(1e9, 6e6),
        name="project",
    )(gain, matrix, *local[last], *pieces[last * QUAD :], *early)
    rest = pl.pallas_call(
        project_rest_kernel,
        grid=(1,),
        in_specs=[pl.BlockSpec((length, depth), lambda i: (0, 0)), side_spec(1)] + early_spec(1),
        out_specs=whole,
        out_shape=small,
        compiler_params=params(28),
        cost_estimate=cost(1e9, 6e6),
        name="project_rest",
    )(mixed, matrix, *early)
    return (keep, send), rest


def norm_kernel(groups, gain, *refs):
    keeps, received, streams = refs[:2], refs[2:4], refs[4 : 4 + groups]
    arrived = refs[4 + groups : 4 + groups + 2 * (groups - 1)]
    normed, mid = refs[-2:]
    rows, width = mid.shape
    cut = width // 2
    for k in range(groups):
        span = slice(k * rows, (k + 1) * rows)
        values, square = [], None
        for side in range(2):
            columns = slice(side * cut, (side + 1) * cut)
            value = keeps[side][span, :] + received[side][span, :].astype(F32)
            for j in range(1, groups):
                there = k ^ j
                part = arrived[side * (groups - 1) + j - 1]
                value = value + part[there * rows : (there + 1) * rows, :].astype(F32)
            value = value + streams[k][:, columns].astype(F32)
            if k == 0:
                mid[:, columns] = value
            term = jnp.sum(value * value, axis=-1, keepdims=True)
            square = term if square is None else square + term
            values.append((columns, value))
        spread = lax.rsqrt(square / width + EPSILON)
        for columns, value in values:
            normed[span, columns] = (value * spread * gain[:, columns]).astype(BF16)


def midstream_norm(groups, gain, keeps, received, streams, arrived):
    rows, width = streams[0].shape
    arrays = [*keeps, *received, *streams, *arrived]
    return pl.pallas_call(
        functools.partial(norm_kernel, groups),
        in_specs=[VMEM] * (1 + len(arrays)),
        out_specs=[VMEM] * 2,
        out_shape=[
            jax.ShapeDtypeStruct((groups * rows, width), BF16),
            jax.ShapeDtypeStruct((rows, width), F32),
        ],
        compiler_params=params(24),
        cost_estimate=cost(1e7, 3e6),
        name="midstream_norm",
    )(gain, *arrays)


def route_kernel(n, half, groups, routes, weights, select, high, low, table):
    me, core, _ = place()
    length = routes.shape[1]
    earlier = tri(length, lambda r, c: c < r).astype(F32).astype(BF16)
    chosen = jnp.transpose(routes[...].astype(F32)).astype(jnp.int32)
    weight = jnp.transpose(weights[...])
    expert = me ^ lax.broadcasted_iota(jnp.int32, (length, n), 1)
    is_first, is_second = chosen[:, 0:1] == expert, chosen[:, 1:2] == expert
    member = jnp.where(is_first | is_second, 1.0, 0.0)
    rank = jnp.dot(earlier, member.astype(BF16), preferred_element_type=F32)
    slot = jnp.where(member > 0.0, rank, -1.0)
    value = jnp.where(is_first, weight[:, 0:1], weight[:, 1:2])
    top = value.astype(BF16)
    rest = (value - top.astype(F32)).astype(BF16)
    column = lax.broadcasted_iota(jnp.int32, (n, n * half), 1)
    owner = lax.broadcasted_iota(jnp.int32, (n, n * half), 0)
    spread = jnp.where(column // half == owner, 1.0, 0.0).astype(BF16)

    def widen(array):
        return jnp.dot(array, spread, preferred_element_type=F32)

    wanted = core * half + lax.broadcasted_iota(jnp.int32, (length, n * half), 1) % half
    hit = widen(slot.astype(BF16)) == wanted.astype(F32)
    table[0] = jnp.where(hit, 1.0, 0.0)
    table[1] = jnp.where(hit, widen(top), 0.0)
    table[2] = jnp.where(hit, widen(rest), 0.0)
    split = length // 2
    ordered = []
    for span, own, other in block_spans(groups, split // groups):
        below = slice(split + span.start, split + span.stop)
        for out, source in ((high, 1), (low, 2)):
            out[span, :] = table[source, own, :].astype(BF16)
            out[below, :] = table[source, other, :].astype(BF16)
        ordered.append((table[0, own, :], table[0, other, :]))
    chosen = jnp.concatenate([own for own, _ in ordered] + [other for _, other in ordered])
    select[...] = jnp.transpose(chosen).astype(BF16)


def slot_tables(n, half, groups, routes, weights):
    length = routes.shape[1]
    return pl.pallas_call(
        functools.partial(route_kernel, n, half, groups),
        in_specs=[VMEM, VMEM],
        out_specs=[VMEM] * 3,
        out_shape=[
            jax.ShapeDtypeStruct((n * half, length), BF16),
            jax.ShapeDtypeStruct((length, n * half), BF16),
            jax.ShapeDtypeStruct((length, n * half), BF16),
        ],
        scratch_shapes=[pltpu.VMEM((3, length, n * half), F32)],
        compiler_params=params(16),
        cost_estimate=cost(1e8, 5e5),
        name="slot_tables",
    )(routes, weights)


def dispatch_kernel(n, half, select, mine, theirs, *outs):
    split = mine.shape[0]
    picked = jnp.dot(select[:, :split], mine[...], preferred_element_type=F32)
    picked = picked + jnp.dot(select[:, split:], theirs[...], preferred_element_type=F32)
    for k in range(n):
        outs[k][...] = picked[k * half : (k + 1) * half, :].astype(BF16)


def dispatch(n, half, select, mine, theirs):
    width = mine.shape[1]
    return pl.pallas_call(
        functools.partial(dispatch_kernel, n, half),
        in_specs=[VMEM] * 3,
        out_specs=[VMEM] * n,
        out_shape=[jax.ShapeDtypeStruct((half, width), BF16)] * n,
        compiler_params=params(16),
        cost_estimate=cost(5e8, 2e6),
        name="dispatch",
    )(select, mine, theirs)


def fetch_kernel(*refs):
    half = (len(refs) - 1) // 2
    ins, outs, sems = refs[:half], refs[half:-1], refs[-1]
    copies = [
        pltpu.make_async_copy(src, dst, sems.at[i])
        for i, (src, dst) in enumerate(zip(ins, outs))
    ]
    for copy in copies:
        copy.start()
    for copy in copies:
        copy.wait()


def fetch(*arrays):
    return pl.pallas_call(
        fetch_kernel,
        in_specs=[HBM] * len(arrays),
        out_specs=[VMEM] * len(arrays),
        out_shape=[jax.ShapeDtypeStruct(a.shape, a.dtype) for a in arrays],
        scratch_shapes=[pltpu.SemaphoreType.DMA((len(arrays),))],
        compiler_params=params(16),
        cost_estimate=cost(2e9, 1e7),
        name="fetch",
    )(*arrays)


def expert_kernel(count, gate, widen, down, *refs):
    ins, (keep, send) = refs[: 2 * count], refs[2 * count :]
    rows = jnp.concatenate([piece[...] for piece in ins], axis=0)
    gated = contract1(rows, gate[...])
    lifted = contract1(rows, widen[...])
    hidden = (gated * jax.nn.sigmoid(gated) * lifted).astype(BF16)
    out = jnp.dot(hidden, down[...], preferred_element_type=F32)
    split = keep.shape[0]
    keep[...] = out[:split, :]
    send[...] = out[split:, :].astype(BF16)


def expert(weights, mine, theirs):
    count = len(mine)
    half, width = mine[0].shape
    return pl.pallas_call(
        functools.partial(expert_kernel, count),
        in_specs=[VMEM] * (3 + 2 * count),
        out_specs=[VMEM] * 2,
        out_shape=[
            jax.ShapeDtypeStruct((count * half, width), F32),
            jax.ShapeDtypeStruct((count * half, width), BF16),
        ],
        compiler_params=params(24),
        cost_estimate=cost(6e8 * count, 4e6),
    )(*weights, *mine, *theirs)


def merge_kernel(count, keep, received, *outs):
    half = outs[0].shape[0]
    for k in range(count):
        span = slice(k * half, (k + 1) * half)
        outs[k][...] = (keep[span, :] + received[span, :].astype(F32)).astype(BF16)


def merge(count, half, keep, received):
    width = keep.shape[1]
    return pl.pallas_call(
        functools.partial(merge_kernel, count),
        in_specs=[VMEM] * 2,
        out_specs=[VMEM] * count,
        out_shape=[jax.ShapeDtypeStruct((half, width), BF16)] * count,
        compiler_params=params(16),
        cost_estimate=cost(1e7, 4e6),
    )(keep, received)


def combine_kernel(n, high, low, *refs):
    ins, (keep, send) = refs[:n], refs[n:]
    rows = jnp.concatenate([piece[...] for piece in ins], axis=0)
    total = jnp.dot(high[...], rows, preferred_element_type=F32)
    total = total + jnp.dot(low[...], rows, preferred_element_type=F32)
    split = keep.shape[0]
    keep[...] = total[:split, :]
    send[...] = total[split:, :].astype(BF16)


def combine(n, side, high, low, pieces):
    half, width = pieces[0].shape
    length, slots = high.shape
    cut = width // 2
    table = pl.BlockSpec((length, slots), lambda i: (0, 0))
    return pl.pallas_call(
        functools.partial(combine_kernel, n),
        grid=(1,),
        in_specs=[table] * 2 + [pl.BlockSpec((half, cut), lambda i: (0, side))] * n,
        out_specs=[pl.BlockSpec((length // 2, cut), lambda i: (0, 0))] * 2,
        out_shape=[
            jax.ShapeDtypeStruct((length // 2, cut), F32),
            jax.ShapeDtypeStruct((length // 2, cut), BF16),
        ],
        compiler_params=params(16),
        cost_estimate=cost(5e8, 2e6),
    )(high, low, *pieces)


def final_kernel(groups, mid, *refs):
    keeps, received, parts, out = refs[:2], refs[2:4], refs[4:-1], refs[-1]
    rows, width = mid.shape
    cut = width // 2
    for side in range(2):
        columns = slice(side * cut, (side + 1) * cut)
        total = mid[:, columns] + keeps[side][:rows, :] + received[side][:rows, :].astype(F32)
        for k in range(groups - 1):
            total = total + parts[side * (groups - 1) + k][...].astype(F32)
        out[:, columns] = total.astype(BF16)


def final(groups, mid, keeps, received, parts):
    arrays = [*keeps, *received, *parts]
    return pl.pallas_call(
        functools.partial(final_kernel, groups),
        in_specs=[VMEM] * (1 + len(arrays)),
        out_specs=VMEM,
        out_shape=jax.ShapeDtypeStruct(mid.shape, BF16),
        compiler_params=params(16),
        cost_estimate=cost(1e6, 2e6),
        name="final",
    )(mid, *arrays)


def swap(value, axis, k):
    return lax.ppermute(value, axis, xor_perm(axis, k))


def exchange(pieces):
    return [pieces[0]] + [swap(pieces[k], "sp", k) for k in range(1, len(pieces))]


def body(
    stream_in,
    queries,
    key_rows,
    values,
    decay_low,
    decay_matrix,
    decay_bias,
    decay_shift,
    head_gain,
    output_matrix,
    feed_gain,
    routes,
    route_weights,
    expert_gate,
    specialist_widen,
    expert_down,
):
    length = queries.shape[0]
    heads = queries.shape[1] // HK
    n = lax.axis_size("sp")
    head_devices = lax.axis_size("tp")
    groups = head_devices // 2
    rows = length // head_devices
    half = TOP * length // n // 2
    bias = decay_bias.reshape(1, -1)

    low, shift = decay_low.T, decay_shift.T
    count = heads // 2 if heads % 2 == 0 else heads

    gathered, states = [], None
    for part, first in enumerate(range(0, heads, count)):
        low_here = low
        if states is not None:
            low_here, states = lax.optimization_barrier((low, states))
        states = device_states(
            first, count, low_here, decay_matrix, bias, shift, key_rows, values
        )
        gathered.append(exchange(states))
    stream_in, _ = lax.optimization_barrier((stream_in, states))
    streams = [stream_in] + [swap(stream_in, "tp", 2 * k) for k in range(1, groups)]
    local = [
        local_attention(
            first, count, low, decay_matrix, bias, shift, queries, key_rows, values
        )
        for first in range(0, heads, count)
    ]
    select, high, low_part = slot_tables(
        n, half, groups, routes.T, route_weights.T
    )
    carried = []
    for part, pieces in enumerate(gathered):
        entry = quad_entry(count, pieces)
        carried += exchange(quad_prefix(count, True, entry, pieces))
    sides = project(
        count, groups, head_gain.reshape(1, -1), output_matrix, local, carried
    )
    received, shared = [], []
    for keep, send in sides:
        received.append(swap(send, "tp", 1))
        shared.append((keep + received[-1].astype(F32)).astype(BF16))
    arrived = [swap(value, "tp", 2 * k) for value in shared for k in range(1, groups)]
    weights, _ = lax.optimization_barrier(
        ((expert_gate[0].T, specialist_widen[0].T, expert_down[0]), shared)
    )
    weights = fetch(*weights)
    arrived, weights, select, high, low_part = lax.optimization_barrier(
        (arrived, weights, select, high, low_part)
    )
    normed, mid = midstream_norm(
        groups,
        feed_gain.reshape(1, -1),
        [keep for keep, _ in sides],
        received,
        streams,
        arrived,
    )
    theirs = swap(normed, "tp", 1)
    slots = dispatch(n, half, select, normed, theirs)
    slots = exchange(slots)
    back, previous = {}, None
    for part, ks in enumerate(expert_chunks(n)):
        mine = [slots[k] for k in ks]
        if previous is not None:
            mine, previous = lax.optimization_barrier((mine, previous))
        theirs = [swap(slot, "tp", 1) for slot in mine]
        kept, sent = expert(weights, mine, theirs)
        received = swap(sent, "tp", 1)
        merged = merge(len(ks), half, kept, received)
        previous = sent if part == 1 else merged
        for k, piece in zip(ks, merged):
            back[k] = piece if k == 0 else swap(piece, "sp", k)
    back = [back[k] for k in range(n)]
    keeps, received, parts = [], [], []
    for side in range(2):
        keep, send = combine(n, side, high, low_part, back)
        other = swap(send, "tp", 1)
        for k in range(1, groups):
            span = slice(k * rows, (k + 1) * rows)
            part = (keep[span] + other[span].astype(F32)).astype(BF16)
            parts.append(swap(part, "tp", 2 * k))
        keeps.append(keep)
        received.append(other)
    return final(groups, mid, keeps, received, parts)


def expert_chunks(n):
    middle = (QUAD + n) // 2
    return [range(QUAD, middle), range(QUAD), range(middle, n)]


def solution(mesh):
    return jax.shard_map(
        body,
        mesh=mesh,
        in_specs=(
            P(("sp", "tp"), None),
            P("sp", "tp"),
            P("sp", "tp"),
            P("sp", "tp"),
            P("sp", None),
            P(None, "tp"),
            P("tp"),
            P("sp", "tp"),
            P(),
            P("tp", None),
            P(),
            P("sp", None),
            P("sp", None),
            P("sp", None, "tp"),
            P("sp", None, "tp"),
            P("sp", "tp", None),
        ),
        out_specs=P(("sp", "tp"), None),
        check_vma=False,
    )
```

```python
import functools
import jax
import jax.numpy as jnp
from jax import lax
from jax.experimental import pallas as pl
from jax.experimental.pallas import tpu as pltpu
from jax.sharding import PartitionSpec as P


HK = 256
HV = 512
TOP = 2
BLK = 128
TEMPER = 16.0
EPSILON = 1e-06
F32 = jnp.float32
BF16 = jnp.bfloat16
VMEM = pl.BlockSpec(memory_space=pltpu.VMEM)
SMEM = pl.BlockSpec(memory_space=pltpu.SMEM)
HBM = pl.BlockSpec(memory_space=pltpu.HBM)
QUAD = 4


def cost(flops, moved):
    return pl.CostEstimate(flops=int(flops), bytes_accessed=int(moved), transcendentals=0)


def params(mib):
    return pltpu.CompilerParams(vmem_limit_bytes=mib * 1024 * 1024)


def place():
    tp = lax.axis_index("tp")
    return lax.axis_index("sp"), tp % 2, tp // 2


def xor_perm(axis, k):
    return [(i, i ^ k) for i in range(lax.axis_size(axis))]


def tri(n, fn):
    row = lax.broadcasted_iota(jnp.int32, (n, n), 0)
    col = lax.broadcasted_iota(jnp.int32, (n, n), 1)
    return fn(row, col)


def contract0(a, b):
    return lax.dot_general(a, b, (((0,), (0,)), ((), ())), preferred_element_type=F32)


def contract1(a, b):
    return lax.dot_general(a, b, (((1,), (1,)), ((), ())), preferred_element_type=F32)


def split_dot(ones, value):
    total = None
    for _ in range(3):
        part = value.astype(BF16)
        value = value - part.astype(F32)
        term = jnp.dot(ones, part, preferred_element_type=F32)
        total = term if total is None else total + term
    return total


def head_log_decay(low, matrix, bias, shift, head):
    pre = contract0(low, matrix) + bias
    logged = (jnp.minimum(pre, 0.0) - jnp.log1p(jnp.exp(-jnp.abs(pre)))) / TEMPER
    return logged + jnp.transpose(shift)[:, head : head + 1]


def state_kernel(first, count, low, matrix, bias, shift, key_rows, values, *rest):
    outs, (state, decays) = rest[:QUAD], rest[QUAD:]
    length = low.shape[1]
    piece = HK // QUAD
    after = tri(length, lambda r, c: c > r).astype(F32).astype(BF16)
    me = place()[0] % QUAD
    decays[...] = jnp.zeros_like(decays)
    for h in range(count):
        narrow, wide = slice(h * HK, (h + 1) * HK), slice(h * HV, (h + 1) * HV)
        logs = head_log_decay(
            low[...], matrix[:, narrow], bias[:, narrow], shift[...], first + h
        )
        suffix = split_dot(after, logs)
        total = jnp.exp(suffix[0:1, :] + logs[0:1, :])
        high = total.astype(BF16).astype(F32)
        decays[h : h + 1, 0:HK] = high
        decays[h : h + 1, HK : 2 * HK] = total - high
        end_keys = (key_rows[:, narrow].astype(F32) * jnp.exp(suffix)).astype(BF16)
        state[...] = contract0(end_keys, values[:, wide])
        for k in range(QUAD):
            start = pl.multiple_of((me ^ k) * piece, piece)
            outs[k][h * piece : (h + 1) * piece, :] = state[pl.ds(start, piece), :].astype(BF16)
    for k in range(QUAD):
        outs[k][count * piece :, :] = decays[...].astype(BF16)


def device_states(first, count, low, matrix, bias, shift, key_rows, values):
    length = key_rows.shape[0]
    rows = count * (HK // QUAD) + 8
    block = first // count

    def whole(array):
        return pl.BlockSpec(array.shape, lambda i: (0, 0))

    def part(height, width):
        return pl.BlockSpec((height, count * width), lambda i: (0, block))

    return pl.pallas_call(
        functools.partial(state_kernel, first, count),
        grid=(1,),
        in_specs=[
            whole(low),
            part(matrix.shape[0], HK),
            part(1, HK),
            whole(shift),
            part(length, HK),
            part(length, HV),
        ],
        out_specs=[pl.BlockSpec((rows, HV), lambda i: (0, 0))] * QUAD,
        out_shape=[jax.ShapeDtypeStruct((rows, HV), BF16)] * QUAD,
        scratch_shapes=[pltpu.VMEM((HK, HV), F32), pltpu.VMEM((8, HV), F32)],
        compiler_params=params(60 if first == 0 else 53),
        cost_estimate=cost(count * 4e8, count * 5e5),
    )(low, matrix, bias, shift, key_rows, values)


def local_kernel(first, count, low, matrix, bias, shift, queries, key_rows, values, *refs):
    out, query_out = refs[-2:]
    length = low.shape[1]
    below = tri(BLK, lambda r, c: c <= r)
    lower = below.astype(F32).astype(BF16)
    scale = HK ** (-0.5)
    for h in range(count):
        narrow, wide = slice(h * HK, (h + 1) * HK), slice(h * HV, (h + 1) * HV)
        logs = head_log_decay(
            low[...], matrix[:, narrow], bias[:, narrow], shift[...], first + h
        )
        before = jnp.zeros((1, HK), F32)
        earlier = []
        for b in range(length // BLK):
            rows = slice(b * BLK, (b + 1) * BLK)
            inside = split_dot(lower, logs[rows])
            final = inside[BLK - 1 : BLK, :]
            middle = inside[BLK // 2 - 1 : BLK // 2, :]
            query = queries[rows, narrow].astype(F32) * scale
            keys = key_rows[rows, narrow].astype(F32)
            grown = query * jnp.exp(inside)
            near_query = (query * jnp.exp(inside - middle)).astype(BF16)
            near_key = (keys * jnp.exp(middle - inside)).astype(BF16)
            scores = jnp.where(below, contract1(near_query, near_key), 0.0).astype(BF16)
            total = jnp.dot(scores, values[rows, wide], preferred_element_type=F32)
            here = grown.astype(BF16)
            for past_keys, past in earlier:
                cross = contract1(here, past_keys.astype(BF16)).astype(BF16)
                total = total + jnp.dot(cross, values[past, wide], preferred_element_type=F32)
            out[rows, wide] = total
            query_out[rows, narrow] = (grown * jnp.exp(before)).astype(BF16)
            if b + 1 < length // BLK:
                earlier = [(old * jnp.exp(final), past) for old, past in earlier]
                earlier.append((keys * jnp.exp(final - inside), rows))
                before = before + final


def local_attention(first, count, low, matrix, bias, shift, queries, key_rows, values):
    length = low.shape[1]
    block = first // count

    def part(width):
        return pl.BlockSpec((length, count * width), lambda i: (0, block))

    return pl.pallas_call(
        functools.partial(local_kernel, first, count),
        grid=(1,),
        in_specs=[
            pl.BlockSpec(low.shape, lambda i: (0, 0)),
            pl.BlockSpec((low.shape[0], count * HK), lambda i: (0, block)),
            pl.BlockSpec((1, count * HK), lambda i: (0, block)),
            pl.BlockSpec(shift.shape, lambda i: (0, 0)),
            part(HK),
            part(HK),
            part(HV),
        ],
        out_specs=[
            pl.BlockSpec((length, count * HV), lambda i: (0, 0)),
            pl.BlockSpec((length, count * HK), lambda i: (0, 0)),
        ],
        out_shape=[
            jax.ShapeDtypeStruct((length, count * HV), F32),
            jax.ShapeDtypeStruct((length, count * HK), BF16),
        ],
        compiler_params=params(24),
        cost_estimate=cost(count * 4e8, count * 1.2e6),
    )(low, matrix, bias, shift, queries, key_rows, values)


def prefix_kernel(count, emit, primed, *refs):
    start, refs = (refs[0], refs[1:]) if primed else (None, refs)
    ins, outs = refs[:QUAD], refs[QUAD:]
    me = place()[0] % QUAD
    piece = HK // QUAD
    rows = count * piece
    tails = jnp.concatenate([ref[rows : rows + 8, :].astype(F32) for ref in ins], axis=0)
    across = jnp.transpose(tails[:, :HK] + tails[:, HK:])
    parts = [across[i * piece : (i + 1) * piece, :] for i in range(QUAD)]
    mine = parts[0]
    for i in range(1, QUAD):
        mine = jnp.where(me == i, parts[i], mine)
    decay = [mine[:, k * 8 : k * 8 + count] for k in range(QUAD)]
    spot = [me ^ k for k in range(QUAD)]
    ends = spot if emit else [jnp.int32(QUAD)]

    def between(low, end):
        factor = jnp.ones_like(decay[0])
        for k in range(QUAD):
            inside = jnp.logical_and(spot[k] > low, spot[k] < end)
            factor = jnp.where(inside, factor * decay[k], factor)
        return factor

    weights = [
        [jnp.where(spot[k] < end, between(spot[k], end), 0.0) for k in range(QUAD)]
        + ([between(-1, end)] if primed else [])
        for end in ends
    ]
    for h in range(count):
        span = slice(h * piece, (h + 1) * piece)
        sources = [ref[span, :].astype(F32) for ref in ins]
        if primed:
            sources.append(start[span, :].astype(F32))
        for out, factors in zip(outs, weights):
            total = None
            for source, factor in zip(sources, factors):
                term = source * factor[:, h : h + 1]
                total = term if total is None else total + term
            out[span, :] = total.astype(BF16)


def quad_prefix(count, emit, start, pieces):
    rows = count * (HK // QUAD)
    outs = QUAD if emit else 1
    primed = [] if start is None else [start]
    return pl.pallas_call(
        functools.partial(prefix_kernel, count, emit, start is not None),
        in_specs=[VMEM] * (QUAD + len(primed)),
        out_specs=[VMEM] * outs,
        out_shape=[jax.ShapeDtypeStruct((rows, HV), BF16)] * outs,
        compiler_params=params(24),
        cost_estimate=cost(1e8, 1e6),
        name="prefix" if emit else "total",
    )(*primed, *pieces)


def quad_entry(count, pieces):
    start = None
    quads = lax.axis_size("sp") // QUAD
    entry = None
    for g in range(quads - 1):
        (total,) = quad_prefix(count, False, start, pieces)
        perm = [(g * QUAD + i, (g + 1) * QUAD + i) for i in range(QUAD)]
        start = lax.ppermute(total, "sp", perm)
        entry = start if entry is None else entry + start
    return entry


def block_spans(groups, rows):
    _, core, line = place()
    for k in range(groups):
        base = (line ^ k) * 2
        own = pl.ds(pl.multiple_of((base + core) * rows, rows), rows)
        other = pl.ds(pl.multiple_of((base + 1 - core) * rows, rows), rows)
        yield slice(k * rows, (k + 1) * rows), own, other


def read_heads(count, groups, gain, local, queries, pieces, mixed, carried):
    me, my_core, my_line = place()
    me = me % QUAD
    piece = HK // QUAD
    rows = mixed.shape[0] // (2 * groups)
    for h in range(count):
        span = slice(h * piece, (h + 1) * piece)
        for k in range(QUAD):
            start = pl.multiple_of((me ^ k) * piece, piece)
            carried[pl.ds(start, piece), :] = pieces[k][span, :]
        narrow, wide = slice(h * HK, (h + 1) * HK), slice(h * HV, (h + 1) * HV)
        out = local[:, wide] + jnp.dot(
            queries[:, narrow], carried[...], preferred_element_type=F32
        )
        spread = lax.rsqrt(jnp.mean(out * out, axis=-1, keepdims=True) + EPSILON)
        value = (out * spread * gain[...]).astype(BF16)
        for b in range(2 * groups):
            line, core = b // 2, b % 2
            there = (line ^ my_line) + (core ^ my_core) * groups
            there = pl.multiple_of(there * rows, rows)
            mixed[pl.ds(there, rows), wide] = value[b * rows : (b + 1) * rows, :]


def project_early_kernel(count, groups, gain, matrix, local, queries, *refs):
    pieces, (total, mixed, carried) = refs[:QUAD], refs[QUAD:]
    read_heads(count, groups, gain, local, queries, pieces, mixed, carried)
    total[...] = jnp.dot(mixed[...], matrix[...], preferred_element_type=F32)


def project_kernel(count, groups, gain, matrix, local, queries, *refs):
    pieces, early, (mixed, keep, send, carried) = refs[:QUAD], refs[QUAD:-4], refs[-4:]
    read_heads(count, groups, gain, local, queries, pieces, mixed, carried)
    project_rest_kernel(mixed, matrix, *early, keep, send)


def project_rest_kernel(mixed, matrix, *refs):
    early, (keep, send) = refs[:-2], refs[-2:]
    split = keep.shape[0]
    total = jnp.dot(mixed[...], matrix[...], preferred_element_type=F32)
    for part in early:
        total = total + part[...]
    keep[...] = total[:split, :]
    send[...] = total[split:, :].astype(BF16)


def project(count, groups, gain, matrix, local, pieces):
    length = local[0][0].shape[0]
    width = matrix.shape[1]
    depth = count * HV
    cut = width // 2
    small = [
        jax.ShapeDtypeStruct((length // 2, cut), F32),
        jax.ShapeDtypeStruct((length // 2, cut), BF16),
    ]
    whole = [pl.BlockSpec((length // 2, cut), lambda i: (0, 0))] * 2
    chunks = len(local)
    early = []
    for part in range(chunks - 1):
        early.append(
            pl.pallas_call(
                functools.partial(project_early_kernel, count, groups),
                grid=(1,),
                in_specs=[VMEM, pl.BlockSpec((depth, width), lambda i, p=part: (p, 0))]
                + [VMEM] * (2 + QUAD),
                out_specs=pl.BlockSpec((length, width), lambda i: (0, 0)),
                out_shape=jax.ShapeDtypeStruct((length, width), F32),
                scratch_shapes=[
                    pltpu.VMEM((length, depth), BF16),
                    pltpu.VMEM((HK, HV), BF16),
                ],
                compiler_params=params(28),
                cost_estimate=cost(2e9, 8e6),
                name="early",
            )(gain, matrix, *local[part], *pieces[part * QUAD : (part + 1) * QUAD])
        )
    last = chunks - 1

    def side_spec(side):
        return pl.BlockSpec((depth, cut), lambda i: (last, side))

    def early_spec(side):
        return [pl.BlockSpec((length, cut), lambda i: (0, side))] * len(early)

    mixed, keep, send = pl.pallas_call(
        functools.partial(project_kernel, count, groups),
        grid=(1,),
        in_specs=[VMEM, side_spec(0)] + [VMEM] * (2 + QUAD) + early_spec(0),
        out_specs=[pl.BlockSpec((length, depth), lambda i: (0, 0))] + whole,
        out_shape=[jax.ShapeDtypeStruct((length, depth), BF16)] + small,
        scratch_shapes=[pltpu.VMEM((HK, HV), BF16)],
        compiler_params=params(28),
        cost_estimate=cost(1e9, 6e6),
        name="project",
    )(gain, matrix, *local[last], *pieces[last * QUAD :], *early)
    rest = pl.pallas_call(
        project_rest_kernel,
        grid=(1,),
        in_specs=[pl.BlockSpec((length, depth), lambda i: (0, 0)), side_spec(1)] + early_spec(1),
        out_specs=whole,
        out_shape=small,
        compiler_params=params(28),
        cost_estimate=cost(1e9, 6e6),
        name="rest",
    )(mixed, matrix, *early)
    return (keep, send), rest


def norm_kernel(groups, gain, *refs):
    keeps, received, streams = refs[:2], refs[2:4], refs[4 : 4 + groups]
    arrived = refs[4 + groups : 4 + groups + 2 * (groups - 1)]
    normed, mid = refs[-2:]
    rows, width = mid.shape
    cut = width // 2
    for k in range(groups):
        span = slice(k * rows, (k + 1) * rows)
        values, square = [], None
        for side in range(2):
            columns = slice(side * cut, (side + 1) * cut)
            value = keeps[side][span, :] + received[side][span, :].astype(F32)
            for j in range(1, groups):
                there = k ^ j
                part = arrived[side * (groups - 1) + j - 1]
                value = value + part[there * rows : (there + 1) * rows, :].astype(F32)
            value = value + streams[k][:, columns].astype(F32)
            if k == 0:
                mid[:, columns] = value
            term = jnp.sum(value * value, axis=-1, keepdims=True)
            square = term if square is None else square + term
            values.append((columns, value))
        spread = lax.rsqrt(square / width + EPSILON)
        for columns, value in values:
            normed[span, columns] = (value * spread * gain[:, columns]).astype(BF16)


def midstream_norm(groups, gain, keeps, received, streams, arrived):
    rows, width = streams[0].shape
    arrays = [*keeps, *received, *streams, *arrived]
    return pl.pallas_call(
        functools.partial(norm_kernel, groups),
        in_specs=[VMEM] * (1 + len(arrays)),
        out_specs=[VMEM] * 2,
        out_shape=[
            jax.ShapeDtypeStruct((groups * rows, width), BF16),
            jax.ShapeDtypeStruct((rows, width), F32),
        ],
        compiler_params=params(24),
        cost_estimate=cost(1e7, 3e6),
        name="norm",
    )(gain, *arrays)


def route_kernel(n, half, groups, routes, weights, select, high, low, table):
    me, core, _ = place()
    length = routes.shape[1]
    earlier = tri(length, lambda r, c: c < r).astype(F32).astype(BF16)
    chosen = jnp.transpose(routes[...].astype(F32)).astype(jnp.int32)
    weight = jnp.transpose(weights[...])
    expert = me ^ lax.broadcasted_iota(jnp.int32, (length, n), 1)
    is_first, is_second = chosen[:, 0:1] == expert, chosen[:, 1:2] == expert
    member = jnp.where(is_first | is_second, 1.0, 0.0)
    rank = jnp.dot(earlier, member.astype(BF16), preferred_element_type=F32)
    slot = jnp.where(member > 0.0, rank, -1.0)
    value = jnp.where(is_first, weight[:, 0:1], weight[:, 1:2])
    top = value.astype(BF16)
    rest = (value - top.astype(F32)).astype(BF16)
    column = lax.broadcasted_iota(jnp.int32, (n, n * half), 1)
    owner = lax.broadcasted_iota(jnp.int32, (n, n * half), 0)
    spread = jnp.where(column // half == owner, 1.0, 0.0).astype(BF16)

    def widen(array):
        return jnp.dot(array, spread, preferred_element_type=F32)

    wanted = core * half + lax.broadcasted_iota(jnp.int32, (length, n * half), 1) % half
    hit = widen(slot.astype(BF16)) == wanted.astype(F32)
    table[0] = jnp.where(hit, 1.0, 0.0)
    table[1] = jnp.where(hit, widen(top), 0.0)
    table[2] = jnp.where(hit, widen(rest), 0.0)
    split = length // 2
    ordered = []
    for span, own, other in block_spans(groups, split // groups):
        below = slice(split + span.start, split + span.stop)
        for out, source in ((high, 1), (low, 2)):
            out[span, :] = table[source, own, :].astype(BF16)
            out[below, :] = table[source, other, :].astype(BF16)
        ordered.append((table[0, own, :], table[0, other, :]))
    chosen = jnp.concatenate([own for own, _ in ordered] + [other for _, other in ordered])
    select[...] = jnp.transpose(chosen).astype(BF16)


def slot_tables(n, half, groups, routes, weights):
    length = routes.shape[1]
    return pl.pallas_call(
        functools.partial(route_kernel, n, half, groups),
        in_specs=[VMEM, VMEM],
        out_specs=[VMEM] * 3,
        out_shape=[
            jax.ShapeDtypeStruct((n * half, length), BF16),
            jax.ShapeDtypeStruct((length, n * half), BF16),
            jax.ShapeDtypeStruct((length, n * half), BF16),
        ],
        scratch_shapes=[pltpu.VMEM((3, length, n * half), F32)],
        compiler_params=params(16),
        cost_estimate=cost(1e8, 5e5),
        name="slots",
    )(routes, weights)


def dispatch_kernel(n, half, select, mine, theirs, *outs):
    split = mine.shape[0]
    picked = jnp.dot(select[:, :split], mine[...], preferred_element_type=F32)
    picked = picked + jnp.dot(select[:, split:], theirs[...], preferred_element_type=F32)
    for k in range(n):
        outs[k][...] = picked[k * half : (k + 1) * half, :].astype(BF16)


def dispatch(n, half, select, mine, theirs):
    width = mine.shape[1]
    return pl.pallas_call(
        functools.partial(dispatch_kernel, n, half),
        in_specs=[VMEM] * 3,
        out_specs=[VMEM] * n,
        out_shape=[jax.ShapeDtypeStruct((half, width), BF16)] * n,
        compiler_params=params(16),
        cost_estimate=cost(5e8, 2e6),
        name="dispatch",
    )(select, mine, theirs)


def fetch_kernel(*refs):
    half = (len(refs) - 1) // 2
    ins, outs, sems = refs[:half], refs[half:-1], refs[-1]
    copies = [
        pltpu.make_async_copy(src, dst, sems.at[i])
        for i, (src, dst) in enumerate(zip(ins, outs))
    ]
    for copy in copies:
        copy.start()
    for copy in copies:
        copy.wait()


def fetch(*arrays):
    return pl.pallas_call(
        fetch_kernel,
        in_specs=[HBM] * len(arrays),
        out_specs=[VMEM] * len(arrays),
        out_shape=[jax.ShapeDtypeStruct(a.shape, a.dtype) for a in arrays],
        scratch_shapes=[pltpu.SemaphoreType.DMA((len(arrays),))],
        compiler_params=params(16),
        cost_estimate=cost(2e9, 1e7),
        name="fetch",
    )(*arrays)


def expert_kernel(count, gate, widen, down, *refs):
    ins, (keep, send) = refs[: 2 * count], refs[2 * count :]
    rows = jnp.concatenate([piece[...] for piece in ins], axis=0)
    gated = contract1(rows, gate[...])
    lifted = contract1(rows, widen[...])
    hidden = (gated * jax.nn.sigmoid(gated) * lifted).astype(BF16)
    out = jnp.dot(hidden, down[...], preferred_element_type=F32)
    split = keep.shape[0]
    keep[...] = out[:split, :]
    send[...] = out[split:, :].astype(BF16)


def expert(weights, mine, theirs):
    count = len(mine)
    half, width = mine[0].shape
    return pl.pallas_call(
        functools.partial(expert_kernel, count),
        in_specs=[VMEM] * (3 + 2 * count),
        out_specs=[VMEM] * 2,
        out_shape=[
            jax.ShapeDtypeStruct((count * half, width), F32),
            jax.ShapeDtypeStruct((count * half, width), BF16),
        ],
        compiler_params=params(24),
        cost_estimate=cost(6e8 * count, 4e6),
    )(*weights, *mine, *theirs)


def merge_kernel(count, keep, received, *outs):
    half = outs[0].shape[0]
    for k in range(count):
        span = slice(k * half, (k + 1) * half)
        outs[k][...] = (keep[span, :] + received[span, :].astype(F32)).astype(BF16)


def merge(count, half, keep, received):
    width = keep.shape[1]
    return pl.pallas_call(
        functools.partial(merge_kernel, count),
        in_specs=[VMEM] * 2,
        out_specs=[VMEM] * count,
        out_shape=[jax.ShapeDtypeStruct((half, width), BF16)] * count,
        compiler_params=params(16),
        cost_estimate=cost(1e7, 4e6),
    )(keep, received)


def combine_kernel(n, high, low, *refs):
    ins, (keep, send) = refs[:n], refs[n:]
    rows = jnp.concatenate([piece[...] for piece in ins], axis=0)
    total = jnp.dot(high[...], rows, preferred_element_type=F32)
    total = total + jnp.dot(low[...], rows, preferred_element_type=F32)
    split = keep.shape[0]
    keep[...] = total[:split, :]
    send[...] = total[split:, :].astype(BF16)


def combine(n, side, high, low, pieces):
    half, width = pieces[0].shape
    length, slots = high.shape
    cut = width // 2
    table = pl.BlockSpec((length, slots), lambda i: (0, 0))
    return pl.pallas_call(
        functools.partial(combine_kernel, n),
        grid=(1,),
        in_specs=[table] * 2 + [pl.BlockSpec((half, cut), lambda i: (0, side))] * n,
        out_specs=[pl.BlockSpec((length // 2, cut), lambda i: (0, 0))] * 2,
        out_shape=[
            jax.ShapeDtypeStruct((length // 2, cut), F32),
            jax.ShapeDtypeStruct((length // 2, cut), BF16),
        ],
        compiler_params=params(16),
        cost_estimate=cost(5e8, 2e6),
    )(high, low, *pieces)


def final_kernel(groups, mid, *refs):
    keeps, received, parts, out = refs[:2], refs[2:4], refs[4:-1], refs[-1]
    rows, width = mid.shape
    cut = width // 2
    for side in range(2):
        columns = slice(side * cut, (side + 1) * cut)
        total = mid[:, columns] + keeps[side][:rows, :] + received[side][:rows, :].astype(F32)
        for k in range(groups - 1):
            total = total + parts[side * (groups - 1) + k][...].astype(F32)
        out[:, columns] = total.astype(BF16)


def final(groups, mid, keeps, received, parts):
    arrays = [*keeps, *received, *parts]
    return pl.pallas_call(
        functools.partial(final_kernel, groups),
        in_specs=[VMEM] * (1 + len(arrays)),
        out_specs=VMEM,
        out_shape=jax.ShapeDtypeStruct(mid.shape, BF16),
        compiler_params=params(16),
        cost_estimate=cost(1e6, 2e6),
        name="final",
    )(mid, *arrays)


def swap(value, axis, k):
    return lax.ppermute(value, axis, xor_perm(axis, k))


def exchange(pieces):
    return [pieces[0]] + [swap(pieces[k], "sp", k) for k in range(1, len(pieces))]


def body(
    stream_in,
    queries,
    key_rows,
    values,
    decay_low,
    decay_matrix,
    decay_bias,
    decay_shift,
    head_gain,
    output_matrix,
    feed_gain,
    routes,
    route_weights,
    expert_gate,
    specialist_widen,
    expert_down,
):
    length = queries.shape[0]
    heads = queries.shape[1] // HK
    n = lax.axis_size("sp")
    head_devices = lax.axis_size("tp")
    groups = head_devices // 2
    rows = length // head_devices
    half = TOP * length // n // 2
    bias = decay_bias.reshape(1, -1)

    low, shift = decay_low.T, decay_shift.T
    count = heads // 2 if heads % 2 == 0 else heads

    gathered, states = [], None
    for part, first in enumerate(range(0, heads, count)):
        low_here = low
        if states is not None:
            low_here, states = lax.optimization_barrier((low, states))
        states = device_states(
            first, count, low_here, decay_matrix, bias, shift, key_rows, values
        )
        gathered.append(exchange(states))
    stream_in, _ = lax.optimization_barrier((stream_in, states))
    streams = [stream_in] + [swap(stream_in, "tp", 2 * k) for k in range(1, groups)]
    local = [
        local_attention(
            first, count, low, decay_matrix, bias, shift, queries, key_rows, values
        )
        for first in range(0, heads, count)
    ]
    select, high, low_part = slot_tables(
        n, half, groups, routes.T, route_weights.T
    )
    carried = []
    for part, pieces in enumerate(gathered):
        entry = quad_entry(count, pieces)
        carried += exchange(quad_prefix(count, True, entry, pieces))
    sides = project(
        count, groups, head_gain.reshape(1, -1), output_matrix, local, carried
    )
    received, shared = [], []
    for keep, send in sides:
        received.append(swap(send, "tp", 1))
        shared.append((keep + received[-1].astype(F32)).astype(BF16))
    arrived = [swap(value, "tp", 2 * k) for value in shared for k in range(1, groups)]
    weights, _ = lax.optimization_barrier(
        ((expert_gate[0].T, specialist_widen[0].T, expert_down[0]), shared)
    )
    weights = fetch(*weights)
    arrived, weights, select, high, low_part = lax.optimization_barrier(
        (arrived, weights, select, high, low_part)
    )
    normed, mid = midstream_norm(
        groups,
        feed_gain.reshape(1, -1),
        [keep for keep, _ in sides],
        received,
        streams,
        arrived,
    )
    theirs = swap(normed, "tp", 1)
    slots = dispatch(n, half, select, normed, theirs)
    slots = exchange(slots)
    back, previous = {}, None
    for part, ks in enumerate(expert_chunks(n)):
        mine = [slots[k] for k in ks]
        if previous is not None:
            mine, previous = lax.optimization_barrier((mine, previous))
        theirs = [swap(slot, "tp", 1) for slot in mine]
        kept, sent = expert(weights, mine, theirs)
        received = swap(sent, "tp", 1)
        merged = merge(len(ks), half, kept, received)
        previous = sent if part == 1 else merged
        for k, piece in zip(ks, merged):
            back[k] = piece if k == 0 else swap(piece, "sp", k)
    back = [back[k] for k in range(n)]
    keeps, received, parts = [], [], []
    for side in range(2):
        keep, send = combine(n, side, high, low_part, back)
        other = swap(send, "tp", 1)
        for k in range(1, groups):
            span = slice(k * rows, (k + 1) * rows)
            part = (keep[span] + other[span].astype(F32)).astype(BF16)
            parts.append(swap(part, "tp", 2 * k))
        keeps.append(keep)
        received.append(other)
    return final(groups, mid, keeps, received, parts)


def expert_chunks(n):
    middle = (QUAD + n) // 2
    return [range(QUAD, middle), range(QUAD), range(middle, n)]


def solution(mesh):
    return jax.shard_map(
        body,
        mesh=mesh,
        in_specs=(
            P(("sp", "tp"), None),
            P("sp", "tp"),
            P("sp", "tp"),
            P("sp", "tp"),
            P("sp", None),
            P(None, "tp"),
            P("tp"),
            P("sp", "tp"),
            P(),
            P("tp", None),
            P(),
            P("sp", None),
            P("sp", None),
            P("sp", None, "tp"),
            P("sp", None, "tp"),
            P("sp", "tp", None),
        ),
        out_specs=P(("sp", "tp"), None),
        check_vma=False,
    )
```
